512 devices in a mesh: sp: 32 (over z, core), tp: 16 (over y, x).
Axes of the slice: x: 4, y: 4, z: 16, core: 2. Of those that a mesh axis runs over, the one named last changes fastest.
Arguments:
- moe_input: bfloat16 [8192, 2048], P('sp', 'tp'), may hold values from -6 to 6
- out_grad: bfloat16 [8192, 2048], P('sp', 'tp'), may hold values from -12 to 12
- routes: int32 [8192, 2], P('sp'), may hold values from 0 to 31, all different within a row; in each aligned block of 256 rows (0 to 255, 256 to 511, ...) at most 20 rows name the same one
- route_weight: float32 [8192, 2], P('sp'), may hold values from 0.2 to 1.5
- w_gate: bfloat16 [32, 2048, 2048], P('sp', None, 'tp'), may hold values from -0.125 to 0.125
- w_up: bfloat16 [32, 2048, 2048], P('sp', None, 'tp'), may hold values from -0.125 to 0.125
- w_down: bfloat16 [32, 2048, 2048], P('sp', 'tp'), may hold values from -0.125 to 0.125
- w_out: bfloat16 [2048, 2048], P(None, 'tp'), may hold values from -0.125 to 0.125
- queries: bfloat16 [8192, 1024], P('sp', 'tp'), may hold values from -6 to 6
- key_rows: bfloat16 [8192, 1024], P('sp', 'tp'), may hold values from -6 to 6
- value_rows: bfloat16 [8192, 2048], P('sp', 'tp'), may hold values from -6 to 6
- log_decay: float32 [8192, 1024], P('sp', 'tp'), may hold values from -1 to 0
Outputs:
- grad_gate: bfloat16 [32, 2048, 2048], P('sp', None, 'tp')
- grad_up: bfloat16 [32, 2048, 2048], P('sp', None, 'tp')
- grad_down: bfloat16 [32, 2048, 2048], P('sp', 'tp')
- grad_proj: float32 [2048, 2048], P('sp', 'tp')
- grad_queries: bfloat16 [8192, 1024], P('sp', 'tp')
- grad_keys: bfloat16 [8192, 1024], P('sp', 'tp')
- grad_values: bfloat16 [8192, 2048], P('sp', 'tp')
- grad_decay: float32 [8192, 1024], P('sp', 'tp')
The draws below stay inside these ranges and needn't reach their ends.
Inputs may be any that keep to these rules, and one draw needn't show every extreme that they name: `routes`: A token's experts differ. Within each aligned block of 256 tokens no expert is named more than 20 times, and in some block one expert is named exactly 20 times.
All inputs are finite; a program needn't handle non-finite values.
Results may differ from the reference program's by a relative error of at most 0.025.
Values may be sent and summed in bfloat16 or wider, within the bound.
No kernel may reach another device: no remote copies, remote signals or barrier semaphores. Data moves between devices by JAX's collectives and lax.ppermute only.
A program may use at most 64 MiB of HBM per device.

```python
import math
import jax
import jax.numpy as jnp
import numpy as np
from jax import lax

D = 2048
HEAD_COUNT = 32
KEY_CHANNELS = 32
VAL_DIM = 64
EXP_HIDDEN = 2048
TOP = 2
BLOCK = 64
TOK_DEV = 256
TOKEN_COUNT = 8192
EXPERTS = 32
CAP = 20
HID_DEV = 128
N_SP = 32
N_TP = 16


def draw_log_decay(key, part):
    sequence_lanes = jax.random.split(jax.random.fold_in(key, 17), 5)
    lagging_head = jax.random.uniform(sequence_lanes[0], (HEAD_COUNT,), jnp.float32) < 0.5
    base_rate = jnp.where(lagging_head, 0.5 / TOKEN_COUNT, 1.0 / 40.0)
    spans = TOKEN_COUNT // TOK_DEV
    span_scale = jnp.exp(jax.random.uniform(sequence_lanes[1], (spans,), jnp.float32, -0.7, 0.7))
    position_scale = jnp.repeat(span_scale, TOK_DEV)
    wobble = jnp.exp(jax.random.uniform(sequence_lanes[2], (TOKEN_COUNT, HEAD_COUNT, KEY_CHANNELS), jnp.float32, -1.0, 1.0))
    smoothed_decay = -(position_scale[:, None, None] * base_rate[None, :, None] * wobble)
    spike_position = jax.random.randint(sequence_lanes[3], (2,), 0, TOKEN_COUNT)
    spike_length = jnp.log(jax.random.uniform(sequence_lanes[4], (2,), jnp.float32, 0.5, 0.8))
    spike_rows = jnp.sum(jnp.where(jnp.arange(TOKEN_COUNT)[:, None] == spike_position[None, :], spike_length[None, :], 0.0), axis=1)
    spike_addend = spike_rows[:, None, None] * lagging_head[None, :, None].astype(jnp.float32)
    return (smoothed_decay + spike_addend).reshape(TOKEN_COUNT, HEAD_COUNT * KEY_CHANNELS)


def raised(entries, key, source, target, parts, factor):
    owner, partner = [(jnp.arange(entries.shape[axis_at]) // (entries.shape[axis_at] // parts)).reshape([-1 if axis == axis_at else 1 for axis in range(entries.ndim)]) for axis_at in (source, target)]
    chosen = jax.random.permutation(key, parts)[partner]
    strong = (owner == chosen) | (owner == (partner + parts // 2) % parts)
    return jnp.where(strong, factor * entries, entries)


def shard_levels(rng, shape, shards, low, top_value):
    gain, own = 1.0, jax.random.fold_in(rng, 6)
    for dim, blocks in shards:
        heights = jnp.exp(jax.random.uniform(jax.random.fold_in(own, dim), (blocks,), jnp.float32, low / len(shards), top_value / len(shards)))
        gain = gain * jnp.repeat(heights, shape[dim] // blocks).reshape([-1 if axis == dim else 1 for axis in range(len(shape))])
    return gain


def shared_out(own_key, own, number, rows, amount, top, reach, lean):
    ranking = jax.random.permutation(own_key, amount)
    crowded, ordinary = shares(amount, rows * top, reach, lean, True), shares(amount, rows * top, reach, lean, False)
    places = jnp.arange(amount)

    def named(tallies, rotation):
        used = int((tallies > 0).sum())
        fixed = max(1, used // 4)
        passed = fixed + (places - fixed + rotation * (used - fixed)) % max(1, amount - fixed)
        return jnp.zeros((amount,), jnp.int32).at[ranking[jnp.where(places < fixed, places, passed)]].set(jnp.asarray(tallies, jnp.int32))

    tallies = jnp.where(number % 4 == 0, named(crowded, number // 4), named(ordinary, number - number // 4 - 1))
    mixed = jax.random.permutation(jax.random.fold_in(own, 3), amount)
    giver, taker = mixed[0:amount // 2 * 2:2], mixed[1:amount // 2 * 2:2]
    room = jnp.minimum(tallies[giver] - 1, reach - tallies[taker]) // 2
    room = jnp.where((giver == ranking[0]) | (taker == ranking[0]) | (tallies[taker] == 0), 0, jnp.maximum(room, 0))
    passed = jax.random.randint(jax.random.fold_in(own, 4), (amount // 2,), 0, 1 << 20) % (room + 1)
    tallies = tallies.at[giver].add(-passed).at[taker].add(passed)
    labels = jnp.searchsorted(jnp.cumsum(tallies), jnp.arange(rows * top), side="right").astype(jnp.int32)
    table = labels.reshape(top, rows).T
    table = table[jax.random.permutation(jax.random.fold_in(own, 1), rows)]
    rotation = jax.random.randint(jax.random.fold_in(own, 2), (rows, 1), 0, top)
    return jnp.take_along_axis(table, (jnp.arange(top)[None, :] + rotation) % top, axis=1)


def shares(count, total, limit, skew, full):
    weights = [(1 << 20) // math.isqrt(rank ** skew) + 1 for rank in range(1, count + 1)]
    largest = limit if full else min(limit, max(-(-total // count), total * weights[0] // sum(weights)))
    least = 1 if total - largest >= count - 1 else 0
    given, spare = [largest] + [least] * (count - 1), total - largest - least * (count - 1)
    while spare > 0:
        candidates = [i for i in range(1, count) if given[i] < largest] or [i for i in range(1, count) if given[i] < limit]
        pool, left = sum([weights[i] for i in candidates]), spare
        for i in candidates:
            addition = min(limit - given[i], max(1, left * weights[i] // pool), spare)
            given[i] = given[i] + addition
            spare = spare - addition
    return np.array(given)


def gaussian(key, shape, spread, limit, cuts=(), kind=jnp.bfloat16):
    entries = spread * jax.random.normal(key, shape, jnp.float32)
    if cuts:
        entries = entries * shard_levels(key, shape, cuts, -0.22, 0.18)
    return jnp.clip(entries, -limit, limit).astype(kind)


def bell_draw_with(key, dims, width, limit, cuts, heavy, held_as=jnp.bfloat16):
    entries = width * jax.random.normal(key, dims, jnp.float32)
    if cuts:
        entries = entries * shard_levels(key, dims, cuts, -0.22, 0.18)
    return jnp.clip(raised(entries, jax.random.fold_in(key, 3), *heavy), -limit, limit).astype(held_as)


def setup_inputs(seed: int = 0) -> dict:
    splits = jax.random.split(jax.random.key(seed), 13)
    moe_input = gaussian(splits[0], (TOKEN_COUNT, D), 1.0, 6.0, ((0, 32), (1, 16)))
    out_grad = bell_draw_with(splits[1], (TOKEN_COUNT, D), 1.0, 12.0, ((0, 32), (1, 16)), (0, 1, 32, 2.75))
    routes_keys = jax.random.split(jax.random.fold_in(splits[2], 1), TOKEN_COUNT // TOK_DEV)
    routes_turns = jax.random.permutation(jax.random.fold_in(splits[2], 3), TOKEN_COUNT // TOK_DEV)
    routes = jax.vmap(lambda own, number: shared_out(jax.random.fold_in(splits[2], 2), own, number, TOK_DEV, EXPERTS, TOP, CAP, 2))(routes_keys, routes_turns).reshape((TOKEN_COUNT, TOP))
    route_weight = jnp.clip(0.2 + 1.3 * jax.random.uniform(splits[3], (TOKEN_COUNT, TOP), jnp.float32) ** shard_levels(splits[3], (TOKEN_COUNT, TOP), ((0, 32),), -0.2, 0.2), 0.2, 1.5)
    w_gate = gaussian(splits[4], (EXPERTS, D, EXP_HIDDEN), D ** -0.5, 0.125, ((0, 32), (2, 16)))
    w_up = gaussian(splits[5], (EXPERTS, D, EXP_HIDDEN), D ** -0.5, 0.125, ((0, 32), (2, 16)))
    w_down = gaussian(splits[6], (EXPERTS, EXP_HIDDEN, D), EXP_HIDDEN ** -0.5, 0.125, ((0, 32), (1, 16)))
    w_out = gaussian(splits[7], (D, HEAD_COUNT * VAL_DIM), (HEAD_COUNT * VAL_DIM) ** -0.5, 0.125, ((1, 16),))
    queries = gaussian(splits[8], (TOKEN_COUNT, HEAD_COUNT * KEY_CHANNELS), 1.0, 6.0, ((0, 32), (1, 16)))
    key_rows = gaussian(splits[9], (TOKEN_COUNT, HEAD_COUNT * KEY_CHANNELS), 1.0, 6.0, ((0, 32), (1, 16)))
    value_rows = gaussian(splits[10], (TOKEN_COUNT, HEAD_COUNT * VAL_DIM), 1.0, 6.0, ((0, 32), (1, 16)))
    log_decay = draw_log_decay(jax.random.fold_in(splits[12], 71), 0)
    return {"moe_input": moe_input, "out_grad": out_grad, "routes": routes, "route_weight": route_weight, "w_gate": w_gate, "w_up": w_up, "w_down": w_down, "w_out": w_out, "queries": queries, "key_rows": key_rows, "value_rows": value_rows, "log_decay": log_decay}


PRECISE = lax.Precision.HIGHEST

def mixer_pass(queries, key_rows, value_rows, log_decay, state_in):
    length = queries.shape[0]
    blocks = length // BLOCK
    nheads = state_in.shape[0]
    query_blocks = queries.reshape(blocks, BLOCK, nheads, KEY_CHANNELS)
    key_blocks = key_rows.reshape(blocks, BLOCK, nheads, KEY_CHANNELS) * KEY_CHANNELS ** (-0.5)
    value_blocks = value_rows.reshape(blocks, BLOCK, nheads, VAL_DIM)
    decays = log_decay.reshape(blocks, BLOCK, nheads, KEY_CHANNELS)
    cumulative = jnp.cumsum(decays, axis=1)
    closing = cumulative[:, -1]
    query_scaled = query_blocks * jnp.exp(cumulative)
    key_scaled = key_blocks * jnp.exp(-cumulative)
    causal = jnp.tril(jnp.ones((BLOCK, BLOCK), jnp.float32))
    scores = jnp.einsum('nthd,nshd->nhts', query_scaled, key_scaled, precision=PRECISE) * causal
    within = jnp.einsum('nhts,nshv->nthv', scores, value_blocks, precision=PRECISE)
    key_tail = key_blocks * jnp.exp(closing[:, None] - cumulative)
    additions = jnp.einsum('nshd,nshv->nhdv', key_tail, value_blocks, precision=PRECISE)

    def advance(state_now, pieces):
        return (jnp.exp(pieces[0])[..., None] * state_now + pieces[1], state_now)
    state_out, entering = lax.scan(advance, state_in, (closing, additions))
    carried = jnp.einsum('nthd,nhdv->nthv', query_scaled, entering, precision=PRECISE)
    return ((within + carried).reshape(length, nheads * VAL_DIM), lax.optimization_barrier(jnp.sum(closing, axis=0)), state_out)

def reference(moe_input, out_grad, routes, route_weight, w_gate, w_up, w_down, w_out, queries, key_rows, value_rows, log_decay):
    pair_count = TOKEN_COUNT * TOP
    weighted = (route_weight[:, :, None] * out_grad[:, None, :].astype(jnp.float32)).astype(jnp.bfloat16)
    grad_pad = jnp.concatenate([weighted.reshape(pair_count, D), jnp.zeros((1, D), jnp.bfloat16)], axis=0)
    input_pad = jnp.concatenate([jnp.repeat(moe_input, TOP, axis=0), jnp.zeros((1, D), jnp.bfloat16)], axis=0)
    flat_routes = routes.reshape(N_SP, TOK_DEV * TOP)
    onehot = (flat_routes[:, :, None] == jnp.arange(EXPERTS, dtype=jnp.int32)[None, None, :]).astype(jnp.int32)
    position = lax.optimization_barrier(jnp.sum((jnp.cumsum(onehot, axis=1) - onehot) * onehot, axis=2))
    slot_index = (jnp.arange(N_SP, dtype=jnp.int32)[:, None] * CAP + position).reshape(pair_count)
    slot_table = jnp.full((EXPERTS, N_SP * CAP), pair_count, jnp.int32)
    slot_table = slot_table.at[routes.reshape(pair_count), slot_index].set(jnp.arange(pair_count, dtype=jnp.int32))

    def one_expert(pieces):
        row_index, gate_weight, up_weight, down_weight = pieces
        rows_in = input_pad[row_index]
        rows_grad = grad_pad[row_index]
        gate_pre = jnp.dot(rows_in, gate_weight, preferred_element_type=jnp.float32)
        up_pre = jnp.dot(rows_in, up_weight, preferred_element_type=jnp.float32)
        sigmoid_gate = jax.nn.sigmoid(gate_pre)
        activated = gate_pre * sigmoid_gate
        hidden = (activated * up_pre).astype(jnp.bfloat16)
        hidden_grad = lax.dot_general(rows_grad, down_weight, (((1,), (1,)), ((), ())), preferred_element_type=jnp.float32)
        down_part = lax.dot_general(hidden, rows_grad, (((0,), (0,)), ((), ())), preferred_element_type=jnp.float32).astype(jnp.bfloat16)
        gate_grad = (hidden_grad * up_pre * sigmoid_gate * (1.0 + gate_pre * (1.0 - sigmoid_gate))).astype(jnp.bfloat16)
        up_grad = (hidden_grad * activated).astype(jnp.bfloat16)
        gate_part = lax.dot_general(rows_in, gate_grad, (((0,), (0,)), ((), ())), preferred_element_type=jnp.float32).astype(jnp.bfloat16)
        up_part = lax.dot_general(rows_in, up_grad, (((0,), (0,)), ((), ())), preferred_element_type=jnp.float32).astype(jnp.bfloat16)
        row_total = gate_grad.shape[0]
        gate_split = gate_grad.astype(jnp.float32).reshape(row_total, N_TP, HID_DEV)
        up_split = up_grad.astype(jnp.float32).reshape(row_total, N_TP, HID_DEV)
        gate_wsplit = gate_weight.astype(jnp.float32).reshape(D, N_TP, HID_DEV)
        up_wsplit = up_weight.astype(jnp.float32).reshape(D, N_TP, HID_DEV)
        partial_value = jnp.einsum('rgf,dgf->grd', gate_split, gate_wsplit, precision=PRECISE)
        partial_value = partial_value + jnp.einsum('rgf,dgf->grd', up_split, up_wsplit, precision=PRECISE)
        rounded = lax.optimization_barrier(partial_value.astype(jnp.bfloat16))
        row_grad = lax.optimization_barrier(jnp.sum(rounded.astype(jnp.float32), axis=0))
        return (gate_part, up_part, down_part, row_grad.astype(jnp.bfloat16))
    grad_gate, grad_up, grad_down, returned = lax.map(one_expert, (slot_table, w_gate, w_up, w_down))
    pair_back = jnp.zeros((pair_count + 1, D), jnp.float32)
    pair_back = pair_back.at[slot_table.reshape(-1)].set(returned.reshape(-1, D).astype(jnp.float32))
    routed = lax.optimization_barrier(jnp.sum(pair_back[:pair_count].reshape(TOKEN_COUNT, TOP, D), axis=1))
    residual_grad = (out_grad.astype(jnp.float32) + routed).astype(jnp.bfloat16)
    zero_state = jnp.zeros((HEAD_COUNT, KEY_CHANNELS, VAL_DIM), jnp.float32)

    def mixer_only(query_full, key_full, value_full, decay_full):
        return mixer_pass(query_full, key_full, value_full, decay_full, zero_state)[0]
    mixer_raw, pull_back = jax.vjp(mixer_only, queries.astype(jnp.float32), key_rows.astype(jnp.float32), value_rows.astype(jnp.float32), log_decay)
    mixer_out = mixer_raw.astype(jnp.bfloat16)
    grad_proj = lax.dot_general(residual_grad, mixer_out, (((0,), (0,)), ((), ())), preferred_element_type=jnp.float32)
    mixer_grad = jnp.dot(residual_grad, w_out, preferred_element_type=jnp.float32)
    query_grad, key_grad, value_grad, decay_grad = pull_back(mixer_grad)
    return (grad_gate, grad_up, grad_down, grad_proj, query_grad.astype(jnp.bfloat16), key_grad.astype(jnp.bfloat16), value_grad.astype(jnp.bfloat16), decay_grad)
```

```python
import jax
import jax.numpy as jnp
from jax import lax
from jax.experimental import pallas as pl
from jax.experimental.pallas import tpu as pltpu
from jax.sharding import Mesh
from jax.sharding import PartitionSpec as P

KEY_CHANNELS = 32
VAL_DIM = 64
TOP = 2
BLOCK = 64
CAP = 20
PAD = 24
SP = ("sp_0", "sp_1")
N_SP = 32
N_TP = 16
TOK = 256
ROWS = N_SP * CAP
SLOTS = N_SP * PAD
NBLK = TOK // BLOCK
BF = jnp.bfloat16
F32 = jnp.float32
HI = lax.Precision.HIGHEST
SCALE = KEY_CHANNELS ** (-0.5)

NN = (((1,), (0,)), ((), ()))
NT = (((1,), (1,)), ((), ()))
TN = (((0,), (0,)), ((), ()))


def mm(a, b, dims=NN):
    return lax.dot_general(a.astype(BF), b.astype(BF), dims, preferred_element_type=F32)


def mm_exact(a, b, dims=NN):
    return lax.dot_general(a, b, dims, precision=HI, preferred_element_type=F32)


def iota(shape, dim):
    return lax.broadcasted_iota(jnp.int32, shape, dim)


def call(fn, outs, *args, name, scratch=(), smem=()):
    return pl.pallas_call(
        fn,
        out_shape=tuple(jax.ShapeDtypeStruct(s, d) for s, d in outs),
        in_specs=[
            pl.BlockSpec(memory_space=pltpu.SMEM if k in smem else pltpu.VMEM)
            for k in range(len(args))
        ],
        out_specs=tuple(pl.BlockSpec(memory_space=pltpu.VMEM) for _ in outs),
        scratch_shapes=scratch,
        name=name,
        compiler_params=pltpu.CompilerParams(vmem_limit_bytes=56 * 1024 * 1024),
    )(*args)


def dispatch_kernel(routes_ref, weight_ref, x_ref, g_ref, sx_ref, sg_ref, pick_ref):
    routes = routes_ref[...]
    expert = iota((N_SP, TOK), 0)
    hot = [(expert == routes[j : j + 1, :]) for j in range(TOP)]
    both = (hot[0] | hot[1]).astype(F32)
    before = (iota((TOK, TOK), 0) < iota((TOK, TOK), 1)).astype(F32)
    place = mm(both, before)
    spread = (iota((SLOTS, N_SP), 0) // PAD == iota((SLOTS, N_SP), 1)).astype(F32)
    slot_place = (iota((SLOTS, TOK), 0) % PAD).astype(F32)
    picks = [(mm(spread, jnp.where(h, place, -1.0)) == slot_place).astype(F32) for h in hot]
    pick = (picks[0] + picks[1]).astype(BF)
    pick_ref[...] = pick
    sx_ref[...] = mm(pick, x_ref[...]).astype(BF).reshape(N_SP, PAD, 128)
    grad = g_ref[...].astype(F32)
    weight = jnp.concatenate([weight_ref[...], jnp.zeros((6, TOK), F32)], axis=0).T
    rows = [(weight[:, j : j + 1] * grad).astype(BF) for j in range(TOP)]
    sent = mm(picks[0], rows[0]) + mm(picks[1], rows[1])
    sg_ref[...] = sent.astype(BF).reshape(N_SP, PAD, 128)


def turned_kernel(pick_ref, out_ref):
    out_ref[...] = pick_ref[...].astype(F32).T.astype(BF)


def copies_kernel(rows_ref, out_ref, packed):
    for e in range(N_SP):
        packed[e * CAP : (e + 1) * CAP, :] = rows_ref[e].astype(F32)[:CAP]
    out = packed[...].astype(BF)
    for k in range(N_TP):
        out_ref[k] = out


STEP = 128


def wide(ref, at, size):
    return jnp.concatenate([ref[k, at : at + size, :] for k in range(N_TP)], axis=1)


def pre_kernel(x_ref, wg_ref, wu_ref, pre_ref):
    weight = jnp.concatenate([wg_ref[...], wu_ref[...]], axis=1)
    for at in range(0, ROWS, STEP):
        pre_ref[at : at + STEP, :] = mm(wide(x_ref, at, STEP), weight)


def partial_kernel(g_ref, pre_ref, wg_ref, wu_ref, wd_ref, part_ref, grads_ref, hidden_ref):
    weight = jnp.concatenate([wg_ref[...], wu_ref[...]], axis=1)
    down = wd_ref[...]
    for at in range(0, ROWS, STEP):
        here = slice(at, at + STEP)
        hidden_grad = mm(wide(g_ref, at, STEP), down, NT)
        gate_pre, up_pre = pre_ref[here, :128], pre_ref[here, 128:]
        sigmoid = jax.nn.sigmoid(gate_pre)
        activated = gate_pre * sigmoid
        hidden_ref[here, :] = (activated * up_pre).astype(BF)
        gate = hidden_grad * up_pre * sigmoid * (1.0 + gate_pre * (1.0 - sigmoid))
        up = hidden_grad * activated
        grads = jnp.concatenate([gate.astype(BF), up.astype(BF)], axis=1)
        grads_ref[here, :] = grads
        part = mm(grads, weight, NT).astype(BF)
        for k in range(N_TP):
            part_ref[k, here, :] = part[:, k * 128 : (k + 1) * 128]


def weight_grads_kernel(x_ref, g_ref, grads_ref, hidden_ref, gate_ref, up_ref, down_ref):
    grads = grads_ref[...]
    hidden = hidden_ref[...]
    for k in range(N_TP):
        both = mm(x_ref[k], grads, TN)
        gate_ref[k * 128 : (k + 1) * 128, :] = both[:, :128].astype(BF)
        up_ref[k * 128 : (k + 1) * 128, :] = both[:, 128:].astype(BF)
        down_ref[:, k * 128 : (k + 1) * 128] = mm(hidden, g_ref[k], TN).astype(BF)


def row_sum_kernel(part_ref, out_ref, total):
    acc = part_ref[0].astype(F32)
    for k in range(1, N_TP):
        acc = acc + part_ref[k].astype(F32)
    total[:ROWS, :] = acc
    total[ROWS:, :] = jnp.zeros((8, 128), F32)
    keep = iota((PAD, 128), 0) < CAP
    for e in range(N_SP):
        out_ref[e] = jnp.where(keep, total[e * CAP : e * CAP + PAD, :], 0.0).astype(BF)


def residual_kernel(back_ref, turned_ref, g_ref, out_ref):
    routed = mm(turned_ref[...], back_ref[...].reshape(SLOTS, 128))
    residual = (g_ref[...].astype(F32) + routed).astype(BF)
    for k in range(N_TP):
        out_ref[k] = residual


def head_masks():
    key_lane = iota((1, 64), 1) // KEY_CHANNELS
    val_lane = iota((1, 128), 1) // VAL_DIM
    keys = [(key_lane == h).astype(F32) for h in range(2)]
    vals = [(val_lane == h).astype(F32) for h in range(2)]
    own = (iota((128, 64), 0) // VAL_DIM == iota((128, 64), 1) // KEY_CHANNELS).astype(F32)
    return keys, vals, own


def packed_state(state):
    both = state[:64] + state[64:]
    return jnp.concatenate([both[:32], both[32:]], axis=1)


def opened_state(packed, own):
    both = jnp.concatenate([packed[:, :64], packed[:, 64:]], axis=0)
    return jnp.concatenate([both, both], axis=0) * own


def block_sums(decay):
    row, col = iota((TOK, TOK), 0), iota((TOK, TOK), 1)
    within = ((row // BLOCK == col // BLOCK) & (col <= row)).astype(F32)
    return mm_exact(within, decay)


def whole_sums(cumulative):
    offset, parts = jnp.zeros((1, 64), F32), []
    for n in range(NBLK):
        block = cumulative[n * BLOCK : (n + 1) * BLOCK]
        parts.append(block + offset)
        offset = offset + block[BLOCK - 1 :]
    return jnp.concatenate(parts, axis=0), offset


def closings(cumulative):
    return [cumulative[(n + 1) * BLOCK - 1 : (n + 1) * BLOCK] for n in range(NBLK)]


def per_block(rows):
    return jnp.concatenate([jnp.broadcast_to(r, (BLOCK, r.shape[1])) for r in rows], axis=0)


def span_kernel(k_ref, v_ref, decay_ref, out_ref):
    _, _, own = head_masks()
    keys = k_ref[...].astype(F32).T * SCALE
    so_far, total = whole_sums(block_sums(decay_ref[...].T))
    state = mm(v_ref[...], keys * jnp.exp(total - so_far), TN) * own
    last = jnp.concatenate([total, jnp.zeros((1, 64), F32)], axis=1)
    rows = jnp.concatenate([packed_state(state), last, jnp.zeros((7, 128), F32)], axis=0)
    for s in range(N_SP):
        out_ref[s] = rows


def scores_of(queries, keys, mask, causal):
    return jnp.where(causal, mm(queries * mask, keys, NT), 0.0)


def causal_blocks():
    row, col = iota((TOK, TOK), 0), iota((TOK, TOK), 1)
    return (row // BLOCK == col // BLOCK) & (col <= row)


def forward_kernel(
    me_ref, spans_ref, q_ref, k_ref, v_ref, decay_ref, out_ref, entering_ref, reach_ref
):
    key_mask, val_mask, own = head_masks()
    me = me_ref[0]
    totals = jnp.concatenate([spans_ref[s, 32:33, :] for s in range(N_SP)], axis=0)[:, :64]
    start, between = iota((N_SP, N_SP), 0), iota((N_SP, N_SP), 1)
    passed = ((start < between) & (between < me)).astype(F32)
    reach = jnp.where(iota((N_SP, 64), 0) < me, jnp.exp(mm_exact(passed, totals)), 0.0)
    reach = jnp.concatenate([reach, reach], axis=1)
    reach_ref[...] = reach
    packed = jnp.zeros((32, 128), F32)
    for s in range(N_SP):
        packed = packed + reach[s : s + 1] * spans_ref[s, :32, :]
    state = opened_state(packed, own)
    queries = q_ref[...].astype(F32).T
    keys = k_ref[...].astype(F32).T * SCALE
    values = v_ref[...].astype(F32)
    cumulative = block_sums(decay_ref[...].T)
    closing = closings(cumulative)
    scaled_q = queries * jnp.exp(cumulative)
    scaled_k = keys * jnp.exp(-cumulative)
    tail = keys * jnp.exp(per_block(closing) - cumulative)
    causal = causal_blocks()
    within = jnp.zeros((TOK, 128), F32)
    for h in range(2):
        scores = scores_of(scaled_q, scaled_k, key_mask[h], causal)
        within = within + mm(scores, values * val_mask[h])
    for n in range(NBLK):
        here = slice(n * BLOCK, (n + 1) * BLOCK)
        entering_ref[n] = state
        out_ref[here, :] = (within[here] + mm(scaled_q[here], state, NT)).astype(BF)
        state = jnp.exp(closing[n]) * state + mm(values[here], tail[here], TN) * own


def mixer_grad_kernel(full_ref, w_ref, q_ref, decay_ref, reach_ref, grad_ref, sent_ref):
    _, _, own = head_masks()
    grad = mm(wide(full_ref, 0, TOK), w_ref[...])
    grad_ref[...] = grad
    so_far, _ = whole_sums(block_sums(decay_ref[...].T))
    scaled = q_ref[...].astype(F32).T * jnp.exp(so_far)
    packed = packed_state(mm(grad, scaled, TN) * own)
    for s in range(N_SP):
        sent_ref[s] = (packed * reach_ref[s : s + 1, :]).astype(BF)


def proj_kernel(full_ref, mixed_ref, out_ref):
    mixed = mixed_ref[...]
    for k in range(N_TP):
        part = mm(full_ref[k], mixed, TN).astype(BF)
        out_ref[2 * k] = part[:64]
        out_ref[2 * k + 1] = part[64:]


def backward_kernel(
    later_ref, grad_ref, entering_ref, q_ref, k_ref, v_ref, decay_ref, gq_ref, gk_ref, gv_ref, gd_ref
):
    key_mask, val_mask, own = head_masks()
    packed = later_ref[0].astype(F32)
    for s in range(1, N_SP):
        packed = packed + later_ref[s].astype(F32)
    state_grad = opened_state(packed, own)
    grad = grad_ref[...]
    queries = q_ref[...].astype(F32).T
    keys = k_ref[...].astype(F32).T * SCALE
    values = v_ref[...].astype(F32)
    cumulative = block_sums(decay_ref[...].T)
    closing = closings(cumulative)
    grow, shrink = jnp.exp(cumulative), jnp.exp(-cumulative)
    rest = jnp.exp(per_block(closing) - cumulative)
    scaled_q, scaled_k, tail = queries * grow, keys * shrink, keys * rest
    causal = causal_blocks()
    value_grad = jnp.zeros((TOK, 128), F32)
    query_grad = jnp.zeros((TOK, 64), F32)
    key_grad = jnp.zeros((TOK, 64), F32)
    for h in range(2):
        scores = scores_of(scaled_q, scaled_k, key_mask[h], causal)
        score_grad = jnp.where(causal, mm(grad * val_mask[h], values, NT), 0.0)
        value_grad = value_grad + mm(scores, grad * val_mask[h], TN)
        query_grad = query_grad + mm(score_grad, scaled_k * key_mask[h])
        key_grad = key_grad + mm(score_grad, scaled_q * key_mask[h], TN)
    carried_v, carried_q, tail_grad, close_grad = ([None] * NBLK for _ in range(4))
    for n in reversed(range(NBLK)):
        here = slice(n * BLOCK, (n + 1) * BLOCK)
        entering = entering_ref[n]
        decay_out = jnp.exp(closing[n])
        carried_v[n] = mm(tail[here], state_grad, NT)
        carried_q[n] = mm(grad[here], entering)
        tail_grad[n] = mm(values[here], state_grad)
        close_grad[n] = decay_out * jnp.sum(state_grad * entering, axis=0, keepdims=True) + jnp.sum(
            tail_grad[n] * tail[here], axis=0, keepdims=True
        )
        state_grad = decay_out * state_grad + mm(grad[here], scaled_q[here], TN) * own
    value_grad = value_grad + jnp.concatenate(carried_v, axis=0)
    query_grad = query_grad + jnp.concatenate(carried_q, axis=0)
    tail_grad = jnp.concatenate(tail_grad, axis=0)
    change = query_grad * scaled_q - key_grad * scaled_k - tail_grad * tail
    row, col = iota((TOK, TOK), 0), iota((TOK, TOK), 1)
    onward = ((row // BLOCK == col // BLOCK) & (col >= row)).astype(F32)
    gd_ref[...] = (mm_exact(onward, change) + per_block(close_grad)).T
    gq_ref[...] = (query_grad * grow).T.astype(BF)
    gk_ref[...] = ((key_grad * shrink + tail_grad * rest) * SCALE).T.astype(BF)
    gv_ref[...] = value_grad.astype(BF)


def proj_sum_kernel(parts_ref, out_ref):
    acc = parts_ref[0].astype(F32)
    for s in range(1, N_SP):
        acc = acc + parts_ref[s].astype(F32)
    out_ref[...] = acc


def exchanged(blocks, axis):
    return lax.all_to_all(blocks, axis, split_axis=0, concat_axis=0, tiled=True)


def body(
    moe_input,
    out_grad,
    routes,
    route_weight,
    w_gate,
    w_up,
    w_down,
    w_out,
    queries,
    key_rows,
    value_rows,
    log_decay,
):
    gate_weight, up_weight, down_weight = w_gate[0], w_up[0], w_down[0]
    q_t, k_t, decay_t = queries.T, key_rows.T, log_decay.T
    me = lax.axis_index(SP).astype(jnp.int32).reshape(1)

    send_in, send_grad, pick = call(
        dispatch_kernel,
        [((N_SP, PAD, 128), BF), ((N_SP, PAD, 128), BF), ((SLOTS, TOK), BF)],
        routes.T,
        route_weight.T,
        moe_input,
        out_grad,
        name="dispatch",
    )
    recv_in = exchanged(send_in, SP)
    recv_grad = exchanged(send_grad, SP)
    (turned,) = call(turned_kernel, [((TOK, SLOTS), BF)], pick, name="turned")
    (spans,) = call(
        span_kernel, [((N_SP, 40, 128), F32)], k_t, value_rows, decay_t, name="span"
    )

    def copies(rows):
        return call(
            copies_kernel,
            [((N_TP, ROWS, 128), BF)],
            rows,
            name="copies",
            scratch=[pltpu.VMEM((ROWS, 128), F32)],
        )[0]

    rows_in = exchanged(copies(recv_in), "tp")
    rows_grad = exchanged(copies(recv_grad), "tp")
    spans = exchanged(spans, SP)
    mixer_out, entering, reach = call(
        forward_kernel,
        [((TOK, 128), BF), ((NBLK, 128, 64), F32), ((N_SP, 128), F32)],
        me,
        spans,
        q_t,
        k_t,
        value_rows,
        decay_t,
        name="forward",
        smem=(0,),
    )
    (pre,) = call(
        pre_kernel, [((ROWS, 256), F32)], rows_in, gate_weight, up_weight, name="pre"
    )
    partial_rows, grads, hidden = call(
        partial_kernel,
        [((N_TP, ROWS, 128), BF), ((ROWS, 256), BF), ((ROWS, 128), BF)],
        rows_grad,
        pre,
        gate_weight,
        up_weight,
        down_weight,
        name="partial",
    )
    arrived = exchanged(partial_rows, "tp")
    gate_part, up_part, down_part = call(
        weight_grads_kernel,
        [((2048, 128), BF), ((2048, 128), BF), ((128, 2048), BF)],
        rows_in,
        rows_grad,
        grads,
        hidden,
        name="weight_grads",
    )
    (returned,) = call(
        row_sum_kernel,
        [((N_SP, PAD, 128), BF)],
        arrived,
        name="row_sum",
        scratch=[pltpu.VMEM((ROWS + 8, 128), F32)],
    )
    back = exchanged(returned, SP)
    (residual,) = call(
        residual_kernel, [((N_TP, TOK, 128), BF)], back, turned, out_grad, name="residual"
    )
    full_grad = exchanged(residual, "tp")
    mixer_grad, state_sent = call(
        mixer_grad_kernel,
        [((TOK, 128), F32), ((N_SP, 32, 128), BF)],
        full_grad,
        w_out,
        q_t,
        decay_t,
        reach,
        name="mixer_grad",
    )
    later = exchanged(state_sent, SP)
    (proj,) = call(proj_kernel, [((N_SP, 64, 128), BF)], full_grad, mixer_out, name="proj")
    proj_parts = exchanged(proj, SP)
    gq, gk, gv, gd = call(
        backward_kernel,
        [((64, TOK), BF), ((64, TOK), BF), ((TOK, 128), BF), ((64, TOK), F32)],
        later,
        mixer_grad,
        entering,
        q_t,
        k_t,
        value_rows,
        decay_t,
        name="backward",
    )
    (grad_proj,) = call(proj_sum_kernel, [((64, 128), F32)], proj_parts, name="proj_sum")
    return (gate_part[None], up_part[None], down_part[None], grad_proj, gq.T, gk.T, gv, gd.T)


def solution(mesh):
    split = Mesh(mesh.devices.reshape(16, 2, mesh.shape["tp"]), ("sp_0", "sp_1", "tp"))
    placed = (
        P(SP, "tp"),
        P(SP, "tp"),
        P(SP, None),
        P(SP, None),
        P(SP, None, "tp"),
        P(SP, None, "tp"),
        P(SP, "tp", None),
        P(None, "tp"),
        P(SP, "tp"),
        P(SP, "tp"),
        P(SP, "tp"),
        P(SP, "tp"),
    )
    return jax.shard_map(
        body,
        mesh=split,
        in_specs=placed,
        out_specs=(
            P(SP, None, "tp"),
            P(SP, None, "tp"),
            P(SP, "tp", None),
            P(SP, "tp"),
            P(SP, "tp"),
            P(SP, "tp"),
            P(SP, "tp"),
            P(SP, "tp"),
        ),
        check_vma=False,
    )
```

```python
import jax
import jax.numpy as jnp
from jax import lax
from jax.experimental import pallas as pl
from jax.experimental.pallas import tpu as pltpu
from jax.sharding import Mesh
from jax.sharding import PartitionSpec as P

KEY_CHANNELS = 32
VAL_DIM = 64
TOP = 2
BLOCK = 64
CAP = 20
PAD = 24
SP = ("sp_0", "sp_1")
N_SP = 32
N_TP = 16
TOK = 256
ROWS = N_SP * CAP
SLOTS = N_SP * PAD
HALF = ROWS // 2
NBLK = TOK // BLOCK
BF = jnp.bfloat16
F32 = jnp.float32
HI = lax.Precision.HIGHEST
SCALE = KEY_CHANNELS ** (-0.5)

NN = (((1,), (0,)), ((), ()))
NT = (((1,), (1,)), ((), ()))
TN = (((0,), (0,)), ((), ()))


def mm(a, b, dims=NN):
    return lax.dot_general(a.astype(BF), b.astype(BF), dims, preferred_element_type=F32)


def mm_exact(a, b, dims=NN):
    return lax.dot_general(a, b, dims, precision=HI, preferred_element_type=F32)


def iota(shape, dim):
    return lax.broadcasted_iota(jnp.int32, shape, dim)


def call(fn, outs, *args, name, scratch=(), smem=(), near=(), near_out=(), after=()):
    spaces = [pltpu.VMEM if k in near else pltpu.HBM for k in range(len(args))]
    args = [
        a if k in smem else pltpu.with_memory_space_constraint(a, spaces[k])
        for k, a in enumerate(args)
    ]
    after = [pltpu.with_memory_space_constraint(a, pltpu.HBM) for a in after]
    count = len(args)

    def run(*refs):
        fn(*refs[:count], *refs[count + len(after) :])

    return pl.pallas_call(
        run,
        out_shape=tuple(
            (pltpu.VMEM if k in near_out else pltpu.HBM)(s, d) for k, (s, d) in enumerate(outs)
        ),
        in_specs=[
            pl.BlockSpec(memory_space=pltpu.SMEM if k in smem else pltpu.VMEM)
            for k in range(count)
        ]
        + [pl.BlockSpec(memory_space=pltpu.HBM) for _ in after],
        out_specs=tuple(pl.BlockSpec(memory_space=pltpu.VMEM) for _ in outs),
        scratch_shapes=scratch,
        name=name,
        compiler_params=pltpu.CompilerParams(vmem_limit_bytes=24 * 1024 * 1024),
    )(*args, *after)


def head_masks():
    key_lane = iota((1, 64), 1) // KEY_CHANNELS
    val_lane = iota((1, 128), 1) // VAL_DIM
    keys = [(key_lane == h).astype(F32) for h in range(2)]
    vals = [(val_lane == h).astype(F32) for h in range(2)]
    own = (iota((128, 64), 0) // VAL_DIM == iota((128, 64), 1) // KEY_CHANNELS).astype(F32)
    return keys, vals, own


def packed_state(state):
    both = state[:64] + state[64:]
    return jnp.concatenate([both[:32], both[32:]], axis=1)


def opened_state(packed, own):
    both = jnp.concatenate([packed[:, :64], packed[:, 64:]], axis=0)
    return jnp.concatenate([both, both], axis=0) * own


def block_sums(decay):
    row, col = iota((TOK, TOK), 0), iota((TOK, TOK), 1)
    within = ((row // BLOCK == col // BLOCK) & (col <= row)).astype(F32)
    return mm_exact(within, decay)


def whole_sums(cumulative):
    offset, parts = jnp.zeros((1, 64), F32), []
    for n in range(NBLK):
        block = cumulative[n * BLOCK : (n + 1) * BLOCK]
        parts.append(block + offset)
        offset = offset + block[BLOCK - 1 :]
    return jnp.concatenate(parts, axis=0), offset


def closings(cumulative):
    return [cumulative[(n + 1) * BLOCK - 1 : (n + 1) * BLOCK] for n in range(NBLK)]


def per_block(rows):
    return jnp.concatenate([jnp.broadcast_to(r, (BLOCK, r.shape[1])) for r in rows], axis=0)


def two_parts(values):
    high = values.astype(BF).astype(F32)
    return high, values - high


def dispatch_kernel(
    routes_ref, weight_ref, x_ref, g_ref, k_ref, v_ref, decay_ref, sent_ref, pick_ref
):
    routes = routes_ref[...]
    expert = iota((N_SP, TOK), 0)
    hot = [(expert == routes[j : j + 1, :]) for j in range(TOP)]
    both = (hot[0] | hot[1]).astype(F32)
    before = (iota((TOK, TOK), 0) < iota((TOK, TOK), 1)).astype(F32)
    place = mm(both, before)
    owner, row = iota((SLOTS, N_SP), 0) // PAD, iota((SLOTS, N_SP), 0) % PAD
    mine = owner == iota((SLOTS, N_SP), 1)
    spread = mine.astype(F32)
    slot_place = (iota((SLOTS, TOK), 0) % PAD).astype(F32)
    picks = [(mm(spread, jnp.where(h, place, -1.0)) == slot_place).astype(F32) for h in hot]
    pick = picks[0] + picks[1]
    pick_ref[...] = pick.astype(BF)

    _, _, own = head_masks()
    keys = k_ref[...].astype(F32).T * SCALE
    so_far, total = whole_sums(block_sums(decay_ref[...].T))
    state = mm(v_ref[...], keys * jnp.exp(total - so_far), TN) * own
    state_high, state_low = two_parts(packed_state(state))
    total_row = jnp.concatenate(two_parts(total), axis=1)

    first = (mine & (row == CAP)).astype(F32)
    second = (mine & (row == CAP + 1)).astype(F32)
    chosen = jnp.concatenate([pick, first, second], axis=1)
    rows = jnp.concatenate([x_ref[...].astype(F32), state_high, state_low], axis=0)
    sent_ref[:, :PAD, :] = mm(chosen, rows).astype(BF).reshape(N_SP, PAD, 128)

    grad = g_ref[...].astype(F32)
    weight = jnp.concatenate([weight_ref[...], jnp.zeros((6, TOK), F32)], axis=0).T
    rows = [(weight[:, j : j + 1] * grad).astype(BF) for j in range(TOP)]
    sent = mm(picks[0], rows[0]) + mm(picks[1], rows[1])
    sent = jnp.where(iota((SLOTS, 128), 0) % PAD == CAP, total_row, sent)
    sent_ref[:, PAD:, :] = sent.astype(BF).reshape(N_SP, PAD, 128)


def turned_kernel(pick_ref, out_ref):
    out_ref[...] = pick_ref[...].astype(F32).T.astype(BF)


def copies_kernel(place_ref, recv_ref, out_ref, states_ref, reach_ref, packed):
    for e in range(N_SP):
        block = recv_ref[e].astype(F32)
        at = e * CAP if e < N_SP // 2 else ROWS + (e - N_SP // 2) * CAP
        packed[at : at + CAP, :] = block[:CAP]
        packed[at + HALF : at + HALF + CAP, :] = block[PAD : PAD + CAP]
    for p in range(2):
        out = packed[p * ROWS : (p + 1) * ROWS, :].astype(BF)
        for k in range(p, N_TP, 2):
            out_ref[k] = out

    chip = place_ref[2]
    totals = [recv_ref[s, PAD + CAP : PAD + CAP + 1, :].astype(F32) for s in range(N_SP)]
    totals = jnp.concatenate(totals, axis=0)
    totals = totals[:, :64] + totals[:, 64:]
    double = jnp.concatenate([totals, totals], axis=1)
    decays = jnp.exp(double)
    state = jnp.zeros((1, 128), F32)
    for s in range(N_SP):
        states_ref[s : s + 1, :] = state
        pair = recv_ref[s, CAP : CAP + 2, :].astype(F32)
        state = decays[s : s + 1] * state + pair[0:1] + pair[1:2]
    target, between = iota((16, N_SP), 0), iota((16, N_SP), 1)
    passed = ((between >= 2 * target + 2) & (between < 2 * chip)).astype(F32)
    reach = jnp.exp(mm_exact(passed, double))
    reach_ref[:16, :] = jnp.where(iota((16, 128), 0) < chip, reach, 0.0)
    here = iota((N_SP, 128), 0)
    even = jnp.sum(jnp.where(here == 2 * chip, decays, 0.0), axis=0, keepdims=True)
    odd = jnp.sum(jnp.where(here == 2 * chip + 1, decays, 0.0), axis=0, keepdims=True)
    reach_ref[16:, :] = jnp.concatenate([even, odd, jnp.zeros((6, 128), F32)], axis=0)


def wide(ref, at, size):
    return jnp.concatenate([ref[k, at : at + size, :] for k in range(N_TP)], axis=1)


def partial_kernel(
    rows_ref, wg_ref, wu_ref, wd_ref, pg_ref, pu_ref, pd_ref, part_ref, grads_ref, hidden_ref
):
    weight = jnp.concatenate([wg_ref[...], wu_ref[...], pg_ref[...], pu_ref[...]], axis=1)
    down = jnp.concatenate([wd_ref[...], pd_ref[...]], axis=0)
    pre = mm(wide(rows_ref, 0, HALF), weight)
    hidden_grad = mm(wide(rows_ref, HALF, HALF), down, NT)
    grads = []
    for b in range(2):
        gate_pre, up_pre = pre[:, 256 * b : 256 * b + 128], pre[:, 256 * b + 128 : 256 * b + 256]
        upper = hidden_grad[:, 128 * b : 128 * b + 128]
        sigmoid = jax.nn.sigmoid(gate_pre)
        activated = gate_pre * sigmoid
        hidden_ref[:, 128 * b : 128 * b + 128] = (activated * up_pre).astype(BF)
        gate = upper * up_pre * sigmoid * (1.0 + gate_pre * (1.0 - sigmoid))
        grads += [gate.astype(BF), (upper * activated).astype(BF)]
    grads = jnp.concatenate(grads, axis=1)
    grads_ref[...] = grads
    for k in range(0, N_TP, 2):
        part = mm(grads, weight[k * 128 : (k + 2) * 128], NT).astype(BF)
        part_ref[k] = part[:, :128]
        part_ref[k + 1] = part[:, 128:]


def weight_grads_kernel(rows_ref, grads_ref, hidden_ref, own_ref, sent_ref):
    grads = grads_ref[...]
    hidden = hidden_ref[...]
    for k in range(0, N_TP, 2):
        x = jnp.concatenate([rows_ref[k, :HALF, :], rows_ref[k + 1, :HALF, :]], axis=1)
        g = jnp.concatenate([rows_ref[k, HALF:, :], rows_ref[k + 1, HALF:, :]], axis=1)
        both = mm(x, grads, TN)
        down = mm(hidden, g, TN)
        here = slice(k * 128, (k + 2) * 128)
        own_ref[0, here, :] = both[:, :128]
        own_ref[1, here, :] = both[:, 128:256]
        sent_ref[0, here, :] = both[:, 256:384].astype(BF)
        sent_ref[1, here, :] = both[:, 384:].astype(BF)
        for n in range(2):
            block = slice((k + n) * 128, (k + n + 1) * 128)
            own_ref[2, block, :] = down[:128, n * 128 : (n + 1) * 128]
            sent_ref[2, block, :] = down[128:, n * 128 : (n + 1) * 128].astype(BF)


def grad_sum_kernel(own_ref, recv_ref, gate_ref, up_ref, down_ref):
    gate_ref[...] = (own_ref[0] + recv_ref[0].astype(F32)).astype(BF)
    up_ref[...] = (own_ref[1] + recv_ref[1].astype(F32)).astype(BF)
    for k in range(N_TP):
        here = slice(k * 128, (k + 1) * 128)
        down_ref[:, here] = (own_ref[2, here, :] + recv_ref[2, here, :].astype(F32)).astype(BF)


def row_sum_kernel(part_ref, states_ref, out_ref, total):
    for p in range(2):
        acc = part_ref[p].astype(F32)
        for k in range(p + 2, N_TP, 2):
            acc = acc + part_ref[k].astype(F32)
        total[p * HALF : (p + 1) * HALF, :] = acc
    total[ROWS:, :] = jnp.zeros((8, 128), F32)
    row = iota((PAD, 128), 0)
    high, low = two_parts(states_ref[...])
    for e in range(N_SP):
        rows = jnp.where(row < CAP, total[e * CAP : e * CAP + PAD, :], 0.0)
        rows = jnp.where(row == CAP, high[e : e + 1], rows)
        rows = jnp.where(row == CAP + 1, low[e : e + 1], rows)
        out_ref[e] = rows.astype(BF)


def residual_kernel(back_ref, turned_ref, g_ref, out_ref):
    routed = mm(turned_ref[...], back_ref[...].reshape(SLOTS, 128))
    residual = (g_ref[...].astype(F32) + routed).astype(BF)
    for k in range(N_TP):
        out_ref[k] = residual


def scores_of(queries, keys, mask, causal):
    return jnp.where(causal, mm(queries * mask, keys, NT), 0.0)


def causal_blocks():
    row, col = iota((TOK, TOK), 0), iota((TOK, TOK), 1)
    return (row // BLOCK == col // BLOCK) & (col <= row)


def forward_kernel(back_ref, q_ref, k_ref, v_ref, decay_ref, out_ref, entering_ref):
    key_mask, val_mask, own = head_masks()
    rows = [back_ref[s, CAP : CAP + 2, :].astype(F32) for s in range(N_SP)]
    packed = jnp.concatenate([r[0:1] + r[1:2] for r in rows], axis=0)
    state = opened_state(packed, own)
    queries = q_ref[...].astype(F32).T
    keys = k_ref[...].astype(F32).T * SCALE
    values = v_ref[...].astype(F32)
    cumulative = block_sums(decay_ref[...].T)
    closing = closings(cumulative)
    scaled_q = queries * jnp.exp(cumulative)
    scaled_k = keys * jnp.exp(-cumulative)
    tail = keys * jnp.exp(per_block(closing) - cumulative)
    causal = causal_blocks()
    within = jnp.zeros((TOK, 128), F32)
    for h in range(2):
        scores = scores_of(scaled_q, scaled_k, key_mask[h], causal)
        within = within + mm(scores, values * val_mask[h])
    for n in range(NBLK):
        here = slice(n * BLOCK, (n + 1) * BLOCK)
        entering_ref[n] = state
        out_ref[here, :] = (within[here] + mm(scaled_q[here], state, NT)).astype(BF)
        state = jnp.exp(closing[n]) * state + mm(values[here], tail[here], TN) * own


def mixer_grad_kernel(
    place_ref, full_ref, w_ref, mixed_ref, q_ref, decay_ref, grad_ref, span_ref, sent_ref, kept_ref
):
    _, _, own = head_masks()
    grad = mm(wide(full_ref, 0, TOK), w_ref[...])
    grad_ref[...] = grad
    so_far, _ = whole_sums(block_sums(decay_ref[...].T))
    scaled = q_ref[...].astype(F32).T * jnp.exp(so_far)
    packed = packed_state(mm(grad, scaled, TN) * own)
    span_ref[...] = packed
    high, low = two_parts(packed)
    sent_ref[1024:1056, :] = high.astype(BF)
    sent_ref[1056:, :] = low.astype(BF)
    mixed = mixed_ref[...]
    first = place_ref[1] == 0
    for k in range(0, N_TP, 2):
        rows = jnp.concatenate([full_ref[k], full_ref[k + 1]], axis=1)
        part = mm(rows, mixed, TN)
        for n in range(2):
            low, high = part[n * 128 : n * 128 + 64], part[n * 128 + 64 : n * 128 + 128]
            here = slice((k + n) * 64, (k + n + 1) * 64)
            kept_ref[here, :] = jnp.where(first, low, high)
            sent_ref[here, :] = jnp.where(first, high, low).astype(BF)


def chip_kernel(place_ref, recv_ref, kept_ref, span_ref, reach_ref, sent_ref, other_ref):
    other = recv_ref[1024:1056, :].astype(F32) + recv_ref[1056:, :].astype(F32)
    other_ref[...] = other
    first = place_ref[1] == 0
    mine = span_ref[...]
    both = jnp.where(first, mine, other) + reach_ref[16:17, :] * jnp.where(first, other, mine)
    for z in range(16):
        here = slice(z * 64, (z + 1) * 64)
        sent_ref[z, :32, :] = (both * reach_ref[z : z + 1, :]).astype(BF)
        sent_ref[z, 32:, :] = (kept_ref[here, :] + recv_ref[here, :].astype(F32)).astype(BF)


def backward_kernel(
    place_ref,
    later_ref,
    other_ref,
    reach_ref,
    grad_ref,
    entering_ref,
    q_ref,
    k_ref,
    v_ref,
    decay_ref,
    gp_ref,
    gq_ref,
    gk_ref,
    gv_ref,
    gd_ref,
):
    key_mask, val_mask, own = head_masks()
    sums = later_ref[0].astype(F32)
    for z in range(1, 16):
        sums = sums + later_ref[z].astype(F32)
    gp_ref[...] = sums[32:]
    packed = sums[:32]
    packed = jnp.where(place_ref[1] == 0, reach_ref[17:18, :] * packed + other_ref[...], packed)
    state_grad = opened_state(packed, own)
    grad = grad_ref[...]
    queries = q_ref[...].astype(F32).T
    keys = k_ref[...].astype(F32).T * SCALE
    values = v_ref[...].astype(F32)
    cumulative = block_sums(decay_ref[...].T)
    closing = closings(cumulative)
    grow, shrink = jnp.exp(cumulative), jnp.exp(-cumulative)
    rest = jnp.exp(per_block(closing) - cumulative)
    scaled_q, scaled_k, tail = queries * grow, keys * shrink, keys * rest
    causal = causal_blocks()
    value_grad = jnp.zeros((TOK, 128), F32)
    query_grad = jnp.zeros((TOK, 64), F32)
    key_grad = jnp.zeros((TOK, 64), F32)
    for h in range(2):
        scores = scores_of(scaled_q, scaled_k, key_mask[h], causal)
        score_grad = jnp.where(causal, mm(grad * val_mask[h], values, NT), 0.0)
        value_grad = value_grad + mm(scores, grad * val_mask[h], TN)
        query_grad = query_grad + mm(score_grad, scaled_k * key_mask[h])
        key_grad = key_grad + mm(score_grad, scaled_q * key_mask[h], TN)
    carried_v, carried_q, tail_grad, close_grad = ([None] * NBLK for _ in range(4))
    for n in reversed(range(NBLK)):
        here = slice(n * BLOCK, (n + 1) * BLOCK)
        entering = entering_ref[n]
        decay_out = jnp.exp(closing[n])
        carried_v[n] = mm(tail[here], state_grad, NT)
        carried_q[n] = mm(grad[here], entering)
        tail_grad[n] = mm(values[here], state_grad)
        close_grad[n] = decay_out * jnp.sum(state_grad * entering, axis=0, keepdims=True) + jnp.sum(
            tail_grad[n] * tail[here], axis=0, keepdims=True
        )
        state_grad = decay_out * state_grad + mm(grad[here], scaled_q[here], TN) * own
    value_grad = value_grad + jnp.concatenate(carried_v, axis=0)
    query_grad = query_grad + jnp.concatenate(carried_q, axis=0)
    tail_grad = jnp.concatenate(tail_grad, axis=0)
    change = query_grad * scaled_q - key_grad * scaled_k - tail_grad * tail
    row, col = iota((TOK, TOK), 0), iota((TOK, TOK), 1)
    onward = ((row // BLOCK == col // BLOCK) & (col >= row)).astype(F32)
    gd_ref[...] = (mm_exact(onward, change) + per_block(close_grad)).T
    gq_ref[...] = (query_grad * grow).T.astype(BF)
    gk_ref[...] = ((key_grad * shrink + tail_grad * rest) * SCALE).T.astype(BF)
    gv_ref[...] = value_grad.astype(BF)


def exchanged(blocks, axis):
    return lax.all_to_all(blocks, axis, split_axis=0, concat_axis=0, tiled=True)


PARTNERS = [(k, k ^ 1) for k in range(N_TP)]


def body(
    moe_input,
    out_grad,
    routes,
    route_weight,
    w_gate,
    w_up,
    w_down,
    w_out,
    queries,
    key_rows,
    value_rows,
    log_decay,
):
    weights = (w_gate[0], w_up[0], w_down[0])
    with jax.named_scope("partner_weights"):
        partner_weights = tuple(lax.ppermute(w, "tp", PARTNERS) for w in weights)
    q_t, k_t, decay_t = queries.T, key_rows.T, log_decay.T
    place = jnp.stack(
        [lax.axis_index(SP), lax.axis_index("sp_1"), lax.axis_index("sp_0")]
    ).astype(jnp.int32)

    sent, pick = call(
        dispatch_kernel,
        [((N_SP, 2 * PAD, 128), BF), ((SLOTS, TOK), BF)],
        routes.T,
        route_weight.T,
        moe_input,
        out_grad,
        k_t,
        value_rows,
        decay_t,
        name="dispatch",
    )
    recv = exchanged(sent, SP)
    (turned,) = call(turned_kernel, [((TOK, SLOTS), BF)], pick, name="turned")
    copies, states, reach = call(
        copies_kernel,
        [((N_TP, ROWS, 128), BF), ((N_SP, 128), F32), ((24, 128), F32)],
        place,
        recv,
        name="copies",
        scratch=[pltpu.VMEM((2 * ROWS, 128), F32)],
        smem=(0,),
        near=(1,),
        near_out=(0,),
        after=partner_weights,
    )
    rows = exchanged(copies, "tp")
    partial_rows, grads, hidden = call(
        partial_kernel,
        [((N_TP, HALF, 128), BF), ((HALF, 512), BF), ((HALF, 256), BF)],
        rows,
        *weights,
        *partner_weights,
        name="partial",
        near=(0,),
        near_out=(0,),
    )
    arrived = exchanged(partial_rows, "tp")
    (returned,) = call(
        row_sum_kernel,
        [((N_SP, PAD, 128), BF)],
        arrived,
        states,
        name="row_sum",
        near=(0,),
        scratch=[pltpu.VMEM((ROWS + 8, 128), F32)],
    )
    own_grads, sent_grads = call(
        weight_grads_kernel,
        [((3, 2048, 128), F32), ((3, 2048, 128), BF)],
        rows,
        grads,
        hidden,
        name="weight_grads",
        near=(0,),
        after=(returned,),
    )
    with jax.named_scope("partner_grads"):
        partner_grads = lax.ppermute(sent_grads, "tp", PARTNERS)
    back = exchanged(returned, SP)
    (residual,) = call(
        residual_kernel,
        [((N_TP, TOK, 128), BF)],
        back,
        turned,
        out_grad,
        name="residual",
        near=(0,),
        after=(own_grads,),
    )
    full_grad = exchanged(residual, "tp")
    mixer_out, entering = call(
        forward_kernel,
        [((TOK, 128), BF), ((NBLK, 128, 64), F32)],
        back,
        q_t,
        k_t,
        value_rows,
        decay_t,
        name="forward",
        near=(0,),
        after=(residual,),
    )
    mixer_grad, span_grad, to_other, kept = call(
        mixer_grad_kernel,
        [((TOK, 128), F32), ((32, 128), F32), ((1088, 128), BF), ((1024, 128), F32)],
        place,
        full_grad,
        w_out,
        mixer_out,
        q_t,
        decay_t,
        name="mixer_grad",
        smem=(0,),
        near=(1,),
        near_out=(2, 3),
    )
    with jax.named_scope("cores"):
        from_other = lax.ppermute(to_other, "sp_1", [(0, 1), (1, 0)])
    chip_sent, other_grad = call(
        chip_kernel,
        [((16, 96, 128), BF), ((32, 128), F32)],
        place,
        from_other,
        kept,
        span_grad,
        reach,
        name="chip",
        smem=(0,),
        near=(1, 2),
    )
    later = exchanged(chip_sent, "sp_0")
    grad_proj, gq, gk, gv, gd = call(
        backward_kernel,
        [((64, 128), F32), ((64, TOK), BF), ((64, TOK), BF), ((TOK, 128), BF), ((64, TOK), F32)],
        place,
        later,
        other_grad,
        reach,
        mixer_grad,
        entering,
        q_t,
        k_t,
        value_rows,
        decay_t,
        name="backward",
        smem=(0,),
        near=(1,),
    )
    gate_part, up_part, down_part = call(
        grad_sum_kernel,
        [((2048, 128), BF), ((2048, 128), BF), ((128, 2048), BF)],
        own_grads,
        partner_grads,
        name="grad_sum",
    )
    return (gate_part[None], up_part[None], down_part[None], grad_proj, gq.T, gk.T, gv, gd.T)


def solution(mesh):
    split = Mesh(mesh.devices.reshape(16, 2, mesh.shape["tp"]), ("sp_0", "sp_1", "tp"))
    placed = (
        P(SP, "tp"),
        P(SP, "tp"),
        P(SP, None),
        P(SP, None),
        P(SP, None, "tp"),
        P(SP, None, "tp"),
        P(SP, "tp", None),
        P(None, "tp"),
        P(SP, "tp"),
        P(SP, "tp"),
        P(SP, "tp"),
        P(SP, "tp"),
    )
    return jax.shard_map(
        body,
        mesh=split,
        in_specs=placed,
        out_specs=(
            P(SP, None, "tp"),
            P(SP, None, "tp"),
            P(SP, "tp", None),
            P(SP, "tp"),
            P(SP, "tp"),
            P(SP, "tp"),
            P(SP, "tp"),
            P(SP, "tp"),
        ),
        check_vma=False,
    )
```

```python
import jax
import jax.numpy as jnp
from jax import lax
from jax.experimental import pallas as pl
from jax.experimental.pallas import tpu as pltpu
from jax.sharding import Mesh
from jax.sharding import PartitionSpec as P


KEY_CHANNELS = 32
VAL_DIM = 64
TOP = 2
BLOCK = 64
CAP = 20
PAD = 24
SP = ("sp_0", "sp_1")
N_SP = 32
N_TP = 16
TOK = 256
ROWS = N_SP * CAP
SLOTS = N_SP * PAD
PART = ROWS // 4
WEIGHT_ROWS = 3 * 2048
NBLK = TOK // BLOCK
BF = jnp.bfloat16
F32 = jnp.float32
HI = lax.Precision.HIGHEST
SCALE = KEY_CHANNELS ** (-0.5)

NN = (((1,), (0,)), ((), ()))
NT = (((1,), (1,)), ((), ()))
TN = (((0,), (0,)), ((), ()))


def mm(a, b, dims=NN):
    return lax.dot_general(a.astype(BF), b.astype(BF), dims, preferred_element_type=F32)


def mm_exact(a, b, dims=NN):
    return lax.dot_general(a, b, dims, precision=HI, preferred_element_type=F32)


def iota(shape, dim):
    return lax.broadcasted_iota(jnp.int32, shape, dim)


def call(fn, outs, *args, scratch=(), smem=(), near=(), near_out=(), after=()):
    spaces = [pltpu.VMEM if k in near else pltpu.HBM for k in range(len(args))]
    args = [
        a if k in smem else pltpu.with_memory_space_constraint(a, spaces[k])
        for k, a in enumerate(args)
    ]
    after = [pltpu.with_memory_space_constraint(a, pltpu.HBM) for a in after]
    count = len(args)

    def run(*refs):
        fn(*refs[:count], *refs[count + len(after) :])

    return pl.pallas_call(
        run,
        out_shape=tuple(
            (pltpu.VMEM if k in near_out else pltpu.HBM)(s, d) for k, (s, d) in enumerate(outs)
        ),
        in_specs=[
            pl.BlockSpec(memory_space=pltpu.SMEM if k in smem else pltpu.VMEM)
            for k in range(count)
        ]
        + [pl.BlockSpec(memory_space=pltpu.HBM) for _ in after],
        out_specs=tuple(pl.BlockSpec(memory_space=pltpu.VMEM) for _ in outs),
        scratch_shapes=scratch,
        compiler_params=pltpu.CompilerParams(vmem_limit_bytes=24 * 1024 * 1024),
    )(*args, *after)


def head_masks():
    key_lane = iota((1, 64), 1) // KEY_CHANNELS
    val_lane = iota((1, 128), 1) // VAL_DIM
    keys = [(key_lane == h).astype(F32) for h in range(2)]
    vals = [(val_lane == h).astype(F32) for h in range(2)]
    own = (iota((128, 64), 0) // VAL_DIM == iota((128, 64), 1) // KEY_CHANNELS).astype(F32)
    return keys, vals, own


def packed_state(state):
    both = state[:64] + state[64:]
    return jnp.concatenate([both[:32], both[32:]], axis=1)


def opened_state(packed, own):
    both = jnp.concatenate([packed[:, :64], packed[:, 64:]], axis=0)
    return jnp.concatenate([both, both], axis=0) * own


def block_sums(decay):
    row, col = iota((TOK, TOK), 0), iota((TOK, TOK), 1)
    within = ((row // BLOCK == col // BLOCK) & (col <= row)).astype(F32)
    return mm_exact(within, decay)


def whole_sums(cumulative):
    offset, parts = jnp.zeros((1, 64), F32), []
    for n in range(NBLK):
        block = cumulative[n * BLOCK : (n + 1) * BLOCK]
        parts.append(block + offset)
        offset = offset + block[BLOCK - 1 :]
    return jnp.concatenate(parts, axis=0), offset


def closings(cumulative):
    return [cumulative[(n + 1) * BLOCK - 1 : (n + 1) * BLOCK] for n in range(NBLK)]


def per_block(rows):
    return jnp.concatenate([jnp.broadcast_to(r, (BLOCK, r.shape[1])) for r in rows], axis=0)


def two_parts(values):
    high = values.astype(BF).astype(F32)
    return high, values - high


def dispatch_kernel(
    routes_ref, weight_ref, x_ref, g_ref, k_ref, v_ref, decay_ref, sent_ref, pick_ref
):
    routes = routes_ref[...]
    expert = iota((N_SP, TOK), 0)
    hot = [(expert == routes[j : j + 1, :]) for j in range(TOP)]
    both = (hot[0] | hot[1]).astype(F32)
    before = (iota((TOK, TOK), 0) < iota((TOK, TOK), 1)).astype(F32)
    place = mm(both, before)
    owner, row = iota((SLOTS, N_SP), 0) // PAD, iota((SLOTS, N_SP), 0) % PAD
    mine = owner == iota((SLOTS, N_SP), 1)
    spread = mine.astype(F32)
    slot_place = (iota((SLOTS, TOK), 0) % PAD).astype(F32)
    picks = [(mm(spread, jnp.where(h, place, -1.0)) == slot_place).astype(F32) for h in hot]
    pick = picks[0] + picks[1]
    pick_ref[...] = pick.astype(BF)

    _, _, own = head_masks()
    keys = k_ref[...].astype(F32).T * SCALE
    so_far, total = whole_sums(block_sums(decay_ref[...].T))
    state = mm(v_ref[...], keys * jnp.exp(total - so_far), TN) * own
    state_high, state_low = two_parts(packed_state(state))
    total_row = jnp.concatenate(two_parts(total), axis=1)

    first = (mine & (row == CAP)).astype(F32)
    second = (mine & (row == CAP + 1)).astype(F32)
    chosen = jnp.concatenate([pick, first, second], axis=1)
    rows = jnp.concatenate([x_ref[...].astype(F32), state_high, state_low], axis=0)
    sent_ref[:, :PAD, :] = mm(chosen, rows).astype(BF).reshape(N_SP, PAD, 128)

    grad = g_ref[...].astype(F32)
    weight = jnp.concatenate([weight_ref[...], jnp.zeros((6, TOK), F32)], axis=0).T
    rows = [(weight[:, j : j + 1] * grad).astype(BF) for j in range(TOP)]
    sent = mm(picks[0], rows[0]) + mm(picks[1], rows[1])
    sent = jnp.where(iota((SLOTS, 128), 0) % PAD == CAP, total_row, sent)
    sent_ref[:, PAD:, :] = sent.astype(BF).reshape(N_SP, PAD, 128)


def turned_kernel(pick_ref, out_ref):
    out_ref[...] = pick_ref[...].astype(F32).T.astype(BF)


def quarter_of(place_ref, k):
    return jnp.where(place_ref[1] == 0, k % 4, k // 4)


def copies_kernel(place_ref, recv_ref, out_ref, states_ref, reach_ref, packed, rounded):
    for e in range(N_SP):
        block = recv_ref[e].astype(F32)
        at = (e // 8) * 2 * PART + (e % 8) * CAP
        packed[at : at + CAP, :] = block[:CAP]
        packed[at + PART : at + PART + CAP, :] = block[PAD : PAD + CAP]
    for q in range(4):
        rounded[q] = packed[q * 2 * PART : (q + 1) * 2 * PART, :].astype(BF)
    for k in range(N_TP):
        out_ref[k] = rounded[quarter_of(place_ref, k)]
    chip = place_ref[2]
    totals = [recv_ref[s, PAD + CAP : PAD + CAP + 1, :].astype(F32) for s in range(N_SP)]
    totals = jnp.concatenate(totals, axis=0)
    totals = totals[:, :64] + totals[:, 64:]
    double = jnp.concatenate([totals, totals], axis=1)
    decays = jnp.exp(double)
    state = jnp.zeros((1, 128), F32)
    for s in range(N_SP):
        states_ref[s : s + 1, :] = state
        pair = recv_ref[s, CAP : CAP + 2, :].astype(F32)
        state = decays[s : s + 1] * state + pair[0:1] + pair[1:2]
    target, between = iota((16, N_SP), 0), iota((16, N_SP), 1)
    passed = ((between >= 2 * target + 2) & (between < 2 * chip)).astype(F32)
    reach = jnp.exp(mm_exact(passed, double))
    reach_ref[:16, :] = jnp.where(iota((16, 128), 0) < chip, reach, 0.0)
    here = iota((N_SP, 128), 0)
    even = jnp.sum(jnp.where(here == 2 * chip, decays, 0.0), axis=0, keepdims=True)
    odd = jnp.sum(jnp.where(here == 2 * chip + 1, decays, 0.0), axis=0, keepdims=True)
    reach_ref[16:, :] = jnp.concatenate([even, odd, jnp.zeros((6, 128), F32)], axis=0)


def pack_kernel(wg_ref, wu_ref, wd_ref, out_ref):
    out_ref[:2048, :] = wg_ref[...]
    out_ref[2048:4096, :] = wu_ref[...]
    for k in range(N_TP):
        at = 4096 + k * 128
        out_ref[at : at + 128, :] = wd_ref[:, k * 128 : (k + 1) * 128]


def wide(ref, at, size):
    return jnp.concatenate([ref[k, at : at + size, :] for k in range(N_TP)], axis=1)


def partial_kernel(
    rows_ref, own_ref, left_ref, right_ref, far_a_ref, far_b_ref, part_ref, grads_ref, hidden_ref
):
    gates, downs = [], []
    for ref in (own_ref, left_ref, right_ref):
        gates += [ref[:2048, :], ref[2048:4096, :]]
        downs.append([ref[4096 + k * 128 : 4224 + k * 128, :] for k in range(N_TP)])
    gates += [far_a_ref[:2048, :], jnp.concatenate([far_a_ref[2048:, :], far_b_ref[:1024, :]], axis=0)]
    downs.append([far_b_ref[1024 + k * 128 : 1152 + k * 128, :] for k in range(N_TP)])
    weight = jnp.concatenate(gates, axis=1)
    down = jnp.concatenate([jnp.concatenate(d, axis=1) for d in downs], axis=0)
    pre = mm(wide(rows_ref, 0, PART), weight)
    hidden_grad = mm(wide(rows_ref, PART, PART), down, NT)
    grads = []
    for b in range(4):
        gate_pre, up_pre = pre[:, 256 * b : 256 * b + 128], pre[:, 256 * b + 128 : 256 * b + 256]
        upper = hidden_grad[:, 128 * b : 128 * b + 128]
        sigmoid = jax.nn.sigmoid(gate_pre)
        activated = gate_pre * sigmoid
        hidden_ref[:, 128 * b : 128 * b + 128] = (activated * up_pre).astype(BF)
        gate = upper * up_pre * sigmoid * (1.0 + gate_pre * (1.0 - sigmoid))
        grads += [gate.astype(BF), (upper * activated).astype(BF)]
    grads = jnp.concatenate(grads, axis=1)
    grads_ref[...] = grads
    for k in range(0, N_TP, 2):
        part = mm(grads, weight[k * 128 : (k + 2) * 128], NT).astype(BF)
        part_ref[k] = part[:, :128]
        part_ref[k + 1] = part[:, 128:]


def weight_grads_kernel(rows_ref, grads_ref, hidden_ref, *out_refs):
    grads = grads_ref[...]
    hidden = hidden_ref[...]
    for k in range(0, N_TP, 2):
        x = jnp.concatenate([rows_ref[k, :PART, :], rows_ref[k + 1, :PART, :]], axis=1)
        g = jnp.concatenate([rows_ref[k, PART:, :], rows_ref[k + 1, PART:, :]], axis=1)
        both = mm(x, grads, TN)
        down = mm(hidden, g, TN)
        at = k * 128
        for b, ref in enumerate(out_refs):
            kind = ref.dtype
            ref[at : at + 256, :] = both[:, 256 * b : 256 * b + 128].astype(kind)
            ref[2048 + at : 2304 + at, :] = both[:, 256 * b + 128 : 256 * b + 256].astype(kind)
            for n in range(2):
                block = 4096 + at + n * 128
                ref[block : block + 128, :] = down[
                    128 * b : 128 * b + 128, n * 128 : (n + 1) * 128
                ].astype(kind)


def grad_sum_kernel(own_ref, a_ref, b_ref, c_ref, gate_ref, up_ref, down_ref):
    def total(at, size):
        parts = [r[at : at + size, :].astype(F32) for r in (a_ref, b_ref, c_ref)]
        return (own_ref[at : at + size, :] + parts[0] + parts[1] + parts[2]).astype(BF)

    for k in range(N_TP):
        here = slice(k * 128, (k + 1) * 128)
        gate_ref[here, :] = total(k * 128, 128)
        up_ref[here, :] = total(2048 + k * 128, 128)
        down_ref[:, here] = total(4096 + k * 128, 128)


def row_sum_kernel(place_ref, part_ref, states_ref, out_ref, total):
    for q in range(4):
        acc = jnp.zeros((PART, 128), F32)
        for j in range(4):
            source = jnp.where(place_ref[1] == 0, 4 * j + q, 4 * q + j)
            acc = acc + part_ref[source].astype(F32)
        total[q * PART : (q + 1) * PART, :] = acc
    total[ROWS:, :] = jnp.zeros((8, 128), F32)
    row = iota((PAD, 128), 0)
    high, low = two_parts(states_ref[...])
    for e in range(N_SP):
        rows = jnp.where(row < CAP, total[e * CAP : e * CAP + PAD, :], 0.0)
        rows = jnp.where(row == CAP, high[e : e + 1], rows)
        rows = jnp.where(row == CAP + 1, low[e : e + 1], rows)
        out_ref[e] = rows.astype(BF)


def residual_kernel(back_ref, turned_ref, g_ref, out_ref):
    routed = mm(turned_ref[...], back_ref[...].reshape(SLOTS, 128))
    residual = (g_ref[...].astype(F32) + routed).astype(BF)
    for k in range(N_TP):
        out_ref[k] = residual


def scores_of(queries, keys, mask, causal):
    return jnp.where(causal, mm(queries * mask, keys, NT), 0.0)


def causal_blocks():
    row, col = iota((TOK, TOK), 0), iota((TOK, TOK), 1)
    return (row // BLOCK == col // BLOCK) & (col <= row)


def forward_kernel(back_ref, q_ref, k_ref, v_ref, decay_ref, out_ref, entering_ref):
    key_mask, val_mask, own = head_masks()
    rows = [back_ref[s, CAP : CAP + 2, :].astype(F32) for s in range(N_SP)]
    packed = jnp.concatenate([r[0:1] + r[1:2] for r in rows], axis=0)
    state = opened_state(packed, own)
    queries = q_ref[...].astype(F32).T
    keys = k_ref[...].astype(F32).T * SCALE
    values = v_ref[...].astype(F32)
    cumulative = block_sums(decay_ref[...].T)
    closing = closings(cumulative)
    scaled_q = queries * jnp.exp(cumulative)
    scaled_k = keys * jnp.exp(-cumulative)
    tail = keys * jnp.exp(per_block(closing) - cumulative)
    causal = causal_blocks()
    within = jnp.zeros((TOK, 128), F32)
    for h in range(2):
        scores = scores_of(scaled_q, scaled_k, key_mask[h], causal)
        within = within + mm(scores, values * val_mask[h])
    for n in range(NBLK):
        here = slice(n * BLOCK, (n + 1) * BLOCK)
        entering_ref[n] = state
        out_ref[here, :] = (within[here] + mm(scaled_q[here], state, NT)).astype(BF)
        state = jnp.exp(closing[n]) * state + mm(values[here], tail[here], TN) * own


def mixer_grad_kernel(
    place_ref, full_ref, w_ref, mixed_ref, q_ref, decay_ref, grad_ref, span_ref, sent_ref, kept_ref
):
    _, _, own = head_masks()
    grad = mm(wide(full_ref, 0, TOK), w_ref[...])
    grad_ref[...] = grad
    so_far, _ = whole_sums(block_sums(decay_ref[...].T))
    scaled = q_ref[...].astype(F32).T * jnp.exp(so_far)
    packed = packed_state(mm(grad, scaled, TN) * own)
    span_ref[...] = packed
    high, low = two_parts(packed)
    sent_ref[1024:1056, :] = high.astype(BF)
    sent_ref[1056:, :] = low.astype(BF)
    mixed = mixed_ref[...]
    first = place_ref[1] == 0
    for k in range(0, N_TP, 2):
        rows = jnp.concatenate([full_ref[k], full_ref[k + 1]], axis=1)
        part = mm(rows, mixed, TN)
        for n in range(2):
            low, high = part[n * 128 : n * 128 + 64], part[n * 128 + 64 : n * 128 + 128]
            here = slice((k + n) * 64, (k + n + 1) * 64)
            kept_ref[here, :] = jnp.where(first, low, high)
            sent_ref[here, :] = jnp.where(first, high, low).astype(BF)


def chip_kernel(place_ref, recv_ref, kept_ref, span_ref, reach_ref, sent_ref, other_ref):
    other = recv_ref[1024:1056, :].astype(F32) + recv_ref[1056:, :].astype(F32)
    other_ref[...] = other
    first = place_ref[1] == 0
    mine = span_ref[...]
    both = jnp.where(first, mine, other) + reach_ref[16:17, :] * jnp.where(first, other, mine)
    for z in range(16):
        here = slice(z * 64, (z + 1) * 64)
        sent_ref[z, :32, :] = (both * reach_ref[z : z + 1, :]).astype(BF)
        sent_ref[z, 32:, :] = (kept_ref[here, :] + recv_ref[here, :].astype(F32)).astype(BF)


def backward_kernel(
    place_ref,
    later_ref,
    other_ref,
    reach_ref,
    grad_ref,
    entering_ref,
    q_ref,
    k_ref,
    v_ref,
    decay_ref,
    gp_ref,
    gq_ref,
    gk_ref,
    gv_ref,
    gd_ref,
):
    key_mask, val_mask, own = head_masks()
    sums = later_ref[0].astype(F32)
    for z in range(1, 16):
        sums = sums + later_ref[z].astype(F32)
    gp_ref[...] = sums[32:]
    packed = sums[:32]
    packed = jnp.where(place_ref[1] == 0, reach_ref[17:18, :] * packed + other_ref[...], packed)
    state_grad = opened_state(packed, own)
    grad = grad_ref[...]
    queries = q_ref[...].astype(F32).T
    keys = k_ref[...].astype(F32).T * SCALE
    values = v_ref[...].astype(F32)
    cumulative = block_sums(decay_ref[...].T)
    closing = closings(cumulative)
    grow, shrink = jnp.exp(cumulative), jnp.exp(-cumulative)
    rest = jnp.exp(per_block(closing) - cumulative)
    scaled_q, scaled_k, tail = queries * grow, keys * shrink, keys * rest
    causal = causal_blocks()
    value_grad = jnp.zeros((TOK, 128), F32)
    query_grad = jnp.zeros((TOK, 64), F32)
    key_grad = jnp.zeros((TOK, 64), F32)
    for h in range(2):
        scores = scores_of(scaled_q, scaled_k, key_mask[h], causal)
        score_grad = jnp.where(causal, mm(grad * val_mask[h], values, NT), 0.0)
        value_grad = value_grad + mm(scores, grad * val_mask[h], TN)
        query_grad = query_grad + mm(score_grad, scaled_k * key_mask[h])
        key_grad = key_grad + mm(score_grad, scaled_q * key_mask[h], TN)
    carried_v, carried_q, tail_grad, close_grad = ([None] * NBLK for _ in range(4))
    for n in reversed(range(NBLK)):
        here = slice(n * BLOCK, (n + 1) * BLOCK)
        entering = entering_ref[n]
        decay_out = jnp.exp(closing[n])
        carried_v[n] = mm(tail[here], state_grad, NT)
        carried_q[n] = mm(grad[here], entering)
        tail_grad[n] = mm(values[here], state_grad)
        close_grad[n] = decay_out * jnp.sum(state_grad * entering, axis=0, keepdims=True) + jnp.sum(
            tail_grad[n] * tail[here], axis=0, keepdims=True
        )
        state_grad = decay_out * state_grad + mm(grad[here], scaled_q[here], TN) * own
    value_grad = value_grad + jnp.concatenate(carried_v, axis=0)
    query_grad = query_grad + jnp.concatenate(carried_q, axis=0)
    tail_grad = jnp.concatenate(tail_grad, axis=0)
    change = query_grad * scaled_q - key_grad * scaled_k - tail_grad * tail
    row, col = iota((TOK, TOK), 0), iota((TOK, TOK), 1)
    onward = ((row // BLOCK == col // BLOCK) & (col >= row)).astype(F32)
    gd_ref[...] = (mm_exact(onward, change) + per_block(close_grad)).T
    gq_ref[...] = (query_grad * grow).T.astype(BF)
    gk_ref[...] = ((key_grad * shrink + tail_grad * rest) * SCALE).T.astype(BF)
    gv_ref[...] = value_grad.astype(BF)


def exchanged(blocks, axis):
    return lax.all_to_all(blocks, axis, split_axis=0, concat_axis=0, tiled=True)


def ring_step(step):
    pairs = []
    for t in range(N_TP):
        y, x = t // 4, t % 4
        pairs.append((t, 4 * y + (x + step) % 4))
        pairs.append((N_TP + t, N_TP + 4 * ((y + step) % 4) + x))
    return pairs


def passed_on(array, step):
    return lax.ppermute(array, ("sp_1", "tp"), ring_step(step))


def body(
    moe_input,
    out_grad,
    routes,
    route_weight,
    w_gate,
    w_up,
    w_down,
    w_out,
    queries,
    key_rows,
    value_rows,
    log_decay,
):
    q_t, k_t, decay_t = queries.T, key_rows.T, log_decay.T
    place = jnp.stack(
        [lax.axis_index(SP), lax.axis_index("sp_1"), lax.axis_index("sp_0")]
    ).astype(jnp.int32)

    sent, pick = call(
        dispatch_kernel,
        [((N_SP, 2 * PAD, 128), BF), ((SLOTS, TOK), BF)],
        routes.T,
        route_weight.T,
        moe_input,
        out_grad,
        k_t,
        value_rows,
        decay_t,
    )
    recv = exchanged(sent, SP)
    (packed,) = call(pack_kernel, [((WEIGHT_ROWS, 128), BF)], w_gate[0], w_up[0], w_down[0])
    left = passed_on(packed, 1)
    right = passed_on(packed, -1)
    far_a = passed_on(left[: WEIGHT_ROWS // 2], 1)
    far_b = passed_on(right[WEIGHT_ROWS // 2 :], -1)
    weights = (packed, left, right, far_a, far_b)
    (turned,) = call(turned_kernel, [((TOK, SLOTS), BF)], pick)
    copies, states, reach = call(
        copies_kernel,
        [((N_TP, 2 * PART, 128), BF), ((N_SP, 128), F32), ((24, 128), F32)],
        place,
        recv,
        scratch=[pltpu.VMEM((2 * ROWS, 128), F32), pltpu.VMEM((4, 2 * PART, 128), BF)],
        smem=(0,),
        near=(1,),
        near_out=(0,),
    )
    rows = exchanged(copies, "tp")
    partial_rows, grads, hidden = call(
        partial_kernel,
        [((N_TP, PART, 128), BF), ((PART, 1024), BF), ((PART, 512), BF)],
        rows,
        *weights,
        near=(0,),
        near_out=(0,),
    )
    arrived = exchanged(partial_rows, "tp")
    (returned,) = call(
        row_sum_kernel,
        [((N_SP, PAD, 128), BF)],
        place,
        arrived,
        states,
        smem=(0,),
        near=(1,),
        scratch=[pltpu.VMEM((ROWS + 8, 128), F32)],
    )
    own_grads, grads_a, grads_b, grads_c = call(
        weight_grads_kernel,
        [((WEIGHT_ROWS, 128), F32)] + 3 * [((WEIGHT_ROWS, 128), BF)],
        rows,
        grads,
        hidden,
        near=(0,),
        after=(returned,),
    )
    other_grads = (passed_on(grads_a, -1), passed_on(grads_b, 1), passed_on(grads_c, 2))
    back = exchanged(returned, SP)
    (residual,) = call(
        residual_kernel,
        [((N_TP, TOK, 128), BF)],
        back,
        turned,
        out_grad,
        near=(0,),
        after=(own_grads,),
    )
    full_grad = exchanged(residual, "tp")
    mixer_out, entering = call(
        forward_kernel,
        [((TOK, 128), BF), ((NBLK, 128, 64), F32)],
        back,
        q_t,
        k_t,
        value_rows,
        decay_t,
        near=(0,),
        after=(residual,),
    )
    mixer_grad, span_grad, to_other, kept = call(
        mixer_grad_kernel,
        [((TOK, 128), F32), ((32, 128), F32), ((1088, 128), BF), ((1024, 128), F32)],
        place,
        full_grad,
        w_out,
        mixer_out,
        q_t,
        decay_t,
        smem=(0,),
        near=(1,),
        near_out=(2, 3),
    )
    from_other = lax.ppermute(to_other, "sp_1", [(0, 1), (1, 0)])
    chip_sent, other_grad = call(
        chip_kernel,
        [((16, 96, 128), BF), ((32, 128), F32)],
        place,
        from_other,
        kept,
        span_grad,
        reach,
        smem=(0,),
        near=(1, 2),
    )
    later = exchanged(chip_sent, "sp_0")
    grad_proj, gq, gk, gv, gd = call(
        backward_kernel,
        [((64, 128), F32), ((64, TOK), BF), ((64, TOK), BF), ((TOK, 128), BF), ((64, TOK), F32)],
        place,
        later,
        other_grad,
        reach,
        mixer_grad,
        entering,
        q_t,
        k_t,
        value_rows,
        decay_t,
        smem=(0,),
        near=(1,),
    )
    gate_part, up_part, down_part = call(
        grad_sum_kernel,
        [((2048, 128), BF), ((2048, 128), BF), ((128, 2048), BF)],
        own_grads,
        *other_grads,
    )
    return (gate_part[None], up_part[None], down_part[None], grad_proj, gq.T, gk.T, gv, gd.T)


def solution(mesh):
    split = Mesh(mesh.devices.reshape(16, 2, mesh.shape["tp"]), ("sp_0", "sp_1", "tp"))
    placed = (
        P(SP, "tp"),
        P(SP, "tp"),
        P(SP, None),
        P(SP, None),
        P(SP, None, "tp"),
        P(SP, None, "tp"),
        P(SP, "tp", None),
        P(None, "tp"),
        P(SP, "tp"),
        P(SP, "tp"),
        P(SP, "tp"),
        P(SP, "tp"),
    )
    return jax.shard_map(
        body,
        mesh=split,
        in_specs=placed,
        out_specs=(
            P(SP, None, "tp"),
            P(SP, None, "tp"),
            P(SP, "tp", None),
            P(SP, "tp"),
            P(SP, "tp"),
            P(SP, "tp"),
            P(SP, "tp"),
            P(SP, "tp"),
        ),
        check_vma=False,
    )
```

```python
import jax
import jax.numpy as jnp
from jax import lax
from jax.experimental import pallas as pl
from jax.experimental.pallas import tpu as pltpu
from jax.sharding import Mesh
from jax.sharding import PartitionSpec as P


KEY_CHANNELS = 32
VAL_DIM = 64
TOP = 2
BLOCK = 64
CAP = 20
PAD = 24
SP = ("sp_0", "sp_1")
N_SP = 32
N_TP = 16
TOK = 256
ROWS = N_SP * CAP
SLOTS = N_SP * PAD
PART = ROWS // 4
LOT = 3 * 1024
NBLK = TOK // BLOCK
BF = jnp.bfloat16
F32 = jnp.float32
HI = lax.Precision.HIGHEST
SCALE = KEY_CHANNELS ** (-0.5)

NN = (((1,), (0,)), ((), ()))
NT = (((1,), (1,)), ((), ()))
TN = (((0,), (0,)), ((), ()))


def mm(a, b, dims=NN):
    return lax.dot_general(a.astype(BF), b.astype(BF), dims, preferred_element_type=F32)


def mm_exact(a, b, dims=NN):
    return lax.dot_general(a, b, dims, precision=HI, preferred_element_type=F32)


def iota(shape, dim):
    return lax.broadcasted_iota(jnp.int32, shape, dim)


def call(fn, outs, *args, scratch=(), smem=(), near=(), near_out=(), after=()):
    spaces = [pltpu.VMEM if k in near else pltpu.HBM for k in range(len(args))]
    args = [
        a if k in smem else pltpu.with_memory_space_constraint(a, spaces[k])
        for k, a in enumerate(args)
    ]
    after = [pltpu.with_memory_space_constraint(a, pltpu.HBM) for a in after]
    count = len(args)

    def run(*refs):
        fn(*refs[:count], *refs[count + len(after) :])

    return pl.pallas_call(
        run,
        out_shape=tuple(
            (pltpu.VMEM if k in near_out else pltpu.HBM)(s, d) for k, (s, d) in enumerate(outs)
        ),
        in_specs=[
            pl.BlockSpec(memory_space=pltpu.SMEM if k in smem else pltpu.VMEM)
            for k in range(count)
        ]
        + [pl.BlockSpec(memory_space=pltpu.HBM) for _ in after],
        out_specs=tuple(pl.BlockSpec(memory_space=pltpu.VMEM) for _ in outs),
        scratch_shapes=scratch,
        compiler_params=pltpu.CompilerParams(vmem_limit_bytes=24 * 1024 * 1024),
    )(*args, *after)


def head_masks():
    key_lane = iota((1, 64), 1) // KEY_CHANNELS
    val_lane = iota((1, 128), 1) // VAL_DIM
    keys = [(key_lane == h).astype(F32) for h in range(2)]
    vals = [(val_lane == h).astype(F32) for h in range(2)]
    own = (iota((128, 64), 0) // VAL_DIM == iota((128, 64), 1) // KEY_CHANNELS).astype(F32)
    return keys, vals, own


def packed_state(state):
    both = state[:64] + state[64:]
    return jnp.concatenate([both[:32], both[32:]], axis=1)


def opened_state(packed, own):
    both = jnp.concatenate([packed[:, :64], packed[:, 64:]], axis=0)
    return jnp.concatenate([both, both], axis=0) * own


def block_sums(decay):
    row, col = iota((TOK, TOK), 0), iota((TOK, TOK), 1)
    within = ((row // BLOCK == col // BLOCK) & (col <= row)).astype(F32)
    return mm_exact(within, decay)


def whole_sums(cumulative):
    offset, parts = jnp.zeros((1, 64), F32), []
    for n in range(NBLK):
        block = cumulative[n * BLOCK : (n + 1) * BLOCK]
        parts.append(block + offset)
        offset = offset + block[BLOCK - 1 :]
    return jnp.concatenate(parts, axis=0), offset


def closings(cumulative):
    return [cumulative[(n + 1) * BLOCK - 1 : (n + 1) * BLOCK] for n in range(NBLK)]


def per_block(rows):
    return jnp.concatenate([jnp.broadcast_to(r, (BLOCK, r.shape[1])) for r in rows], axis=0)


def two_parts(values):
    high = values.astype(BF).astype(F32)
    return high, values - high


def dispatch_kernel(
    routes_ref, weight_ref, x_ref, g_ref, k_ref, v_ref, decay_ref, sent_ref, pick_ref
):
    routes = routes_ref[...]
    expert = iota((N_SP, TOK), 0)
    hot = [(expert == routes[j : j + 1, :]) for j in range(TOP)]
    both = (hot[0] | hot[1]).astype(F32)
    before = (iota((TOK, TOK), 0) < iota((TOK, TOK), 1)).astype(F32)
    place = mm(both, before)
    owner, row = iota((SLOTS, N_SP), 0) // PAD, iota((SLOTS, N_SP), 0) % PAD
    mine = owner == iota((SLOTS, N_SP), 1)
    spread = mine.astype(F32)
    slot_place = (iota((SLOTS, TOK), 0) % PAD).astype(F32)
    picks = [(mm(spread, jnp.where(h, place, -1.0)) == slot_place).astype(F32) for h in hot]
    pick = picks[0] + picks[1]
    pick_ref[...] = pick.astype(BF)

    _, _, own = head_masks()
    keys = k_ref[...].astype(F32).T * SCALE
    so_far, total = whole_sums(block_sums(decay_ref[...].T))
    state = mm(v_ref[...], keys * jnp.exp(total - so_far), TN) * own
    state_high, state_low = two_parts(packed_state(state))
    total_row = jnp.concatenate(two_parts(total), axis=1)

    first = (mine & (row == CAP)).astype(F32)
    second = (mine & (row == CAP + 1)).astype(F32)
    chosen = jnp.concatenate([pick, first, second], axis=1)
    rows = jnp.concatenate([x_ref[...].astype(F32), state_high, state_low], axis=0)
    sent_ref[:, :PAD, :] = mm(chosen, rows).astype(BF).reshape(N_SP, PAD, 128)

    grad = g_ref[...].astype(F32)
    weight = jnp.concatenate([weight_ref[...], jnp.zeros((6, TOK), F32)], axis=0).T
    rows = [(weight[:, j : j + 1] * grad).astype(BF) for j in range(TOP)]
    sent = mm(picks[0], rows[0]) + mm(picks[1], rows[1])
    sent = jnp.where(iota((SLOTS, 128), 0) % PAD == CAP, total_row, sent)
    sent_ref[:, PAD:, :] = sent.astype(BF).reshape(N_SP, PAD, 128)


def turned_kernel(pick_ref, out_ref):
    out_ref[...] = pick_ref[...].astype(F32).T.astype(BF)


def quarter_of(place_ref, k):
    return jnp.where(place_ref[1] == 0, k % 4, k // 4)


def copies_kernel(place_ref, recv_ref, out_ref, states_ref, reach_ref, packed, rounded):
    for e in range(N_SP):
        block = recv_ref[e].astype(F32)
        at = (e // 8) * 2 * PART + (e % 8) * CAP
        packed[at : at + CAP, :] = block[:CAP]
        packed[at + PART : at + PART + CAP, :] = block[PAD : PAD + CAP]
    for q in range(4):
        rounded[q] = packed[q * 2 * PART : (q + 1) * 2 * PART, :].astype(BF)
    for k in range(N_TP):
        out_ref[k] = rounded[quarter_of(place_ref, k)]
    chip = place_ref[2]
    totals = [recv_ref[s, PAD + CAP : PAD + CAP + 1, :].astype(F32) for s in range(N_SP)]
    totals = jnp.concatenate(totals, axis=0)
    totals = totals[:, :64] + totals[:, 64:]
    double = jnp.concatenate([totals, totals], axis=1)
    decays = jnp.exp(double)
    state = jnp.zeros((1, 128), F32)
    for s in range(N_SP):
        states_ref[s : s + 1, :] = state
        pair = recv_ref[s, CAP : CAP + 2, :].astype(F32)
        state = decays[s : s + 1] * state + pair[0:1] + pair[1:2]
    target, between = iota((16, N_SP), 0), iota((16, N_SP), 1)
    passed = ((between >= 2 * target + 2) & (between < 2 * chip)).astype(F32)
    reach = jnp.exp(mm_exact(passed, double))
    reach_ref[:16, :] = jnp.where(iota((16, 128), 0) < chip, reach, 0.0)
    here = iota((N_SP, 128), 0)
    even = jnp.sum(jnp.where(here == 2 * chip, decays, 0.0), axis=0, keepdims=True)
    odd = jnp.sum(jnp.where(here == 2 * chip + 1, decays, 0.0), axis=0, keepdims=True)
    reach_ref[16:, :] = jnp.concatenate([even, odd, jnp.zeros((6, 128), F32)], axis=0)


def pack_kernel(wg_ref, wu_ref, wd_ref, a_ref, b_ref):
    a_ref[:2048, :] = wg_ref[...]
    a_ref[2048:, :] = wu_ref[:1024, :]
    b_ref[:1024, :] = wu_ref[1024:, :]
    for k in range(N_TP):
        b_ref[1024 + k * 128 : 1152 + k * 128, :] = wd_ref[:, k * 128 : (k + 1) * 128]


def wide(ref, at, size):
    return jnp.concatenate([ref[k, at : at + size, :] for k in range(N_TP)], axis=1)


def partial_kernel(rows_ref, *refs):
    lots, (part_ref, grads_ref, hidden_ref) = refs[:8], refs[8:]
    gates, downs = [], []
    for a_ref, b_ref in zip(lots[::2], lots[1::2]):
        gates += [a_ref[:2048, :], jnp.concatenate([a_ref[2048:, :], b_ref[:1024, :]], axis=0)]
        downs.append([b_ref[1024 + k * 128 : 1152 + k * 128, :] for k in range(N_TP)])
    weight = jnp.concatenate(gates, axis=1)
    down = jnp.concatenate([jnp.concatenate(d, axis=1) for d in downs], axis=0)
    pre = mm(wide(rows_ref, 0, PART), weight)
    hidden_grad = mm(wide(rows_ref, PART, PART), down, NT)
    grads = []
    for b in range(4):
        gate_pre, up_pre = pre[:, 256 * b : 256 * b + 128], pre[:, 256 * b + 128 : 256 * b + 256]
        upper = hidden_grad[:, 128 * b : 128 * b + 128]
        sigmoid = jax.nn.sigmoid(gate_pre)
        activated = gate_pre * sigmoid
        hidden_ref[:, 128 * b : 128 * b + 128] = (activated * up_pre).astype(BF)
        gate = upper * up_pre * sigmoid * (1.0 + gate_pre * (1.0 - sigmoid))
        grads += [gate.astype(BF), (upper * activated).astype(BF)]
    grads = jnp.concatenate(grads, axis=1)
    grads_ref[...] = grads
    for k in range(0, N_TP, 2):
        part = mm(grads, weight[k * 128 : (k + 2) * 128], NT).astype(BF)
        part_ref[k] = part[:, :128]
        part_ref[k + 1] = part[:, 128:]


def weight_grads_kernel(rows_ref, grads_ref, hidden_ref, *out_refs):
    grads = grads_ref[...]
    hidden = hidden_ref[...]
    for k in range(0, N_TP, 2):
        x = jnp.concatenate([rows_ref[k, :PART, :], rows_ref[k + 1, :PART, :]], axis=1)
        g = jnp.concatenate([rows_ref[k, PART:, :], rows_ref[k + 1, PART:, :]], axis=1)
        both = mm(x, grads, TN)
        down = mm(hidden, g, TN)
        at = k * 128
        for b in range(4):
            a_ref, b_ref = out_refs[2 * b : 2 * b + 2]
            kind = a_ref.dtype
            up = both[:, 256 * b + 128 : 256 * b + 256].astype(kind)
            a_ref[at : at + 256, :] = both[:, 256 * b : 256 * b + 128].astype(kind)
            if k < N_TP // 2:
                a_ref[2048 + at : 2304 + at, :] = up
            else:
                b_ref[at - 1024 : at - 768, :] = up
            for n in range(2):
                block = 1024 + at + n * 128
                b_ref[block : block + 128, :] = down[
                    128 * b : 128 * b + 128, n * 128 : (n + 1) * 128
                ].astype(kind)


def relay_kernel(
    left_a_ref, left_b_ref, right_a_ref, right_b_ref, far_a_ref, far_b_ref, left_ref, right_ref
):
    right_ref[:LOT, :] = (right_a_ref[...].astype(F32) + far_a_ref[...].astype(F32)).astype(BF)
    right_ref[LOT:, :] = right_b_ref[...]
    left_ref[:LOT, :] = left_a_ref[...]
    left_ref[LOT:, :] = (left_b_ref[...].astype(F32) + far_b_ref[...].astype(F32)).astype(BF)


def grad_sum_kernel(own_a_ref, own_b_ref, x_ref, y_ref, gate_ref, up_ref, down_ref):
    def total(at, size):
        ref, start = (own_a_ref, at) if at < LOT else (own_b_ref, at - LOT)
        other = x_ref[at : at + size, :].astype(F32) + y_ref[at : at + size, :].astype(F32)
        return (ref[start : start + size, :] + other).astype(BF)

    for k in range(N_TP):
        here = slice(k * 128, (k + 1) * 128)
        gate_ref[here, :] = total(k * 128, 128)
        up_ref[here, :] = total(2048 + k * 128, 128)
        down_ref[:, here] = total(4096 + k * 128, 128)


def row_sum_kernel(place_ref, part_ref, states_ref, out_ref, total):
    for q in range(4):
        acc = jnp.zeros((PART, 128), F32)
        for j in range(4):
            source = jnp.where(place_ref[1] == 0, 4 * j + q, 4 * q + j)
            acc = acc + part_ref[source].astype(F32)
        total[q * PART : (q + 1) * PART, :] = acc
    total[ROWS:, :] = jnp.zeros((8, 128), F32)
    row = iota((PAD, 128), 0)
    high, low = two_parts(states_ref[...])
    for e in range(N_SP):
        rows = jnp.where(row < CAP, total[e * CAP : e * CAP + PAD, :], 0.0)
        rows = jnp.where(row == CAP, high[e : e + 1], rows)
        rows = jnp.where(row == CAP + 1, low[e : e + 1], rows)
        out_ref[e] = rows.astype(BF)


def residual_kernel(back_ref, turned_ref, g_ref, out_ref):
    routed = mm(turned_ref[...], back_ref[...].reshape(SLOTS, 128))
    residual = (g_ref[...].astype(F32) + routed).astype(BF)
    for k in range(N_TP):
        out_ref[k] = residual


def scores_of(queries, keys, mask, causal):
    return jnp.where(causal, mm(queries * mask, keys, NT), 0.0)


def causal_blocks():
    row, col = iota((TOK, TOK), 0), iota((TOK, TOK), 1)
    return (row // BLOCK == col // BLOCK) & (col <= row)


def forward_kernel(back_ref, q_ref, k_ref, v_ref, decay_ref, out_ref, entering_ref):
    key_mask, val_mask, own = head_masks()
    rows = [back_ref[s, CAP : CAP + 2, :].astype(F32) for s in range(N_SP)]
    packed = jnp.concatenate([r[0:1] + r[1:2] for r in rows], axis=0)
    state = opened_state(packed, own)
    queries = q_ref[...].astype(F32).T
    keys = k_ref[...].astype(F32).T * SCALE
    values = v_ref[...].astype(F32)
    cumulative = block_sums(decay_ref[...].T)
    closing = closings(cumulative)
    scaled_q = queries * jnp.exp(cumulative)
    scaled_k = keys * jnp.exp(-cumulative)
    tail = keys * jnp.exp(per_block(closing) - cumulative)
    causal = causal_blocks()
    within = jnp.zeros((TOK, 128), F32)
    for h in range(2):
        scores = scores_of(scaled_q, scaled_k, key_mask[h], causal)
        within = within + mm(scores, values * val_mask[h])
    for n in range(NBLK):
        here = slice(n * BLOCK, (n + 1) * BLOCK)
        entering_ref[n] = state
        out_ref[here, :] = (within[here] + mm(scaled_q[here], state, NT)).astype(BF)
        state = jnp.exp(closing[n]) * state + mm(values[here], tail[here], TN) * own


def mixer_grad_kernel(
    place_ref, full_ref, w_ref, mixed_ref, q_ref, decay_ref, grad_ref, span_ref, sent_ref, kept_ref
):
    _, _, own = head_masks()
    grad = mm(wide(full_ref, 0, TOK), w_ref[...])
    grad_ref[...] = grad
    so_far, _ = whole_sums(block_sums(decay_ref[...].T))
    scaled = q_ref[...].astype(F32).T * jnp.exp(so_far)
    packed = packed_state(mm(grad, scaled, TN) * own)
    span_ref[...] = packed
    high, low = two_parts(packed)
    sent_ref[1024:1056, :] = high.astype(BF)
    sent_ref[1056:, :] = low.astype(BF)
    mixed = mixed_ref[...]
    first = place_ref[1] == 0
    for k in range(0, N_TP, 2):
        rows = jnp.concatenate([full_ref[k], full_ref[k + 1]], axis=1)
        part = mm(rows, mixed, TN)
        for n in range(2):
            low, high = part[n * 128 : n * 128 + 64], part[n * 128 + 64 : n * 128 + 128]
            here = slice((k + n) * 64, (k + n + 1) * 64)
            kept_ref[here, :] = jnp.where(first, low, high)
            sent_ref[here, :] = jnp.where(first, high, low).astype(BF)


def chip_kernel(place_ref, recv_ref, kept_ref, span_ref, reach_ref, sent_ref, other_ref):
    other = recv_ref[1024:1056, :].astype(F32) + recv_ref[1056:, :].astype(F32)
    other_ref[...] = other
    first = place_ref[1] == 0
    mine = span_ref[...]
    both = jnp.where(first, mine, other) + reach_ref[16:17, :] * jnp.where(first, other, mine)
    for z in range(16):
        here = slice(z * 64, (z + 1) * 64)
        sent_ref[z, :32, :] = (both * reach_ref[z : z + 1, :]).astype(BF)
        sent_ref[z, 32:, :] = (kept_ref[here, :] + recv_ref[here, :].astype(F32)).astype(BF)


def backward_kernel(
    place_ref,
    later_ref,
    other_ref,
    reach_ref,
    grad_ref,
    entering_ref,
    q_ref,
    k_ref,
    v_ref,
    decay_ref,
    gp_ref,
    gq_ref,
    gk_ref,
    gv_ref,
    gd_ref,
):
    key_mask, val_mask, own = head_masks()
    sums = later_ref[0].astype(F32)
    for z in range(1, 16):
        sums = sums + later_ref[z].astype(F32)
    gp_ref[...] = sums[32:]
    packed = sums[:32]
    packed = jnp.where(place_ref[1] == 0, reach_ref[17:18, :] * packed + other_ref[...], packed)
    state_grad = opened_state(packed, own)
    grad = grad_ref[...]
    queries = q_ref[...].astype(F32).T
    keys = k_ref[...].astype(F32).T * SCALE
    values = v_ref[...].astype(F32)
    cumulative = block_sums(decay_ref[...].T)
    closing = closings(cumulative)
    grow, shrink = jnp.exp(cumulative), jnp.exp(-cumulative)
    rest = jnp.exp(per_block(closing) - cumulative)
    scaled_q, scaled_k, tail = queries * grow, keys * shrink, keys * rest
    causal = causal_blocks()
    value_grad = jnp.zeros((TOK, 128), F32)
    query_grad = jnp.zeros((TOK, 64), F32)
    key_grad = jnp.zeros((TOK, 64), F32)
    for h in range(2):
        scores = scores_of(scaled_q, scaled_k, key_mask[h], causal)
        score_grad = jnp.where(causal, mm(grad * val_mask[h], values, NT), 0.0)
        value_grad = value_grad + mm(scores, grad * val_mask[h], TN)
        query_grad = query_grad + mm(score_grad, scaled_k * key_mask[h])
        key_grad = key_grad + mm(score_grad, scaled_q * key_mask[h], TN)
    carried_v, carried_q, tail_grad, close_grad = ([None] * NBLK for _ in range(4))
    for n in reversed(range(NBLK)):
        here = slice(n * BLOCK, (n + 1) * BLOCK)
        entering = entering_ref[n]
        decay_out = jnp.exp(closing[n])
        carried_v[n] = mm(tail[here], state_grad, NT)
        carried_q[n] = mm(grad[here], entering)
        tail_grad[n] = mm(values[here], state_grad)
        close_grad[n] = decay_out * jnp.sum(state_grad * entering, axis=0, keepdims=True) + jnp.sum(
            tail_grad[n] * tail[here], axis=0, keepdims=True
        )
        state_grad = decay_out * state_grad + mm(grad[here], scaled_q[here], TN) * own
    value_grad = value_grad + jnp.concatenate(carried_v, axis=0)
    query_grad = query_grad + jnp.concatenate(carried_q, axis=0)
    tail_grad = jnp.concatenate(tail_grad, axis=0)
    change = query_grad * scaled_q - key_grad * scaled_k - tail_grad * tail
    row, col = iota((TOK, TOK), 0), iota((TOK, TOK), 1)
    onward = ((row // BLOCK == col // BLOCK) & (col >= row)).astype(F32)
    gd_ref[...] = (mm_exact(onward, change) + per_block(close_grad)).T
    gq_ref[...] = (query_grad * grow).T.astype(BF)
    gk_ref[...] = ((key_grad * shrink + tail_grad * rest) * SCALE).T.astype(BF)
    gv_ref[...] = value_grad.astype(BF)


def exchanged(blocks, axis):
    return lax.all_to_all(blocks, axis, split_axis=0, concat_axis=0, tiled=True)


def ring_step(step):
    pairs = []
    for t in range(N_TP):
        y, x = t // 4, t % 4
        pairs.append((t, 4 * y + (x + step) % 4))
        pairs.append((N_TP + t, N_TP + 4 * ((y + step) % 4) + x))
    return pairs


def passed_on(array, step):
    return lax.ppermute(array, ("sp_1", "tp"), ring_step(step))


def body(
    moe_input,
    out_grad,
    routes,
    route_weight,
    w_gate,
    w_up,
    w_down,
    w_out,
    queries,
    key_rows,
    value_rows,
    log_decay,
):
    q_t, k_t, decay_t = queries.T, key_rows.T, log_decay.T
    place = jnp.stack(
        [lax.axis_index(SP), lax.axis_index("sp_1"), lax.axis_index("sp_0")]
    ).astype(jnp.int32)

    sent, pick = call(
        dispatch_kernel,
        [((N_SP, 2 * PAD, 128), BF), ((SLOTS, TOK), BF)],
        routes.T,
        route_weight.T,
        moe_input,
        out_grad,
        k_t,
        value_rows,
        decay_t,
    )
    recv = exchanged(sent, SP)
    own_a, own_b = call(
        pack_kernel, [((LOT, 128), BF), ((LOT, 128), BF)], w_gate[0], w_up[0], w_down[0]
    )
    left_a = passed_on(own_a, 1)
    right_b = passed_on(own_b, -1)
    left_b = passed_on(own_b, 1)
    right_a = passed_on(own_a, -1)
    far_a = passed_on(left_a, 1)
    far_b = passed_on(right_b, -1)
    weights = (own_a, own_b, left_a, left_b, right_a, right_b, far_a, far_b)
    (turned,) = call(turned_kernel, [((TOK, SLOTS), BF)], pick)
    copies, states, reach = call(
        copies_kernel,
        [((N_TP, 2 * PART, 128), BF), ((N_SP, 128), F32), ((24, 128), F32)],
        place,
        recv,
        scratch=[pltpu.VMEM((2 * ROWS, 128), F32), pltpu.VMEM((4, 2 * PART, 128), BF)],
        smem=(0,),
        near=(1,),
        near_out=(0,),
    )
    rows = exchanged(copies, "tp")
    partial_rows, grads, hidden = call(
        partial_kernel,
        [((N_TP, PART, 128), BF), ((PART, 1024), BF), ((PART, 512), BF)],
        rows,
        *weights,
        near=(0,),
        near_out=(0,),
    )
    arrived = exchanged(partial_rows, "tp")
    (returned,) = call(
        row_sum_kernel,
        [((N_SP, PAD, 128), BF)],
        place,
        arrived,
        states,
        smem=(0,),
        near=(1,),
        scratch=[pltpu.VMEM((ROWS + 8, 128), F32)],
    )
    own_grad_a, own_grad_b, *lots = call(
        weight_grads_kernel,
        2 * [((LOT, 128), F32)] + 6 * [((LOT, 128), BF)],
        rows,
        grads,
        hidden,
        near=(0,),
        after=(returned,),
    )
    via_right = passed_on(lots[4], 1)
    via_left = passed_on(lots[5], -1)
    back = exchanged(returned, SP)
    (residual,) = call(
        residual_kernel,
        [((N_TP, TOK, 128), BF)],
        back,
        turned,
        out_grad,
        near=(0,),
        after=(own_grad_a,),
    )
    full_grad = exchanged(residual, "tp")
    mixer_out, entering = call(
        forward_kernel,
        [((TOK, 128), BF), ((NBLK, 128, 64), F32)],
        back,
        q_t,
        k_t,
        value_rows,
        decay_t,
        near=(0,),
        after=(residual,),
    )
    to_left, to_right = call(
        relay_kernel, 2 * [((2 * LOT, 128), BF)], *lots[:4], via_right, via_left, after=(residual,)
    )
    mixer_grad, span_grad, to_other, kept = call(
        mixer_grad_kernel,
        [((TOK, 128), F32), ((32, 128), F32), ((1088, 128), BF), ((1024, 128), F32)],
        place,
        full_grad,
        w_out,
        mixer_out,
        q_t,
        decay_t,
        smem=(0,),
        after=(to_left,),
        near=(1,),
        near_out=(2, 3),
    )
    from_other = lax.ppermute(to_other, "sp_1", [(0, 1), (1, 0)])
    chip_sent, other_grad = call(
        chip_kernel,
        [((16, 96, 128), BF), ((32, 128), F32)],
        place,
        from_other,
        kept,
        span_grad,
        reach,
        smem=(0,),
        near=(1, 2),
    )
    later = exchanged(chip_sent, "sp_0")
    grad_proj, gq, gk, gv, gd = call(
        backward_kernel,
        [((64, 128), F32), ((64, TOK), BF), ((64, TOK), BF), ((TOK, 128), BF), ((64, TOK), F32)],
        place,
        later,
        other_grad,
        reach,
        mixer_grad,
        entering,
        q_t,
        k_t,
        value_rows,
        decay_t,
        smem=(0,),
        near=(1,),
    )
    from_right = passed_on(to_left, -1)
    from_left = passed_on(to_right, 1)
    gate_part, up_part, down_part = call(
        grad_sum_kernel,
        [((2048, 128), BF), ((2048, 128), BF), ((128, 2048), BF)],
        own_grad_a,
        own_grad_b,
        from_left,
        from_right,
    )
    return (gate_part[None], up_part[None], down_part[None], grad_proj, gq.T, gk.T, gv, gd.T)


def solution(mesh):
    split = Mesh(mesh.devices.reshape(16, 2, mesh.shape["tp"]), ("sp_0", "sp_1", "tp"))
    placed = (
        P(SP, "tp"),
        P(SP, "tp"),
        P(SP, None),
        P(SP, None),
        P(SP, None, "tp"),
        P(SP, None, "tp"),
        P(SP, "tp", None),
        P(None, "tp"),
        P(SP, "tp"),
        P(SP, "tp"),
        P(SP, "tp"),
        P(SP, "tp"),
    )
    return jax.shard_map(
        body,
        mesh=split,
        in_specs=placed,
        out_specs=(
            P(SP, None, "tp"),
            P(SP, None, "tp"),
            P(SP, "tp", None),
            P(SP, "tp"),
            P(SP, "tp"),
            P(SP, "tp"),
            P(SP, "tp"),
            P(SP, "tp"),
        ),
        check_vma=False,
    )
```

```python
import jax
import jax.numpy as jnp
from jax import lax
from jax.experimental import pallas as pl
from jax.experimental.pallas import tpu as pltpu
from jax.sharding import Mesh
from jax.sharding import PartitionSpec as P


KEY_CHANNELS = 32
VAL_DIM = 64
TOP = 2
BLOCK = 64
CAP = 20
PAD = 24
SP = ("sp_0", "sp_1")
N_SP = 32
N_TP = 16
TOK = 256
ROWS = N_SP * CAP
SLOTS = N_SP * PAD
PART = ROWS // 4
LOT = 3 * 1024
NBLK = TOK // BLOCK
BF = jnp.bfloat16
F32 = jnp.float32
HI = lax.Precision.HIGHEST
SCALE = KEY_CHANNELS ** (-0.5)

NN = (((1,), (0,)), ((), ()))
NT = (((1,), (1,)), ((), ()))
TN = (((0,), (0,)), ((), ()))


def mm(a, b, dims=NN):
    return lax.dot_general(a.astype(BF), b.astype(BF), dims, preferred_element_type=F32)


def mm_exact(a, b, dims=NN):
    return lax.dot_general(a, b, dims, precision=HI, preferred_element_type=F32)


def iota(shape, dim):
    return lax.broadcasted_iota(jnp.int32, shape, dim)


def call(fn, outs, *args, scratch=(), smem=(), near=(), near_out=(), after=()):
    spaces = [pltpu.VMEM if k in near else pltpu.HBM for k in range(len(args))]
    args = [
        a if k in smem else pltpu.with_memory_space_constraint(a, spaces[k])
        for k, a in enumerate(args)
    ]
    after = [pltpu.with_memory_space_constraint(a, pltpu.HBM) for a in after]
    count = len(args)

    def run(*refs):
        fn(*refs[:count], *refs[count + len(after) :])

    return pl.pallas_call(
        run,
        out_shape=tuple(
            (pltpu.VMEM if k in near_out else pltpu.HBM)(s, d) for k, (s, d) in enumerate(outs)
        ),
        in_specs=[
            pl.BlockSpec(memory_space=pltpu.SMEM if k in smem else pltpu.VMEM)
            for k in range(count)
        ]
        + [pl.BlockSpec(memory_space=pltpu.HBM) for _ in after],
        out_specs=tuple(pl.BlockSpec(memory_space=pltpu.VMEM) for _ in outs),
        scratch_shapes=scratch,
        compiler_params=pltpu.CompilerParams(vmem_limit_bytes=24 * 1024 * 1024),
    )(*args, *after)


def head_masks():
    key_lane = iota((1, 64), 1) // KEY_CHANNELS
    val_lane = iota((1, 128), 1) // VAL_DIM
    keys = [(key_lane == h).astype(F32) for h in range(2)]
    vals = [(val_lane == h).astype(F32) for h in range(2)]
    own = (iota((128, 64), 0) // VAL_DIM == iota((128, 64), 1) // KEY_CHANNELS).astype(F32)
    return keys, vals, own


def packed_state(state):
    both = state[:64] + state[64:]
    return jnp.concatenate([both[:32], both[32:]], axis=1)


def opened_state(packed, own):
    both = jnp.concatenate([packed[:, :64], packed[:, 64:]], axis=0)
    return jnp.concatenate([both, both], axis=0) * own


def block_sums(decay):
    row, col = iota((TOK, TOK), 0), iota((TOK, TOK), 1)
    within = ((row // BLOCK == col // BLOCK) & (col <= row)).astype(F32)
    return mm_exact(within, decay)


def whole_sums(cumulative):
    offset, parts = jnp.zeros((1, 64), F32), []
    for n in range(NBLK):
        block = cumulative[n * BLOCK : (n + 1) * BLOCK]
        parts.append(block + offset)
        offset = offset + block[BLOCK - 1 :]
    return jnp.concatenate(parts, axis=0), offset


def closings(cumulative):
    return [cumulative[(n + 1) * BLOCK - 1 : (n + 1) * BLOCK] for n in range(NBLK)]


def per_block(rows):
    return jnp.concatenate([jnp.broadcast_to(r, (BLOCK, r.shape[1])) for r in rows], axis=0)


def two_parts(values):
    high = values.astype(BF).astype(F32)
    return high, values - high


def dispatch_kernel(
    routes_ref, weight_ref, x_ref, g_ref, k_ref, v_ref, decay_ref, sent_ref, pick_ref
):
    routes = routes_ref[...]
    expert = iota((N_SP, TOK), 0)
    hot = [(expert == routes[j : j + 1, :]) for j in range(TOP)]
    both = (hot[0] | hot[1]).astype(F32)
    before = (iota((TOK, TOK), 0) < iota((TOK, TOK), 1)).astype(F32)
    place = mm(both, before)
    owner, row = iota((SLOTS, N_SP), 0) // PAD, iota((SLOTS, N_SP), 0) % PAD
    mine = owner == iota((SLOTS, N_SP), 1)
    spread = mine.astype(F32)
    slot_place = (iota((SLOTS, TOK), 0) % PAD).astype(F32)
    picks = [(mm(spread, jnp.where(h, place, -1.0)) == slot_place).astype(F32) for h in hot]
    pick = picks[0] + picks[1]
    pick_ref[...] = pick.astype(BF)

    _, _, own = head_masks()
    keys = k_ref[...].astype(F32).T * SCALE
    so_far, total = whole_sums(block_sums(decay_ref[...].T))
    state = mm(v_ref[...], keys * jnp.exp(total - so_far), TN) * own
    state_high, state_low = two_parts(packed_state(state))
    total_row = jnp.concatenate(two_parts(total), axis=1)

    first = (mine & (row == CAP)).astype(F32)
    second = (mine & (row == CAP + 1)).astype(F32)
    chosen = jnp.concatenate([pick, first, second], axis=1)
    rows = jnp.concatenate([x_ref[...].astype(F32), state_high, state_low], axis=0)
    sent_ref[:, :PAD, :] = mm(chosen, rows).astype(BF).reshape(N_SP, PAD, 128)

    grad = g_ref[...].astype(F32)
    weight = jnp.concatenate([weight_ref[...], jnp.zeros((6, TOK), F32)], axis=0).T
    rows = [(weight[:, j : j + 1] * grad).astype(BF) for j in range(TOP)]
    sent = mm(picks[0], rows[0]) + mm(picks[1], rows[1])
    sent = jnp.where(iota((SLOTS, 128), 0) % PAD == CAP, total_row, sent)
    sent_ref[:, PAD:, :] = sent.astype(BF).reshape(N_SP, PAD, 128)


def turned_kernel(pick_ref, out_ref):
    out_ref[...] = pick_ref[...].astype(F32).T.astype(BF)


def quarter_of(place_ref, k):
    return jnp.where(place_ref[1] == 0, k % 4, k // 4)


def copies_kernel(place_ref, recv_ref, out_ref, states_ref, reach_ref, packed, rounded):
    for e in range(N_SP):
        block = recv_ref[e].astype(F32)
        at = (e // 8) * 2 * PART + (e % 8) * CAP
        packed[at : at + CAP, :] = block[:CAP]
        packed[at + PART : at + PART + CAP, :] = block[PAD : PAD + CAP]
    for q in range(4):
        rounded[q] = packed[q * 2 * PART : (q + 1) * 2 * PART, :].astype(BF)
    for k in range(N_TP):
        out_ref[k] = rounded[quarter_of(place_ref, k)]
    chip = place_ref[2]
    totals = [recv_ref[s, PAD + CAP : PAD + CAP + 1, :].astype(F32) for s in range(N_SP)]
    totals = jnp.concatenate(totals, axis=0)
    totals = totals[:, :64] + totals[:, 64:]
    double = jnp.concatenate([totals, totals], axis=1)
    decays = jnp.exp(double)
    state = jnp.zeros((1, 128), F32)
    for s in range(N_SP):
        states_ref[s : s + 1, :] = state
        pair = recv_ref[s, CAP : CAP + 2, :].astype(F32)
        state = decays[s : s + 1] * state + pair[0:1] + pair[1:2]
    target, between = iota((16, N_SP), 0), iota((16, N_SP), 1)
    passed = ((between >= 2 * target + 2) & (between < 2 * chip)).astype(F32)
    reach = jnp.exp(mm_exact(passed, double))
    reach_ref[:16, :] = jnp.where(iota((16, 128), 0) < chip, reach, 0.0)
    here = iota((N_SP, 128), 0)
    even = jnp.sum(jnp.where(here == 2 * chip, decays, 0.0), axis=0, keepdims=True)
    odd = jnp.sum(jnp.where(here == 2 * chip + 1, decays, 0.0), axis=0, keepdims=True)
    reach_ref[16:, :] = jnp.concatenate([even, odd, jnp.zeros((6, 128), F32)], axis=0)


def pack_kernel(wg_ref, wu_ref, wd_ref, a_ref, b_ref):
    a_ref[:2048, :] = wg_ref[...]
    a_ref[2048:, :] = wu_ref[:1024, :]
    b_ref[:1024, :] = wu_ref[1024:, :]
    for k in range(N_TP):
        b_ref[1024 + k * 128 : 1152 + k * 128, :] = wd_ref[:, k * 128 : (k + 1) * 128]


def wide(ref, at, size):
    return jnp.concatenate([ref[k, at : at + size, :] for k in range(N_TP)], axis=1)


def partial_kernel(rows_ref, *refs):
    lots, (part_ref, grads_ref, hidden_ref) = refs[:8], refs[8:]
    gates, downs = [], []
    for a_ref, b_ref in zip(lots[::2], lots[1::2]):
        gates += [a_ref[:2048, :], jnp.concatenate([a_ref[2048:, :], b_ref[:1024, :]], axis=0)]
        downs.append([b_ref[1024 + k * 128 : 1152 + k * 128, :] for k in range(N_TP)])
    weight = jnp.concatenate(gates, axis=1)
    down = jnp.concatenate([jnp.concatenate(d, axis=1) for d in downs], axis=0)
    pre = mm(wide(rows_ref, 0, PART), weight)
    hidden_grad = mm(wide(rows_ref, PART, PART), down, NT)
    grads = []
    for b in range(4):
        gate_pre, up_pre = pre[:, 256 * b : 256 * b + 128], pre[:, 256 * b + 128 : 256 * b + 256]
        upper = hidden_grad[:, 128 * b : 128 * b + 128]
        sigmoid = jax.nn.sigmoid(gate_pre)
        activated = gate_pre * sigmoid
        hidden_ref[:, 128 * b : 128 * b + 128] = (activated * up_pre).astype(BF)
        gate = upper * up_pre * sigmoid * (1.0 + gate_pre * (1.0 - sigmoid))
        grads += [gate.astype(BF), (upper * activated).astype(BF)]
    grads = jnp.concatenate(grads, axis=1)
    grads_ref[...] = grads
    for k in range(0, N_TP, 2):
        part = mm(grads, weight[k * 128 : (k + 2) * 128], NT).astype(BF)
        part_ref[k] = part[:, :128]
        part_ref[k + 1] = part[:, 128:]


def weight_grads_kernel(rows_ref, grads_ref, hidden_ref, *out_refs):
    grads = grads_ref[...]
    hidden = hidden_ref[...]
    for k in range(0, N_TP, 2):
        x = jnp.concatenate([rows_ref[k, :PART, :], rows_ref[k + 1, :PART, :]], axis=1)
        g = jnp.concatenate([rows_ref[k, PART:, :], rows_ref[k + 1, PART:, :]], axis=1)
        both = mm(x, grads, TN)
        down = mm(hidden, g, TN)
        at = k * 128
        for b, (a_part, b_part) in enumerate(lots_of(out_refs)):
            (a_ref, a_at), (b_ref, b_at) = a_part, b_part
            kind = a_ref.dtype
            up = both[:, 256 * b + 128 : 256 * b + 256].astype(kind)
            a_ref[a_at + at : a_at + at + 256, :] = both[:, 256 * b : 256 * b + 128].astype(kind)
            if k < N_TP // 2:
                a_ref[a_at + 2048 + at : a_at + 2304 + at, :] = up
            else:
                b_ref[b_at + at - 1024 : b_at + at - 768, :] = up
            for n in range(2):
                block = b_at + 1024 + at + n * 128
                b_ref[block : block + 128, :] = down[
                    128 * b : 128 * b + 128, n * 128 : (n + 1) * 128
                ].astype(kind)


def lots_of(refs):
    own_a, own_b, to_left, to_right, left_b, right_a = refs
    return (
        ((own_a, 0), (own_b, 0)),
        ((to_left, 0), (left_b, 0)),
        ((right_a, 0), (to_right, LOT)),
        ((to_right, 0), (to_left, LOT)),
    )


def relay_kernel(left_b_ref, right_a_ref, from_right_ref, from_left_ref, to_left_ref, to_right_ref):
    far_a, far_b = from_left_ref[:LOT, :].astype(F32), from_right_ref[LOT:, :].astype(F32)
    to_right_ref[...] = (right_a_ref[...].astype(F32) + far_a).astype(BF)
    to_left_ref[...] = (left_b_ref[...].astype(F32) + far_b).astype(BF)


def grad_sum_kernel(
    own_a_ref,
    own_b_ref,
    from_right_ref,
    from_left_ref,
    last_a_ref,
    last_b_ref,
    gate_ref,
    up_ref,
    down_ref,
):
    def total(at, size):
        if at < LOT:
            refs = (own_a_ref, from_right_ref, last_a_ref)
            rows = [r[at : at + size, :].astype(F32) for r in refs]
        else:
            own, last = (r[at - LOT : at - LOT + size, :] for r in (own_b_ref, last_b_ref))
            rows = [own, from_left_ref[at : at + size, :].astype(F32), last.astype(F32)]
        return (rows[0] + rows[1] + rows[2]).astype(BF)

    for k in range(N_TP):
        here = slice(k * 128, (k + 1) * 128)
        gate_ref[here, :] = total(k * 128, 128)
        up_ref[here, :] = total(2048 + k * 128, 128)
        down_ref[:, here] = total(4096 + k * 128, 128)


def row_sum_kernel(place_ref, part_ref, states_ref, out_ref, total):
    for q in range(4):
        acc = jnp.zeros((PART, 128), F32)
        for j in range(4):
            source = jnp.where(place_ref[1] == 0, 4 * j + q, 4 * q + j)
            acc = acc + part_ref[source].astype(F32)
        total[q * PART : (q + 1) * PART, :] = acc
    total[ROWS:, :] = jnp.zeros((8, 128), F32)
    row = iota((PAD, 128), 0)
    high, low = two_parts(states_ref[...])
    for e in range(N_SP):
        rows = jnp.where(row < CAP, total[e * CAP : e * CAP + PAD, :], 0.0)
        rows = jnp.where(row == CAP, high[e : e + 1], rows)
        rows = jnp.where(row == CAP + 1, low[e : e + 1], rows)
        out_ref[e] = rows.astype(BF)


def residual_kernel(back_ref, turned_ref, g_ref, out_ref):
    routed = mm(turned_ref[...], back_ref[...].reshape(SLOTS, 128))
    residual = (g_ref[...].astype(F32) + routed).astype(BF)
    for k in range(N_TP):
        out_ref[k] = residual


def scores_of(queries, keys, mask, causal):
    return jnp.where(causal, mm(queries * mask, keys, NT), 0.0)


def causal_blocks():
    row, col = iota((TOK, TOK), 0), iota((TOK, TOK), 1)
    return (row // BLOCK == col // BLOCK) & (col <= row)


def forward_kernel(back_ref, q_ref, k_ref, v_ref, decay_ref, out_ref, entering_ref):
    key_mask, val_mask, own = head_masks()
    rows = [back_ref[s, CAP : CAP + 2, :].astype(F32) for s in range(N_SP)]
    packed = jnp.concatenate([r[0:1] + r[1:2] for r in rows], axis=0)
    state = opened_state(packed, own)
    queries = q_ref[...].astype(F32).T
    keys = k_ref[...].astype(F32).T * SCALE
    values = v_ref[...].astype(F32)
    cumulative = block_sums(decay_ref[...].T)
    closing = closings(cumulative)
    scaled_q = queries * jnp.exp(cumulative)
    scaled_k = keys * jnp.exp(-cumulative)
    tail = keys * jnp.exp(per_block(closing) - cumulative)
    causal = causal_blocks()
    within = jnp.zeros((TOK, 128), F32)
    for h in range(2):
        scores = scores_of(scaled_q, scaled_k, key_mask[h], causal)
        within = within + mm(scores, values * val_mask[h])
    for n in range(NBLK):
        here = slice(n * BLOCK, (n + 1) * BLOCK)
        entering_ref[n] = state
        out_ref[here, :] = (within[here] + mm(scaled_q[here], state, NT)).astype(BF)
        state = jnp.exp(closing[n]) * state + mm(values[here], tail[here], TN) * own


def mixer_grad_kernel(
    place_ref, full_ref, w_ref, mixed_ref, q_ref, decay_ref, grad_ref, span_ref, sent_ref, kept_ref
):
    _, _, own = head_masks()
    grad = mm(wide(full_ref, 0, TOK), w_ref[...])
    grad_ref[...] = grad
    so_far, _ = whole_sums(block_sums(decay_ref[...].T))
    scaled = q_ref[...].astype(F32).T * jnp.exp(so_far)
    packed = packed_state(mm(grad, scaled, TN) * own)
    span_ref[...] = packed
    high, low = two_parts(packed)
    sent_ref[1024:1056, :] = high.astype(BF)
    sent_ref[1056:, :] = low.astype(BF)
    mixed = mixed_ref[...]
    first = place_ref[1] == 0
    for k in range(0, N_TP, 2):
        rows = jnp.concatenate([full_ref[k], full_ref[k + 1]], axis=1)
        part = mm(rows, mixed, TN)
        for n in range(2):
            low, high = part[n * 128 : n * 128 + 64], part[n * 128 + 64 : n * 128 + 128]
            here = slice((k + n) * 64, (k + n + 1) * 64)
            kept_ref[here, :] = jnp.where(first, low, high)
            sent_ref[here, :] = jnp.where(first, high, low).astype(BF)


def chip_kernel(place_ref, recv_ref, kept_ref, span_ref, reach_ref, sent_ref, other_ref):
    other = recv_ref[1024:1056, :].astype(F32) + recv_ref[1056:, :].astype(F32)
    other_ref[...] = other
    first = place_ref[1] == 0
    mine = span_ref[...]
    both = jnp.where(first, mine, other) + reach_ref[16:17, :] * jnp.where(first, other, mine)
    for z in range(16):
        here = slice(z * 64, (z + 1) * 64)
        sent_ref[z, :32, :] = (both * reach_ref[z : z + 1, :]).astype(BF)
        sent_ref[z, 32:, :] = (kept_ref[here, :] + recv_ref[here, :].astype(F32)).astype(BF)


def backward_kernel(
    place_ref,
    later_ref,
    other_ref,
    reach_ref,
    grad_ref,
    entering_ref,
    q_ref,
    k_ref,
    v_ref,
    decay_ref,
    gp_ref,
    gq_ref,
    gk_ref,
    gv_ref,
    gd_ref,
):
    key_mask, val_mask, own = head_masks()
    sums = later_ref[0].astype(F32)
    for z in range(1, 16):
        sums = sums + later_ref[z].astype(F32)
    gp_ref[...] = sums[32:]
    packed = sums[:32]
    packed = jnp.where(place_ref[1] == 0, reach_ref[17:18, :] * packed + other_ref[...], packed)
    state_grad = opened_state(packed, own)
    grad = grad_ref[...]
    queries = q_ref[...].astype(F32).T
    keys = k_ref[...].astype(F32).T * SCALE
    values = v_ref[...].astype(F32)
    cumulative = block_sums(decay_ref[...].T)
    closing = closings(cumulative)
    grow, shrink = jnp.exp(cumulative), jnp.exp(-cumulative)
    rest = jnp.exp(per_block(closing) - cumulative)
    scaled_q, scaled_k, tail = queries * grow, keys * shrink, keys * rest
    causal = causal_blocks()
    value_grad = jnp.zeros((TOK, 128), F32)
    query_grad = jnp.zeros((TOK, 64), F32)
    key_grad = jnp.zeros((TOK, 64), F32)
    for h in range(2):
        scores = scores_of(scaled_q, scaled_k, key_mask[h], causal)
        score_grad = jnp.where(causal, mm(grad * val_mask[h], values, NT), 0.0)
        value_grad = value_grad + mm(scores, grad * val_mask[h], TN)
        query_grad = query_grad + mm(score_grad, scaled_k * key_mask[h])
        key_grad = key_grad + mm(score_grad, scaled_q * key_mask[h], TN)
    carried_v, carried_q, tail_grad, close_grad = ([None] * NBLK for _ in range(4))
    for n in reversed(range(NBLK)):
        here = slice(n * BLOCK, (n + 1) * BLOCK)
        entering = entering_ref[n]
        decay_out = jnp.exp(closing[n])
        carried_v[n] = mm(tail[here], state_grad, NT)
        carried_q[n] = mm(grad[here], entering)
        tail_grad[n] = mm(values[here], state_grad)
        close_grad[n] = decay_out * jnp.sum(state_grad * entering, axis=0, keepdims=True) + jnp.sum(
            tail_grad[n] * tail[here], axis=0, keepdims=True
        )
        state_grad = decay_out * state_grad + mm(grad[here], scaled_q[here], TN) * own
    value_grad = value_grad + jnp.concatenate(carried_v, axis=0)
    query_grad = query_grad + jnp.concatenate(carried_q, axis=0)
    tail_grad = jnp.concatenate(tail_grad, axis=0)
    change = query_grad * scaled_q - key_grad * scaled_k - tail_grad * tail
    row, col = iota((TOK, TOK), 0), iota((TOK, TOK), 1)
    onward = ((row // BLOCK == col // BLOCK) & (col >= row)).astype(F32)
    gd_ref[...] = (mm_exact(onward, change) + per_block(close_grad)).T
    gq_ref[...] = (query_grad * grow).T.astype(BF)
    gk_ref[...] = ((key_grad * shrink + tail_grad * rest) * SCALE).T.astype(BF)
    gv_ref[...] = value_grad.astype(BF)


def exchanged(blocks, axis):
    return lax.all_to_all(blocks, axis, split_axis=0, concat_axis=0, tiled=True)


def ring_step(step):
    pairs = []
    for t in range(N_TP):
        y, x = t // 4, t % 4
        pairs.append((t, 4 * y + (x + step) % 4))
        pairs.append((N_TP + t, N_TP + 4 * ((y + step) % 4) + x))
    return pairs


def passed_on(array, step):
    return lax.ppermute(array, ("sp_1", "tp"), ring_step(step))


def body(
    moe_input,
    out_grad,
    routes,
    route_weight,
    w_gate,
    w_up,
    w_down,
    w_out,
    queries,
    key_rows,
    value_rows,
    log_decay,
):
    q_t, k_t, decay_t = queries.T, key_rows.T, log_decay.T
    place = jnp.stack(
        [lax.axis_index(SP), lax.axis_index("sp_1"), lax.axis_index("sp_0")]
    ).astype(jnp.int32)

    sent, pick = call(
        dispatch_kernel,
        [((N_SP, 2 * PAD, 128), BF), ((SLOTS, TOK), BF)],
        routes.T,
        route_weight.T,
        moe_input,
        out_grad,
        k_t,
        value_rows,
        decay_t,
    )
    recv = exchanged(sent, SP)
    own_a, own_b = call(
        pack_kernel,
        [((LOT, 128), BF), ((LOT, 128), BF)],
        w_gate[0],
        w_up[0],
        w_down[0],
        near_out=(0, 1),
    )
    left_a = passed_on(own_a, 1)
    right_b = passed_on(own_b, -1)
    left_b = passed_on(own_b, 1)
    right_a = passed_on(own_a, -1)
    far_a = passed_on(left_a, 1)
    far_b = passed_on(right_b, -1)
    weights = (own_a, own_b, left_a, left_b, right_a, right_b, far_a, far_b)
    copies, states, reach = call(
        copies_kernel,
        [((N_TP, 2 * PART, 128), BF), ((N_SP, 128), F32), ((24, 128), F32)],
        place,
        recv,
        scratch=[pltpu.VMEM((2 * ROWS, 128), F32), pltpu.VMEM((4, 2 * PART, 128), BF)],
        smem=(0,),
        near=(1,),
        near_out=(0,),
    )
    rows = exchanged(copies, "tp")
    (turned,) = call(turned_kernel, [((TOK, SLOTS), BF)], pick, after=(copies,))
    partial_rows, grads, hidden = call(
        partial_kernel,
        [((N_TP, PART, 128), BF), ((PART, 1024), BF), ((PART, 512), BF)],
        rows,
        *weights,
        near=tuple(range(9)),
        near_out=(1, 2),
    )
    arrived = exchanged(partial_rows, "tp")
    own_grad_a, own_grad_b, to_left, to_right, left_lot, right_lot = call(
        weight_grads_kernel,
        2 * [((LOT, 128), F32)] + 2 * [((2 * LOT, 128), BF)] + 2 * [((LOT, 128), BF)],
        rows,
        grads,
        hidden,
        near=(0, 1, 2),
        near_out=(2, 3),
    )
    from_left = passed_on(to_right, 1)
    from_right = passed_on(to_left, -1)
    lot_left, lot_right = call(
        relay_kernel,
        2 * [((LOT, 128), BF)],
        left_lot,
        right_lot,
        from_right,
        from_left,
        near=(2, 3),
        near_out=(0, 1),
    )
    last_a = passed_on(lot_right, 1)
    last_b = passed_on(lot_left, -1)
    (returned,) = call(
        row_sum_kernel,
        [((N_SP, PAD, 128), BF)],
        place,
        arrived,
        states,
        smem=(0,),
        near=(1,),
        scratch=[pltpu.VMEM((ROWS + 8, 128), F32)],
    )
    back = exchanged(returned, SP)
    (residual,) = call(residual_kernel, [((N_TP, TOK, 128), BF)], back, turned, out_grad, near=(0,))
    full_grad = exchanged(residual, "tp")
    mixer_out, entering = call(
        forward_kernel,
        [((TOK, 128), BF), ((NBLK, 128, 64), F32)],
        back,
        q_t,
        k_t,
        value_rows,
        decay_t,
        near=(0,),
        near_out=(0,),
        after=(residual,),
    )
    mixer_grad, span_grad, to_other, kept = call(
        mixer_grad_kernel,
        [((TOK, 128), F32), ((32, 128), F32), ((1088, 128), BF), ((1024, 128), F32)],
        place,
        full_grad,
        w_out,
        mixer_out,
        q_t,
        decay_t,
        smem=(0,),
        near=(1, 3),
        near_out=(0, 1, 2, 3),
    )
    from_other = lax.ppermute(to_other, "sp_1", [(0, 1), (1, 0)])
    chip_sent, other_grad = call(
        chip_kernel,
        [((16, 96, 128), BF), ((32, 128), F32)],
        place,
        from_other,
        kept,
        span_grad,
        reach,
        smem=(0,),
        near=(1, 2, 3),
        near_out=(1,),
    )
    later = exchanged(chip_sent, "sp_0")
    grad_proj, gq, gk, gv, gd = call(
        backward_kernel,
        [((64, 128), F32), ((64, TOK), BF), ((64, TOK), BF), ((TOK, 128), BF), ((64, TOK), F32)],
        place,
        later,
        other_grad,
        reach,
        mixer_grad,
        entering,
        q_t,
        k_t,
        value_rows,
        decay_t,
        smem=(0,),
        near=(1, 2, 4),
    )
    gate_part, up_part, down_part = call(
        grad_sum_kernel,
        [((2048, 128), BF), ((2048, 128), BF), ((128, 2048), BF)],
        own_grad_a,
        own_grad_b,
        from_right,
        from_left,
        last_a,
        last_b,
        near=(2, 3, 4, 5),
        after=(residual,),
    )
    return (gate_part[None], up_part[None], down_part[None], grad_proj, gq.T, gk.T, gv, gd.T)


def solution(mesh):
    split = Mesh(mesh.devices.reshape(16, 2, mesh.shape["tp"]), ("sp_0", "sp_1", "tp"))
    placed = (
        P(SP, "tp"),
        P(SP, "tp"),
        P(SP, None),
        P(SP, None),
        P(SP, None, "tp"),
        P(SP, None, "tp"),
        P(SP, "tp", None),
        P(None, "tp"),
        P(SP, "tp"),
        P(SP, "tp"),
        P(SP, "tp"),
        P(SP, "tp"),
    )
    return jax.shard_map(
        body,
        mesh=split,
        in_specs=placed,
        out_specs=(
            P(SP, None, "tp"),
            P(SP, None, "tp"),
            P(SP, "tp", None),
            P(SP, "tp"),
            P(SP, "tp"),
            P(SP, "tp"),
            P(SP, "tp"),
            P(SP, "tp"),
        ),
        check_vma=False,
    )
```

```python
import jax
import jax.numpy as jnp
from jax import lax
from jax.experimental import pallas as pl
from jax.experimental.pallas import tpu as pltpu
from jax.sharding import Mesh
from jax.sharding import PartitionSpec as P


KEY_CHANNELS = 32
VAL_DIM = 64
TOP = 2
BLOCK = 64
CAP = 20
PAD = 24
SP = ("sp_0", "sp_1")
N_SP = 32
N_TP = 16
TOK = 256
ROWS = N_SP * CAP
SLOTS = N_SP * PAD
PART = ROWS // 4
LOT = 3 * 1024
NBLK = TOK // BLOCK
BF = jnp.bfloat16
F32 = jnp.float32
HI = lax.Precision.HIGHEST
SCALE = KEY_CHANNELS ** (-0.5)

NN = (((1,), (0,)), ((), ()))
NT = (((1,), (1,)), ((), ()))
TN = (((0,), (0,)), ((), ()))


def mm(a, b, dims=NN):
    return lax.dot_general(a.astype(BF), b.astype(BF), dims, preferred_element_type=F32)


def mm_exact(a, b, dims=NN):
    return lax.dot_general(a, b, dims, precision=HI, preferred_element_type=F32)


def iota(shape, dim):
    return lax.broadcasted_iota(jnp.int32, shape, dim)


def call(fn, outs, *args, scratch=(), smem=(), near=(), near_out=(), after=(), raw=()):
    spaces = [pltpu.VMEM if k in near else pltpu.HBM for k in range(len(args))]
    args = [
        a if k in smem else pltpu.with_memory_space_constraint(a, spaces[k])
        for k, a in enumerate(args)
    ]
    after = [pltpu.with_memory_space_constraint(a, pltpu.HBM) for a in after]
    count = len(args)

    def run(*refs):
        fn(*refs[:count], *refs[count + len(after) :])

    return pl.pallas_call(
        run,
        out_shape=tuple(
            (pltpu.VMEM if k in near_out else pltpu.HBM)(s, d) for k, (s, d) in enumerate(outs)
        ),
        in_specs=[
            pl.BlockSpec(
                memory_space=pltpu.SMEM if k in smem else pltpu.HBM if k in raw else pltpu.VMEM
            )
            for k in range(count)
        ]
        + [pl.BlockSpec(memory_space=pltpu.HBM) for _ in after],
        out_specs=tuple(pl.BlockSpec(memory_space=pltpu.VMEM) for _ in outs),
        scratch_shapes=scratch,
        compiler_params=pltpu.CompilerParams(vmem_limit_bytes=24 * 1024 * 1024),
    )(*args, *after)


def head_masks():
    key_lane = iota((1, 64), 1) // KEY_CHANNELS
    val_lane = iota((1, 128), 1) // VAL_DIM
    keys = [(key_lane == h).astype(F32) for h in range(2)]
    vals = [(val_lane == h).astype(F32) for h in range(2)]
    own = (iota((128, 64), 0) // VAL_DIM == iota((128, 64), 1) // KEY_CHANNELS).astype(F32)
    return keys, vals, own


def packed_state(state):
    both = state[:64] + state[64:]
    return jnp.concatenate([both[:32], both[32:]], axis=1)


def opened_state(packed, own):
    both = jnp.concatenate([packed[:, :64], packed[:, 64:]], axis=0)
    return jnp.concatenate([both, both], axis=0) * own


def picked_sums(mask, values):
    high = values.astype(BF).astype(F32)
    middle = (values - high).astype(BF).astype(F32)
    sums = mm(mask, jnp.concatenate([high, middle, values - high - middle], axis=1))
    return sums[:, :64] + sums[:, 64:128] + sums[:, 128:192]


def block_sums(decay):
    row, col = iota((TOK, TOK), 0), iota((TOK, TOK), 1)
    within = ((row // BLOCK == col // BLOCK) & (col <= row)).astype(F32)
    return picked_sums(within, decay)


def whole_sums(cumulative):
    offset, parts = jnp.zeros((1, 64), F32), []
    for n in range(NBLK):
        block = cumulative[n * BLOCK : (n + 1) * BLOCK]
        parts.append(block + offset)
        offset = offset + block[BLOCK - 1 :]
    return jnp.concatenate(parts, axis=0), offset


def closings(cumulative):
    return [cumulative[(n + 1) * BLOCK - 1 : (n + 1) * BLOCK] for n in range(NBLK)]


def per_block(rows):
    return jnp.concatenate([jnp.broadcast_to(r, (BLOCK, r.shape[1])) for r in rows], axis=0)


def two_parts(values):
    high = values.astype(BF).astype(F32)
    return high, values - high


def dispatch_kernel(
    routes_ref, weight_ref, x_ref, g_ref, k_ref, v_ref, decay_ref, sent_ref, pick_ref
):
    routes = routes_ref[...]
    expert = iota((N_SP, TOK), 0)
    hot = [(expert == routes[j : j + 1, :]) for j in range(TOP)]
    both = (hot[0] | hot[1]).astype(F32)
    before = (iota((TOK, TOK), 0) < iota((TOK, TOK), 1)).astype(F32)
    place = mm(both, before)
    owner, row = iota((SLOTS, N_SP), 0) // PAD, iota((SLOTS, N_SP), 0) % PAD
    mine = owner == iota((SLOTS, N_SP), 1)
    spread = mine.astype(F32)
    slot_place = (iota((SLOTS, TOK), 0) % PAD).astype(F32)
    picks = [(mm(spread, jnp.where(h, place, -1.0)) == slot_place).astype(F32) for h in hot]
    pick = picks[0] + picks[1]
    pick_ref[...] = pick.astype(BF)

    _, _, own = head_masks()
    keys = k_ref[...].astype(F32).T * SCALE
    so_far, total = whole_sums(block_sums(decay_ref[...].T))
    state = mm(v_ref[...], keys * jnp.exp(total - so_far), TN) * own
    state_high, state_low = two_parts(packed_state(state))
    total_row = jnp.concatenate(two_parts(total), axis=1)

    first = (mine & (row == CAP)).astype(F32)
    second = (mine & (row == CAP + 1)).astype(F32)
    chosen = jnp.concatenate([pick, first, second], axis=1)
    rows = jnp.concatenate([x_ref[...].astype(F32), state_high, state_low], axis=0)
    sent_ref[:, :PAD, :] = mm(chosen, rows).astype(BF).reshape(N_SP, PAD, 128)

    grad = g_ref[...].astype(F32)
    weight = jnp.concatenate([weight_ref[...], jnp.zeros((6, TOK), F32)], axis=0).T
    rows = [(weight[:, j : j + 1] * grad).astype(BF) for j in range(TOP)]
    sent = mm(picks[0], rows[0]) + mm(picks[1], rows[1])
    sent = jnp.where(iota((SLOTS, 128), 0) % PAD == CAP, total_row, sent)
    sent_ref[:, PAD:, :] = sent.astype(BF).reshape(N_SP, PAD, 128)


def turned_kernel(pick_ref, out_ref):
    out_ref[...] = pick_ref[...].astype(F32).T.astype(BF)


def quarter_of(place_ref, k):
    return jnp.where(place_ref[1] == 0, k % 4, k // 4)


def copies_kernel(place_ref, recv_ref, out_ref, states_ref, reach_ref, packed, rounded):
    for e in range(N_SP):
        block = recv_ref[e].astype(F32)
        at = (e // 8) * 2 * PART + (e % 8) * CAP
        packed[at : at + CAP, :] = block[:CAP]
        packed[at + PART : at + PART + CAP, :] = block[PAD : PAD + CAP]
    for q in range(4):
        rounded[q] = packed[q * 2 * PART : (q + 1) * 2 * PART, :].astype(BF)
    for k in range(N_TP):
        out_ref[k] = rounded[quarter_of(place_ref, k)]
    chip = place_ref[2]
    totals = [recv_ref[s, PAD + CAP : PAD + CAP + 1, :].astype(F32) for s in range(N_SP)]
    totals = jnp.concatenate(totals, axis=0)
    totals = totals[:, :64] + totals[:, 64:]
    double = jnp.concatenate([totals, totals], axis=1)
    decays = jnp.exp(double)
    state = jnp.zeros((1, 128), F32)
    for s in range(N_SP):
        states_ref[s : s + 1, :] = state
        pair = recv_ref[s, CAP : CAP + 2, :].astype(F32)
        state = decays[s : s + 1] * state + pair[0:1] + pair[1:2]
    target, between = iota((16, N_SP), 0), iota((16, N_SP), 1)
    passed = ((between >= 2 * target + 2) & (between < 2 * chip)).astype(F32)
    reach = jnp.exp(mm_exact(passed, double))
    reach_ref[:16, :] = jnp.where(iota((16, 128), 0) < chip, reach, 0.0)
    here = iota((N_SP, 128), 0)
    even = jnp.sum(jnp.where(here == 2 * chip, decays, 0.0), axis=0, keepdims=True)
    odd = jnp.sum(jnp.where(here == 2 * chip + 1, decays, 0.0), axis=0, keepdims=True)
    reach_ref[16:, :] = jnp.concatenate([even, odd, jnp.zeros((6, 128), F32)], axis=0)


def pack_kernel(wg_ref, wu_ref, wd_ref, a_ref, b_ref):
    a_ref[:2048, :] = wg_ref[...]
    a_ref[2048:, :] = wu_ref[:1024, :]
    b_ref[:1024, :] = wu_ref[1024:, :]
    for k in range(N_TP):
        b_ref[1024 + k * 128 : 1152 + k * 128, :] = wd_ref[:, k * 128 : (k + 1) * 128]


def wide(ref, at, size):
    return jnp.concatenate([ref[k, at : at + size, :] for k in range(N_TP)], axis=1)


def partial_kernel(rows_ref, *refs):
    lots, (part_ref, grads_ref, hidden_ref, held, done) = refs[:8], refs[8:]
    copies = [pltpu.make_async_copy(lots[i], held.at[i], done.at[i]) for i in range(8)]
    for copy in copies:
        copy.start()
    x, g = wide(rows_ref, 0, PART), wide(rows_ref, PART, PART)
    for b in range(4):
        copies[2 * b].wait()
        copies[2 * b + 1].wait()
        gate_weight = held[2 * b, :2048, :]
        up_weight = jnp.concatenate([held[2 * b, 2048:, :], held[2 * b + 1, :1024, :]], axis=0)
        blocks = [held[2 * b + 1, 1024 + k * 128 : 1152 + k * 128, :] for k in range(N_TP)]
        pre = mm(x, jnp.concatenate([gate_weight, up_weight], axis=1))
        upper = mm(g, jnp.concatenate(blocks, axis=1), NT)
        gate_pre, up_pre = pre[:, :128], pre[:, 128:]
        sigmoid = jax.nn.sigmoid(gate_pre)
        activated = gate_pre * sigmoid
        hidden_ref[:, 128 * b : 128 * b + 128] = (activated * up_pre).astype(BF)
        gate = upper * up_pre * sigmoid * (1.0 + gate_pre * (1.0 - sigmoid))
        grads_ref[:, 256 * b : 256 * b + 128] = gate.astype(BF)
        grads_ref[:, 256 * b + 128 : 256 * b + 256] = (upper * activated).astype(BF)
    grads = grads_ref[...]

    def up_rows(b, at):
        if at < 1024:
            return held[2 * b, 2048 + at : 2304 + at, :]
        return held[2 * b + 1, at - 1024 : at - 768, :]

    for k in range(0, N_TP, 2):
        at = k * 128
        weight = []
        for b in range(4):
            weight += [held[2 * b, at : at + 256, :], up_rows(b, at)]
        part = mm(grads, jnp.concatenate(weight, axis=1), NT).astype(BF)
        part_ref[k] = part[:, :128]
        part_ref[k + 1] = part[:, 128:]


def weight_grads_kernel(rows_ref, grads_ref, hidden_ref, *out_refs):
    grads = grads_ref[...]
    hidden = hidden_ref[...]
    for k in range(0, N_TP, 2):
        x = jnp.concatenate([rows_ref[k, :PART, :], rows_ref[k + 1, :PART, :]], axis=1)
        g = jnp.concatenate([rows_ref[k, PART:, :], rows_ref[k + 1, PART:, :]], axis=1)
        both = mm(x, grads, TN)
        down = mm(hidden, g, TN)
        at = k * 128
        for b, (a_part, b_part) in enumerate(lots_of(out_refs)):
            (a_ref, a_at), (b_ref, b_at) = a_part, b_part
            kind = a_ref.dtype
            up = both[:, 256 * b + 128 : 256 * b + 256].astype(kind)
            a_ref[a_at + at : a_at + at + 256, :] = both[:, 256 * b : 256 * b + 128].astype(kind)
            if k < N_TP // 2:
                a_ref[a_at + 2048 + at : a_at + 2304 + at, :] = up
            else:
                b_ref[b_at + at - 1024 : b_at + at - 768, :] = up
            for n in range(2):
                block = b_at + 1024 + at + n * 128
                b_ref[block : block + 128, :] = down[
                    128 * b : 128 * b + 128, n * 128 : (n + 1) * 128
                ].astype(kind)


def lots_of(refs):
    own_a, own_b, to_left, to_right, left_b, right_a = refs
    return (
        ((own_a, 0), (own_b, 0)),
        ((to_left, 0), (left_b, 0)),
        ((right_a, 0), (to_right, LOT)),
        ((to_right, 0), (to_left, LOT)),
    )


def relay_kernel(left_b_ref, right_a_ref, from_right_ref, from_left_ref, to_left_ref, to_right_ref):
    far_a, far_b = from_left_ref[:LOT, :].astype(F32), from_right_ref[LOT:, :].astype(F32)
    to_right_ref[...] = (right_a_ref[...].astype(F32) + far_a).astype(BF)
    to_left_ref[...] = (left_b_ref[...].astype(F32) + far_b).astype(BF)


def grad_sum_kernel(
    own_a_ref,
    own_b_ref,
    from_right_ref,
    from_left_ref,
    last_a_ref,
    last_b_ref,
    gate_ref,
    up_ref,
    down_ref,
):
    def total(at, size):
        if at < LOT:
            refs = (own_a_ref, from_right_ref, last_a_ref)
            rows = [r[at : at + size, :].astype(F32) for r in refs]
        else:
            own, last = (r[at - LOT : at - LOT + size, :] for r in (own_b_ref, last_b_ref))
            rows = [own, from_left_ref[at : at + size, :].astype(F32), last.astype(F32)]
        return (rows[0] + rows[1] + rows[2]).astype(BF)

    for k in range(N_TP):
        here = slice(k * 128, (k + 1) * 128)
        gate_ref[here, :] = total(k * 128, 128)
        up_ref[here, :] = total(2048 + k * 128, 128)
        down_ref[:, here] = total(4096 + k * 128, 128)


def row_sum_kernel(place_ref, part_ref, states_ref, out_ref, total):
    for q in range(4):
        acc = jnp.zeros((PART, 128), F32)
        for j in range(4):
            source = jnp.where(place_ref[1] == 0, 4 * j + q, 4 * q + j)
            acc = acc + part_ref[source].astype(F32)
        total[q * PART : (q + 1) * PART, :] = acc
    total[ROWS:, :] = jnp.zeros((8, 128), F32)
    row = iota((PAD, 128), 0)
    high, low = two_parts(states_ref[...])
    for e in range(N_SP):
        rows = jnp.where(row < CAP, total[e * CAP : e * CAP + PAD, :], 0.0)
        rows = jnp.where(row == CAP, high[e : e + 1], rows)
        rows = jnp.where(row == CAP + 1, low[e : e + 1], rows)
        out_ref[e] = rows.astype(BF)


def residual_kernel(back_ref, turned_ref, g_ref, out_ref):
    routed = mm(turned_ref[...], back_ref[...].reshape(SLOTS, 128))
    residual = (g_ref[...].astype(F32) + routed).astype(BF)
    for k in range(N_TP):
        out_ref[k] = residual


def scores_of(queries, keys, mask, causal):
    return jnp.where(causal, mm(queries * mask, keys, NT), 0.0)


def causal_blocks():
    row, col = iota((TOK, TOK), 0), iota((TOK, TOK), 1)
    return (row // BLOCK == col // BLOCK) & (col <= row)


def forward_kernel(back_ref, q_ref, k_ref, v_ref, decay_ref, out_ref, entering_ref):
    key_mask, val_mask, own = head_masks()
    rows = [back_ref[s, CAP : CAP + 2, :].astype(F32) for s in range(N_SP)]
    packed = jnp.concatenate([r[0:1] + r[1:2] for r in rows], axis=0)
    state = opened_state(packed, own)
    queries = q_ref[...].astype(F32).T
    keys = k_ref[...].astype(F32).T * SCALE
    values = v_ref[...].astype(F32)
    cumulative = block_sums(decay_ref[...].T)
    closing = closings(cumulative)
    scaled_q = queries * jnp.exp(cumulative)
    scaled_k = keys * jnp.exp(-cumulative)
    tail = keys * jnp.exp(per_block(closing) - cumulative)
    causal = causal_blocks()
    within = jnp.zeros((TOK, 128), F32)
    for h in range(2):
        scores = scores_of(scaled_q, scaled_k, key_mask[h], causal)
        within = within + mm(scores, values * val_mask[h])
    for n in range(NBLK):
        here = slice(n * BLOCK, (n + 1) * BLOCK)
        entering_ref[n] = state
        out_ref[here, :] = (within[here] + mm(scaled_q[here], state, NT)).astype(BF)
        state = jnp.exp(closing[n]) * state + mm(values[here], tail[here], TN) * own


def mixer_grad_kernel(
    place_ref, full_ref, w_ref, mixed_ref, q_ref, decay_ref, grad_ref, span_ref, sent_ref, kept_ref
):
    _, _, own = head_masks()
    grad = mm(wide(full_ref, 0, TOK), w_ref[...])
    grad_ref[...] = grad
    so_far, _ = whole_sums(block_sums(decay_ref[...].T))
    scaled = q_ref[...].astype(F32).T * jnp.exp(so_far)
    packed = packed_state(mm(grad, scaled, TN) * own)
    span_ref[...] = packed
    high, low = two_parts(packed)
    sent_ref[1024:1056, :] = high.astype(BF)
    sent_ref[1056:, :] = low.astype(BF)
    mixed = mixed_ref[...]
    first = place_ref[1] == 0
    for k in range(0, N_TP, 2):
        rows = jnp.concatenate([full_ref[k], full_ref[k + 1]], axis=1)
        part = mm(rows, mixed, TN)
        for n in range(2):
            low, high = part[n * 128 : n * 128 + 64], part[n * 128 + 64 : n * 128 + 128]
            here = slice((k + n) * 64, (k + n + 1) * 64)
            kept_ref[here, :] = jnp.where(first, low, high)
            sent_ref[here, :] = jnp.where(first, high, low).astype(BF)


def chip_kernel(place_ref, recv_ref, kept_ref, span_ref, reach_ref, sent_ref, other_ref):
    other = recv_ref[1024:1056, :].astype(F32) + recv_ref[1056:, :].astype(F32)
    other_ref[...] = other
    first = place_ref[1] == 0
    mine = span_ref[...]
    both = jnp.where(first, mine, other) + reach_ref[16:17, :] * jnp.where(first, other, mine)
    for z in range(16):
        here = slice(z * 64, (z + 1) * 64)
        sent_ref[z, :32, :] = (both * reach_ref[z : z + 1, :]).astype(BF)
        sent_ref[z, 32:, :] = (kept_ref[here, :] + recv_ref[here, :].astype(F32)).astype(BF)


def local_backward_kernel(
    grad_ref,
    entering_ref,
    q_ref,
    k_ref,
    v_ref,
    decay_ref,
    gq_ref,
    value_ref,
    keys_ref,
    change_ref,
    tail_ref,
    reach_ref,
    rest_ref,
    leave_ref,
):
    key_mask, val_mask, own = head_masks()
    grad = grad_ref[...]
    queries = q_ref[...].astype(F32).T
    keys = k_ref[...].astype(F32).T * SCALE
    values = v_ref[...].astype(F32)
    cumulative = block_sums(decay_ref[...].T)
    closing = closings(cumulative)
    grow, shrink = jnp.exp(cumulative), jnp.exp(-cumulative)
    rest = jnp.exp(per_block(closing) - cumulative)
    scaled_q, scaled_k, tail = queries * grow, keys * shrink, keys * rest
    causal = causal_blocks()
    value_grad = jnp.zeros((TOK, 128), F32)
    query_grad = jnp.zeros((TOK, 64), F32)
    key_grad = jnp.zeros((TOK, 64), F32)
    for h in range(2):
        scores = scores_of(scaled_q, scaled_k, key_mask[h], causal)
        score_grad = jnp.where(causal, mm(grad * val_mask[h], values, NT), 0.0)
        value_grad = value_grad + mm(scores, grad * val_mask[h], TN)
        query_grad = query_grad + mm(score_grad, scaled_k * key_mask[h])
        key_grad = key_grad + mm(score_grad, scaled_q * key_mask[h], TN)
    carried_v, carried_q, tail_grad, close_grad, reach = ([None] * NBLK for _ in range(5))
    state_grad, later = jnp.zeros((128, 64), F32), jnp.zeros((1, 64), F32)
    for n in reversed(range(NBLK)):
        here = slice(n * BLOCK, (n + 1) * BLOCK)
        entering = entering_ref[n]
        decay_out = jnp.exp(closing[n])
        reach[n] = jnp.exp(later)
        later = later + closing[n]
        leave_ref[n : n + 1, :] = jnp.exp(later)
        carried_v[n] = mm(tail[here], state_grad, NT)
        carried_q[n] = mm(grad[here], entering)
        tail_grad[n] = mm(values[here], state_grad)
        close_grad[n] = decay_out * jnp.sum(state_grad * entering, axis=0, keepdims=True) + jnp.sum(
            tail_grad[n] * tail[here], axis=0, keepdims=True
        )
        state_grad = decay_out * state_grad + mm(grad[here], scaled_q[here], TN) * own
    value_ref[...] = value_grad + jnp.concatenate(carried_v, axis=0)
    query_grad = query_grad + jnp.concatenate(carried_q, axis=0)
    tail_grad = jnp.concatenate(tail_grad, axis=0)
    change = query_grad * scaled_q - key_grad * scaled_k - tail_grad * tail
    row, col = iota((TOK, TOK), 0), iota((TOK, TOK), 1)
    onward = ((row // BLOCK == col // BLOCK) & (col >= row)).astype(F32)
    change_ref[...] = picked_sums(onward, change) + per_block(close_grad)
    gq_ref[...] = (query_grad * grow).T.astype(BF)
    keys_ref[...] = (key_grad * shrink + tail_grad * rest) * SCALE
    tail_ref[...] = tail
    reach_ref[...] = per_block(reach)
    rest_ref[...] = rest * SCALE


def backward_kernel(
    place_ref,
    later_ref,
    other_ref,
    chips_ref,
    entering_ref,
    v_ref,
    value_ref,
    keys_ref,
    change_ref,
    tail_ref,
    reach_ref,
    rest_ref,
    leave_ref,
    gp_ref,
    gk_ref,
    gv_ref,
    gd_ref,
):
    _, _, own = head_masks()
    sums = later_ref[0].astype(F32)
    for z in range(1, 16):
        sums = sums + later_ref[z].astype(F32)
    gp_ref[...] = sums[32:]
    packed = sums[:32]
    packed = jnp.where(place_ref[1] == 0, chips_ref[17:18, :] * packed + other_ref[...], packed)
    state_grad = opened_state(packed, own)
    tail, reach = tail_ref[...], reach_ref[...]
    gv_ref[...] = (value_ref[...] + mm(tail * reach, state_grad, NT)).astype(BF)
    tail_grad = mm(v_ref[...], state_grad) * reach
    gk_ref[...] = (keys_ref[...] + tail_grad * rest_ref[...]).T.astype(BF)
    row, col = iota((TOK, TOK), 0), iota((TOK, TOK), 1)
    ahead = ((row // BLOCK == col // BLOCK) & (col < row)).astype(F32)
    passed = [
        leave_ref[n : n + 1, :] * jnp.sum(state_grad * entering_ref[n], axis=0, keepdims=True)
        for n in range(NBLK)
    ]
    change = change_ref[...] + picked_sums(ahead, tail_grad * tail) + per_block(passed)
    gd_ref[...] = change.T


def exchanged(blocks, axis):
    return lax.all_to_all(blocks, axis, split_axis=0, concat_axis=0, tiled=True)


def ring_step(step):
    pairs = []
    for t in range(N_TP):
        y, x = t // 4, t % 4
        pairs.append((t, 4 * y + (x + step) % 4))
        pairs.append((N_TP + t, N_TP + 4 * ((y + step) % 4) + x))
    return pairs


def passed_on(array, step):
    return lax.ppermute(array, ("sp_1", "tp"), ring_step(step))


def body(
    moe_input,
    out_grad,
    routes,
    route_weight,
    w_gate,
    w_up,
    w_down,
    w_out,
    queries,
    key_rows,
    value_rows,
    log_decay,
):
    q_t, k_t, decay_t = queries.T, key_rows.T, log_decay.T
    place = jnp.stack(
        [lax.axis_index(SP), lax.axis_index("sp_1"), lax.axis_index("sp_0")]
    ).astype(jnp.int32)

    sent, pick = call(
        dispatch_kernel,
        [((N_SP, 2 * PAD, 128), BF), ((SLOTS, TOK), BF)],
        routes.T,
        route_weight.T,
        moe_input,
        out_grad,
        k_t,
        value_rows,
        decay_t,
    )
    recv = exchanged(sent, SP)
    own_a, own_b = call(
        pack_kernel, [((LOT, 128), BF), ((LOT, 128), BF)], w_gate[0], w_up[0], w_down[0]
    )
    left_a = passed_on(own_a, 1)
    right_b = passed_on(own_b, -1)
    left_b = passed_on(own_b, 1)
    right_a = passed_on(own_a, -1)
    far_a = passed_on(left_a, 1)
    far_b = passed_on(right_b, -1)
    weights = (own_a, own_b, left_a, left_b, right_a, right_b, far_a, far_b)
    copies, states, reach = call(
        copies_kernel,
        [((N_TP, 2 * PART, 128), BF), ((N_SP, 128), F32), ((24, 128), F32)],
        place,
        recv,
        scratch=[pltpu.VMEM((2 * ROWS, 128), F32), pltpu.VMEM((4, 2 * PART, 128), BF)],
        smem=(0,),
        near=(1,),
        near_out=(0,),
    )
    rows = exchanged(copies, "tp")
    (turned,) = call(turned_kernel, [((TOK, SLOTS), BF)], pick, after=(copies,))
    partial_rows, grads, hidden = call(
        partial_kernel,
        [((N_TP, PART, 128), BF), ((PART, 1024), BF), ((PART, 512), BF)],
        rows,
        *weights,
        scratch=[pltpu.VMEM((8, LOT, 128), BF), pltpu.SemaphoreType.DMA((8,))],
        near=(0,),
        near_out=(1, 2),
        raw=tuple(range(1, 9)),
    )
    arrived = exchanged(partial_rows, "tp")
    own_grad_a, own_grad_b, to_left, to_right, left_lot, right_lot = call(
        weight_grads_kernel,
        2 * [((LOT, 128), F32)] + 2 * [((2 * LOT, 128), BF)] + 2 * [((LOT, 128), BF)],
        rows,
        grads,
        hidden,
        near=(0, 1, 2),
        near_out=(2, 3),
    )
    from_left = passed_on(to_right, 1)
    from_right = passed_on(to_left, -1)
    (returned,) = call(
        row_sum_kernel,
        [((N_SP, PAD, 128), BF)],
        place,
        arrived,
        states,
        near_out=(0,),
        smem=(0,),
        near=(1,),
        scratch=[pltpu.VMEM((ROWS + 8, 128), F32)],
    )
    back = exchanged(returned, SP)
    (residual,) = call(residual_kernel, [((N_TP, TOK, 128), BF)], back, turned, out_grad, near=(0,))
    full_grad = exchanged(residual, "tp")
    lot_left, lot_right = call(
        relay_kernel,
        2 * [((LOT, 128), BF)],
        left_lot,
        right_lot,
        from_right,
        from_left,
        after=(residual,),
        near=(2, 3),
        near_out=(0, 1),
    )
    last_a = passed_on(lot_right, 1)
    last_b = passed_on(lot_left, -1)
    mixer_out, entering = call(
        forward_kernel,
        [((TOK, 128), BF), ((NBLK, 128, 64), F32)],
        back,
        q_t,
        k_t,
        value_rows,
        decay_t,
        near=(0,),
        near_out=(0,),
        after=(residual,),
    )
    mixer_grad, span_grad, to_other, kept = call(
        mixer_grad_kernel,
        [((TOK, 128), F32), ((32, 128), F32), ((1088, 128), BF), ((1024, 128), F32)],
        place,
        full_grad,
        w_out,
        mixer_out,
        q_t,
        decay_t,
        smem=(0,),
        near=(1, 3),
        near_out=(1, 2, 3),
    )
    from_other = lax.ppermute(to_other, "sp_1", [(0, 1), (1, 0)])
    chip_sent, other_grad = call(
        chip_kernel,
        [((16, 96, 128), BF), ((32, 128), F32)],
        place,
        from_other,
        kept,
        span_grad,
        reach,
        smem=(0,),
        near=(1, 2, 3),
    )
    later = exchanged(chip_sent, "sp_0")
    gq, *local = call(
        local_backward_kernel,
        [
            ((64, TOK), BF),
            ((TOK, 128), F32),
            ((TOK, 64), F32),
            ((TOK, 64), F32),
            ((TOK, 64), F32),
            ((TOK, 64), F32),
            ((TOK, 64), F32),
            ((NBLK, 64), F32),
        ],
        mixer_grad,
        entering,
        q_t,
        k_t,
        value_rows,
        decay_t,
        after=(chip_sent,),
    )
    grad_proj, gk, gv, gd = call(
        backward_kernel,
        [((64, 128), F32), ((64, TOK), BF), ((TOK, 128), BF), ((64, TOK), F32)],
        place,
        later,
        other_grad,
        reach,
        entering,
        value_rows,
        *local,
        smem=(0,),
        near=(1,),
    )
    gate_part, up_part, down_part = call(
        grad_sum_kernel,
        [((2048, 128), BF), ((2048, 128), BF), ((128, 2048), BF)],
        own_grad_a,
        own_grad_b,
        from_right,
        from_left,
        last_a,
        last_b,
        near=(2, 3, 4, 5),
        after=(chip_sent,),
    )
    return (gate_part[None], up_part[None], down_part[None], grad_proj, gq.T, gk.T, gv, gd.T)


def solution(mesh):
    split = Mesh(mesh.devices.reshape(16, 2, mesh.shape["tp"]), ("sp_0", "sp_1", "tp"))
    placed = (
        P(SP, "tp"),
        P(SP, "tp"),
        P(SP, None),
        P(SP, None),
        P(SP, None, "tp"),
        P(SP, None, "tp"),
        P(SP, "tp", None),
        P(None, "tp"),
        P(SP, "tp"),
        P(SP, "tp"),
        P(SP, "tp"),
        P(SP, "tp"),
    )
    return jax.shard_map(
        body,
        mesh=split,
        in_specs=placed,
        out_specs=(
            P(SP, None, "tp"),
            P(SP, None, "tp"),
            P(SP, "tp", None),
            P(SP, "tp"),
            P(SP, "tp"),
            P(SP, "tp"),
            P(SP, "tp"),
            P(SP, "tp"),
        ),
        check_vma=False,
    )
```

```python
import jax
import jax.numpy as jnp
from jax import lax
from jax.experimental import pallas as pl
from jax.experimental.pallas import tpu as pltpu
from jax.sharding import Mesh
from jax.sharding import PartitionSpec as P


KEY_CHANNELS = 32
VAL_DIM = 64
TOP = 2
BLOCK = 64
CAP = 20
PAD = 24
SP = ("sp_0", "sp_1")
N_SP = 32
N_TP = 16
TOK = 256
ROWS = N_SP * CAP
SLOTS = N_SP * PAD
PART = ROWS // 4
LOT = 3 * 1024
NBLK = TOK // BLOCK
BF = jnp.bfloat16
F32 = jnp.float32
HI = lax.Precision.HIGHEST
SCALE = KEY_CHANNELS ** (-0.5)

NN = (((1,), (0,)), ((), ()))
NT = (((1,), (1,)), ((), ()))
TN = (((0,), (0,)), ((), ()))


def mm(a, b, dims=NN):
    return lax.dot_general(a.astype(BF), b.astype(BF), dims, preferred_element_type=F32)


def mm_exact(a, b, dims=NN):
    return lax.dot_general(a, b, dims, precision=HI, preferred_element_type=F32)


def iota(shape, dim):
    return lax.broadcasted_iota(jnp.int32, shape, dim)


def call(fn, outs, *args, scratch=(), smem=(), near=(), near_out=(), after=(), raw=()):
    spaces = [pltpu.VMEM if k in near else pltpu.HBM for k in range(len(args))]
    args = [
        a if k in smem else pltpu.with_memory_space_constraint(a, spaces[k])
        for k, a in enumerate(args)
    ]
    after = [pltpu.with_memory_space_constraint(a, pltpu.HBM) for a in after]
    count = len(args)

    def run(*refs):
        fn(*refs[:count], *refs[count + len(after) :])

    return pl.pallas_call(
        run,
        out_shape=tuple(
            (pltpu.VMEM if k in near_out else pltpu.HBM)(s, d) for k, (s, d) in enumerate(outs)
        ),
        in_specs=[
            pl.BlockSpec(
                memory_space=pltpu.SMEM if k in smem else pltpu.HBM if k in raw else pltpu.VMEM
            )
            for k in range(count)
        ]
        + [pl.BlockSpec(memory_space=pltpu.HBM) for _ in after],
        out_specs=tuple(pl.BlockSpec(memory_space=pltpu.VMEM) for _ in outs),
        scratch_shapes=scratch,
        compiler_params=pltpu.CompilerParams(vmem_limit_bytes=24 * 1024 * 1024),
    )(*args, *after)


def head_masks():
    key_lane = iota((1, 64), 1) // KEY_CHANNELS
    val_lane = iota((1, 128), 1) // VAL_DIM
    keys = [(key_lane == h).astype(F32) for h in range(2)]
    vals = [(val_lane == h).astype(F32) for h in range(2)]
    own = (iota((128, 64), 0) // VAL_DIM == iota((128, 64), 1) // KEY_CHANNELS).astype(F32)
    return keys, vals, own


def packed_state(state):
    both = state[:64] + state[64:]
    return jnp.concatenate([both[:32], both[32:]], axis=1)


def opened_state(packed, own):
    both = jnp.concatenate([packed[:, :64], packed[:, 64:]], axis=0)
    return jnp.concatenate([both, both], axis=0) * own


def picked_sums(mask, values):
    high = values.astype(BF).astype(F32)
    middle = (values - high).astype(BF).astype(F32)
    sums = mm(mask, jnp.concatenate([high, middle, values - high - middle], axis=1))
    return sums[:, :64] + sums[:, 64:128] + sums[:, 128:192]


def block_sums(decay):
    row, col = iota((TOK, TOK), 0), iota((TOK, TOK), 1)
    within = ((row // BLOCK == col // BLOCK) & (col <= row)).astype(F32)
    return picked_sums(within, decay)


def whole_sums(cumulative):
    offset, parts = jnp.zeros((1, 64), F32), []
    for n in range(NBLK):
        block = cumulative[n * BLOCK : (n + 1) * BLOCK]
        parts.append(block + offset)
        offset = offset + block[BLOCK - 1 :]
    return jnp.concatenate(parts, axis=0), offset


def closings(cumulative):
    return [cumulative[(n + 1) * BLOCK - 1 : (n + 1) * BLOCK] for n in range(NBLK)]


def per_block(rows):
    return jnp.concatenate([jnp.broadcast_to(r, (BLOCK, r.shape[1])) for r in rows], axis=0)


def two_parts(values):
    high = values.astype(BF).astype(F32)
    return high, values - high


def dispatch_kernel(
    routes_ref, weight_ref, x_ref, g_ref, k_ref, v_ref, decay_ref, sent_ref, pick_ref
):
    routes = routes_ref[...]
    expert = iota((N_SP, TOK), 0)
    hot = [(expert == routes[j : j + 1, :]) for j in range(TOP)]
    both = (hot[0] | hot[1]).astype(F32)
    before = (iota((TOK, TOK), 0) < iota((TOK, TOK), 1)).astype(F32)
    place = mm(both, before)
    owner, row = iota((SLOTS, N_SP), 0) // PAD, iota((SLOTS, N_SP), 0) % PAD
    mine = owner == iota((SLOTS, N_SP), 1)
    spread = mine.astype(F32)
    slot_place = (iota((SLOTS, TOK), 0) % PAD).astype(F32)
    picks = [(mm(spread, jnp.where(h, place, -1.0)) == slot_place).astype(F32) for h in hot]
    pick = picks[0] + picks[1]
    pick_ref[...] = pick.astype(BF)

    _, _, own = head_masks()
    keys = k_ref[...].astype(F32).T * SCALE
    so_far, total = whole_sums(block_sums(decay_ref[...].T))
    state = mm(v_ref[...], keys * jnp.exp(total - so_far), TN) * own
    state_high, state_low = two_parts(packed_state(state))
    total_row = jnp.concatenate(two_parts(total), axis=1)

    first = (mine & (row == CAP)).astype(F32)
    second = (mine & (row == CAP + 1)).astype(F32)
    chosen = jnp.concatenate([pick, first, second], axis=1)
    rows = jnp.concatenate([x_ref[...].astype(F32), state_high, state_low], axis=0)
    sent_ref[:, :PAD, :] = mm(chosen, rows).astype(BF).reshape(N_SP, PAD, 128)

    grad = g_ref[...].astype(F32)
    weight = jnp.concatenate([weight_ref[...], jnp.zeros((6, TOK), F32)], axis=0).T
    rows = [(weight[:, j : j + 1] * grad).astype(BF) for j in range(TOP)]
    sent = mm(picks[0], rows[0]) + mm(picks[1], rows[1])
    sent = jnp.where(iota((SLOTS, 128), 0) % PAD == CAP, total_row, sent)
    sent_ref[:, PAD:, :] = sent.astype(BF).reshape(N_SP, PAD, 128)


def turned_kernel(pick_ref, out_ref):
    out_ref[...] = pick_ref[...].astype(F32).T.astype(BF)


def quarter_of(place_ref, k):
    return jnp.where(place_ref[1] == 0, k % 4, k // 4)


def copies_kernel(place_ref, recv_ref, out_ref, states_ref, reach_ref, packed, rounded):
    for e in range(N_SP):
        block = recv_ref[e].astype(F32)
        at = (e // 8) * 2 * PART + (e % 8) * CAP
        packed[at : at + CAP, :] = block[:CAP]
        packed[at + PART : at + PART + CAP, :] = block[PAD : PAD + CAP]
    for q in range(4):
        rounded[q] = packed[q * 2 * PART : (q + 1) * 2 * PART, :].astype(BF)
    for k in range(N_TP):
        out_ref[k] = rounded[quarter_of(place_ref, k)]
    chip = place_ref[2]
    totals = [recv_ref[s, PAD + CAP : PAD + CAP + 1, :].astype(F32) for s in range(N_SP)]
    totals = jnp.concatenate(totals, axis=0)
    totals = totals[:, :64] + totals[:, 64:]
    double = jnp.concatenate([totals, totals], axis=1)
    decays = jnp.exp(double)
    state = jnp.zeros((1, 128), F32)
    for s in range(N_SP):
        states_ref[s : s + 1, :] = state
        pair = recv_ref[s, CAP : CAP + 2, :].astype(F32)
        state = decays[s : s + 1] * state + pair[0:1] + pair[1:2]
    target, between = iota((16, N_SP), 0), iota((16, N_SP), 1)
    passed = ((between >= 2 * target + 2) & (between < 2 * chip)).astype(F32)
    reach = jnp.exp(mm_exact(passed, double))
    reach_ref[:16, :] = jnp.where(iota((16, 128), 0) < chip, reach, 0.0)
    here = iota((N_SP, 128), 0)
    even = jnp.sum(jnp.where(here == 2 * chip, decays, 0.0), axis=0, keepdims=True)
    odd = jnp.sum(jnp.where(here == 2 * chip + 1, decays, 0.0), axis=0, keepdims=True)
    reach_ref[16:, :] = jnp.concatenate([even, odd, jnp.zeros((6, 128), F32)], axis=0)


def pack_kernel(wg_ref, wu_ref, wd_ref, a_ref, b_ref):
    a_ref[:2048, :] = wg_ref[...]
    a_ref[2048:, :] = wu_ref[:1024, :]
    b_ref[:1024, :] = wu_ref[1024:, :]
    for k in range(N_TP):
        b_ref[1024 + k * 128 : 1152 + k * 128, :] = wd_ref[:, k * 128 : (k + 1) * 128]


def wide(ref, at, size):
    return jnp.concatenate([ref[k, at : at + size, :] for k in range(N_TP)], axis=1)


def partial_kernel(rows_ref, *refs):
    lots, (part_ref, grads_ref, hidden_ref, held, done) = refs[:8], refs[8:]
    copies = [pltpu.make_async_copy(lots[i], held.at[i], done.at[i]) for i in range(8)]
    for copy in copies:
        copy.start()
    x, g = wide(rows_ref, 0, PART), wide(rows_ref, PART, PART)
    for pair in range(2):
        gates, downs = [], []
        for b in (2 * pair, 2 * pair + 1):
            copies[2 * b].wait()
            copies[2 * b + 1].wait()
            gates.append(held[2 * b, :2048, :])
            gates.append(
                jnp.concatenate([held[2 * b, 2048:, :], held[2 * b + 1, :1024, :]], axis=0)
            )
            blocks = [held[2 * b + 1, 1024 + k * 128 : 1152 + k * 128, :] for k in range(N_TP)]
            downs.append(jnp.concatenate(blocks, axis=1))
        pres = mm(x, jnp.concatenate(gates, axis=1))
        uppers = mm(g, jnp.concatenate(downs, axis=0), NT)
        for n in range(2):
            b = 2 * pair + n
            gate_pre, up_pre = pres[:, 256 * n : 256 * n + 128], pres[:, 256 * n + 128 : 256 * n + 256]
            upper = uppers[:, 128 * n : 128 * n + 128]
            sigmoid = jax.nn.sigmoid(gate_pre)
            activated = gate_pre * sigmoid
            hidden_ref[:, 128 * b : 128 * b + 128] = (activated * up_pre).astype(BF)
            gate = upper * up_pre * sigmoid * (1.0 + gate_pre * (1.0 - sigmoid))
            grads_ref[:, 256 * b : 256 * b + 128] = gate.astype(BF)
            grads_ref[:, 256 * b + 128 : 256 * b + 256] = (upper * activated).astype(BF)
    grads = grads_ref[...]

    def up_rows(b, at):
        if at < 1024:
            return held[2 * b, 2048 + at : 2304 + at, :]
        return held[2 * b + 1, at - 1024 : at - 768, :]

    for k in range(0, N_TP, 2):
        at = k * 128
        weight = []
        for b in range(4):
            weight += [held[2 * b, at : at + 256, :], up_rows(b, at)]
        part = mm(grads, jnp.concatenate(weight, axis=1), NT).astype(BF)
        part_ref[k] = part[:, :128]
        part_ref[k + 1] = part[:, 128:]


def weight_grads_kernel(rows_ref, grads_ref, hidden_ref, *out_refs):
    grads = grads_ref[...]
    hidden = hidden_ref[...]
    for k in range(0, N_TP, 2):
        x = jnp.concatenate([rows_ref[k, :PART, :], rows_ref[k + 1, :PART, :]], axis=1)
        g = jnp.concatenate([rows_ref[k, PART:, :], rows_ref[k + 1, PART:, :]], axis=1)
        both = mm(x, grads, TN)
        down = mm(hidden, g, TN)
        at = k * 128
        for b, (a_part, b_part) in enumerate(lots_of(out_refs)):
            (a_ref, a_at), (b_ref, b_at) = a_part, b_part
            kind = a_ref.dtype
            up = both[:, 256 * b + 128 : 256 * b + 256].astype(kind)
            a_ref[a_at + at : a_at + at + 256, :] = both[:, 256 * b : 256 * b + 128].astype(kind)
            if k < N_TP // 2:
                a_ref[a_at + 2048 + at : a_at + 2304 + at, :] = up
            else:
                b_ref[b_at + at - 1024 : b_at + at - 768, :] = up
            for n in range(2):
                block = b_at + 1024 + at + n * 128
                b_ref[block : block + 128, :] = down[
                    128 * b : 128 * b + 128, n * 128 : (n + 1) * 128
                ].astype(kind)


def lots_of(refs):
    own_a, own_b, to_left, to_right, left_b, right_a = refs
    return (
        ((own_a, 0), (own_b, 0)),
        ((to_left, 0), (left_b, 0)),
        ((right_a, 0), (to_right, LOT)),
        ((to_right, 0), (to_left, LOT)),
    )


def relay_kernel(left_b_ref, right_a_ref, from_right_ref, from_left_ref, to_left_ref, to_right_ref):
    far_a, far_b = from_left_ref[:LOT, :].astype(F32), from_right_ref[LOT:, :].astype(F32)
    to_right_ref[...] = (right_a_ref[...].astype(F32) + far_a).astype(BF)
    to_left_ref[...] = (left_b_ref[...].astype(F32) + far_b).astype(BF)


def grad_sum_kernel(
    own_a_ref,
    own_b_ref,
    from_right_ref,
    from_left_ref,
    last_a_ref,
    last_b_ref,
    gate_ref,
    up_ref,
    down_ref,
):
    def total(at, size):
        if at < LOT:
            refs = (own_a_ref, from_right_ref, last_a_ref)
            rows = [r[at : at + size, :].astype(F32) for r in refs]
        else:
            own, last = (r[at - LOT : at - LOT + size, :] for r in (own_b_ref, last_b_ref))
            rows = [own, from_left_ref[at : at + size, :].astype(F32), last.astype(F32)]
        return (rows[0] + rows[1] + rows[2]).astype(BF)

    for k in range(N_TP):
        here = slice(k * 128, (k + 1) * 128)
        gate_ref[here, :] = total(k * 128, 128)
        up_ref[here, :] = total(2048 + k * 128, 128)
        down_ref[:, here] = total(4096 + k * 128, 128)


def row_sum_kernel(place_ref, part_ref, states_ref, out_ref, total):
    for q in range(4):
        acc = jnp.zeros((PART, 128), F32)
        for j in range(4):
            source = jnp.where(place_ref[1] == 0, 4 * j + q, 4 * q + j)
            acc = acc + part_ref[source].astype(F32)
        total[q * PART : (q + 1) * PART, :] = acc
    total[ROWS:, :] = jnp.zeros((8, 128), F32)
    row = iota((PAD, 128), 0)
    high, low = two_parts(states_ref[...])
    for e in range(N_SP):
        rows = jnp.where(row < CAP, total[e * CAP : e * CAP + PAD, :], 0.0)
        rows = jnp.where(row == CAP, high[e : e + 1], rows)
        rows = jnp.where(row == CAP + 1, low[e : e + 1], rows)
        out_ref[e] = rows.astype(BF)


def residual_kernel(back_ref, turned_ref, g_ref, out_ref):
    routed = mm(turned_ref[...], back_ref[...].reshape(SLOTS, 128))
    residual = (g_ref[...].astype(F32) + routed).astype(BF)
    for k in range(N_TP):
        out_ref[k] = residual


def scores_of(queries, keys, mask, causal):
    return jnp.where(causal, mm(queries * mask, keys, NT), 0.0)


def causal_blocks():
    row, col = iota((TOK, TOK), 0), iota((TOK, TOK), 1)
    return (row // BLOCK == col // BLOCK) & (col <= row)


def forward_kernel(back_ref, q_ref, k_ref, v_ref, decay_ref, out_ref, entering_ref):
    key_mask, val_mask, own = head_masks()
    rows = [back_ref[s, CAP : CAP + 2, :].astype(F32) for s in range(N_SP)]
    packed = jnp.concatenate([r[0:1] + r[1:2] for r in rows], axis=0)
    state = opened_state(packed, own)
    queries = q_ref[...].astype(F32).T
    keys = k_ref[...].astype(F32).T * SCALE
    values = v_ref[...].astype(F32)
    cumulative = block_sums(decay_ref[...].T)
    closing = closings(cumulative)
    scaled_q = queries * jnp.exp(cumulative)
    scaled_k = keys * jnp.exp(-cumulative)
    tail = keys * jnp.exp(per_block(closing) - cumulative)
    causal = causal_blocks()
    within = jnp.zeros((TOK, 128), F32)
    for h in range(2):
        scores = scores_of(scaled_q, scaled_k, key_mask[h], causal)
        within = within + mm(scores, values * val_mask[h])
    for n in range(NBLK):
        here = slice(n * BLOCK, (n + 1) * BLOCK)
        entering_ref[n] = state
        out_ref[here, :] = (within[here] + mm(scaled_q[here], state, NT)).astype(BF)
        state = jnp.exp(closing[n]) * state + mm(values[here], tail[here], TN) * own


def mixer_grad_kernel(
    place_ref, full_ref, w_ref, mixed_ref, q_ref, decay_ref, grad_ref, span_ref, sent_ref, kept_ref
):
    _, _, own = head_masks()
    grad = mm(wide(full_ref, 0, TOK), w_ref[...])
    grad_ref[...] = grad
    so_far, _ = whole_sums(block_sums(decay_ref[...].T))
    scaled = q_ref[...].astype(F32).T * jnp.exp(so_far)
    packed = packed_state(mm(grad, scaled, TN) * own)
    span_ref[...] = packed
    high, low = two_parts(packed)
    sent_ref[1024:1056, :] = high.astype(BF)
    sent_ref[1056:, :] = low.astype(BF)
    mixed = mixed_ref[...]
    first = place_ref[1] == 0
    for k in range(0, N_TP, 2):
        rows = jnp.concatenate([full_ref[k], full_ref[k + 1]], axis=1)
        part = mm(rows, mixed, TN)
        for n in range(2):
            low, high = part[n * 128 : n * 128 + 64], part[n * 128 + 64 : n * 128 + 128]
            here = slice((k + n) * 64, (k + n + 1) * 64)
            kept_ref[here, :] = jnp.where(first, low, high)
            sent_ref[here, :] = jnp.where(first, high, low).astype(BF)


def chip_kernel(place_ref, recv_ref, kept_ref, span_ref, reach_ref, sent_ref, other_ref):
    other = recv_ref[1024:1056, :].astype(F32) + recv_ref[1056:, :].astype(F32)
    other_ref[...] = other
    first = place_ref[1] == 0
    mine = span_ref[...]
    both = jnp.where(first, mine, other) + reach_ref[16:17, :] * jnp.where(first, other, mine)
    for z in range(16):
        here = slice(z * 64, (z + 1) * 64)
        sent_ref[z, :32, :] = (both * reach_ref[z : z + 1, :]).astype(BF)
        sent_ref[z, 32:, :] = (kept_ref[here, :] + recv_ref[here, :].astype(F32)).astype(BF)


def local_backward_kernel(
    grad_ref,
    entering_ref,
    q_ref,
    k_ref,
    v_ref,
    decay_ref,
    gq_ref,
    value_ref,
    keys_ref,
    change_ref,
    tail_ref,
    reach_ref,
    rest_ref,
    leave_ref,
):
    key_mask, val_mask, own = head_masks()
    grad = grad_ref[...]
    queries = q_ref[...].astype(F32).T
    keys = k_ref[...].astype(F32).T * SCALE
    values = v_ref[...].astype(F32)
    cumulative = block_sums(decay_ref[...].T)
    closing = closings(cumulative)
    grow, shrink = jnp.exp(cumulative), jnp.exp(-cumulative)
    rest = jnp.exp(per_block(closing) - cumulative)
    scaled_q, scaled_k, tail = queries * grow, keys * shrink, keys * rest
    causal = causal_blocks()
    value_grad = jnp.zeros((TOK, 128), F32)
    query_grad = jnp.zeros((TOK, 64), F32)
    key_grad = jnp.zeros((TOK, 64), F32)
    for h in range(2):
        scores = scores_of(scaled_q, scaled_k, key_mask[h], causal)
        score_grad = jnp.where(causal, mm(grad * val_mask[h], values, NT), 0.0)
        value_grad = value_grad + mm(scores, grad * val_mask[h], TN)
        query_grad = query_grad + mm(score_grad, scaled_k * key_mask[h])
        key_grad = key_grad + mm(score_grad, scaled_q * key_mask[h], TN)
    carried_v, carried_q, tail_grad, close_grad, reach = ([None] * NBLK for _ in range(5))
    state_grad, later = jnp.zeros((128, 64), F32), jnp.zeros((1, 64), F32)
    for n in reversed(range(NBLK)):
        here = slice(n * BLOCK, (n + 1) * BLOCK)
        entering = entering_ref[n]
        decay_out = jnp.exp(closing[n])
        reach[n] = jnp.exp(later)
        later = later + closing[n]
        leave_ref[n : n + 1, :] = jnp.exp(later)
        carried_v[n] = mm(tail[here], state_grad, NT)
        carried_q[n] = mm(grad[here], entering)
        tail_grad[n] = mm(values[here], state_grad)
        close_grad[n] = decay_out * jnp.sum(state_grad * entering, axis=0, keepdims=True) + jnp.sum(
            tail_grad[n] * tail[here], axis=0, keepdims=True
        )
        state_grad = decay_out * state_grad + mm(grad[here], scaled_q[here], TN) * own
    value_ref[...] = value_grad + jnp.concatenate(carried_v, axis=0)
    query_grad = query_grad + jnp.concatenate(carried_q, axis=0)
    tail_grad = jnp.concatenate(tail_grad, axis=0)
    change = query_grad * scaled_q - key_grad * scaled_k - tail_grad * tail
    row, col = iota((TOK, TOK), 0), iota((TOK, TOK), 1)
    onward = ((row // BLOCK == col // BLOCK) & (col >= row)).astype(F32)
    change_ref[...] = picked_sums(onward, change) + per_block(close_grad)
    gq_ref[...] = (query_grad * grow).T.astype(BF)
    keys_ref[...] = (key_grad * shrink + tail_grad * rest) * SCALE
    tail_ref[...] = tail
    reach_ref[...] = per_block(reach)
    rest_ref[...] = rest * SCALE


def backward_kernel(
    place_ref,
    later_ref,
    other_ref,
    chips_ref,
    entering_ref,
    v_ref,
    value_ref,
    keys_ref,
    change_ref,
    tail_ref,
    reach_ref,
    rest_ref,
    leave_ref,
    gp_ref,
    gk_ref,
    gv_ref,
    gd_ref,
):
    _, _, own = head_masks()
    sums = later_ref[0].astype(F32)
    for z in range(1, 16):
        sums = sums + later_ref[z].astype(F32)
    gp_ref[...] = sums[32:]
    packed = sums[:32]
    packed = jnp.where(place_ref[1] == 0, chips_ref[17:18, :] * packed + other_ref[...], packed)
    state_grad = opened_state(packed, own)
    tail, reach = tail_ref[...], reach_ref[...]
    gv_ref[...] = (value_ref[...] + mm(tail * reach, state_grad, NT)).astype(BF)
    tail_grad = mm(v_ref[...], state_grad) * reach
    gk_ref[...] = (keys_ref[...] + tail_grad * rest_ref[...]).T.astype(BF)
    row, col = iota((TOK, TOK), 0), iota((TOK, TOK), 1)
    ahead = ((row // BLOCK == col // BLOCK) & (col < row)).astype(F32)
    passed = [
        leave_ref[n : n + 1, :] * jnp.sum(state_grad * entering_ref[n], axis=0, keepdims=True)
        for n in range(NBLK)
    ]
    change = change_ref[...] + picked_sums(ahead, tail_grad * tail) + per_block(passed)
    gd_ref[...] = change.T


def exchanged(blocks, axis):
    return lax.all_to_all(blocks, axis, split_axis=0, concat_axis=0, tiled=True)


def ring_step(step):
    pairs = []
    for t in range(N_TP):
        y, x = t // 4, t % 4
        pairs.append((t, 4 * y + (x + step) % 4))
        pairs.append((N_TP + t, N_TP + 4 * ((y + step) % 4) + x))
    return pairs


def passed_on(array, step):
    return lax.ppermute(array, ("sp_1", "tp"), ring_step(step))


def body(
    moe_input,
    out_grad,
    routes,
    route_weight,
    w_gate,
    w_up,
    w_down,
    w_out,
    queries,
    key_rows,
    value_rows,
    log_decay,
):
    q_t, k_t, decay_t = queries.T, key_rows.T, log_decay.T
    place = jnp.stack(
        [lax.axis_index(SP), lax.axis_index("sp_1"), lax.axis_index("sp_0")]
    ).astype(jnp.int32)

    sent, pick = call(
        dispatch_kernel,
        [((N_SP, 2 * PAD, 128), BF), ((SLOTS, TOK), BF)],
        routes.T,
        route_weight.T,
        moe_input,
        out_grad,
        k_t,
        value_rows,
        decay_t,
    )
    recv = exchanged(sent, SP)
    own_a, own_b = call(
        pack_kernel, [((LOT, 128), BF), ((LOT, 128), BF)], w_gate[0], w_up[0], w_down[0]
    )
    left_a = passed_on(own_a, 1)
    right_b = passed_on(own_b, -1)
    left_b = passed_on(own_b, 1)
    right_a = passed_on(own_a, -1)
    far_a = passed_on(left_a, 1)
    far_b = passed_on(right_b, -1)
    weights = (own_a, own_b, left_a, left_b, right_a, right_b, far_a, far_b)
    copies, states, reach = call(
        copies_kernel,
        [((N_TP, 2 * PART, 128), BF), ((N_SP, 128), F32), ((24, 128), F32)],
        place,
        recv,
        scratch=[pltpu.VMEM((2 * ROWS, 128), F32), pltpu.VMEM((4, 2 * PART, 128), BF)],
        smem=(0,),
        near=(1,),
        near_out=(0,),
    )
    rows = exchanged(copies, "tp")
    (turned,) = call(turned_kernel, [((TOK, SLOTS), BF)], pick, after=(copies,))
    partial_rows, grads, hidden = call(
        partial_kernel,
        [((N_TP, PART, 128), BF), ((PART, 1024), BF), ((PART, 512), BF)],
        rows,
        *weights,
        scratch=[pltpu.VMEM((8, LOT, 128), BF), pltpu.SemaphoreType.DMA((8,))],
        near=(0,),
        near_out=(1, 2),
        raw=tuple(range(1, 9)),
    )
    arrived = exchanged(partial_rows, "tp")
    own_grad_a, own_grad_b, to_left, to_right, left_lot, right_lot = call(
        weight_grads_kernel,
        2 * [((LOT, 128), F32)] + 2 * [((2 * LOT, 128), BF)] + 2 * [((LOT, 128), BF)],
        rows,
        grads,
        hidden,
        near=(0, 1, 2),
    )
    from_left = passed_on(to_right, 1)
    from_right = passed_on(to_left, -1)
    (returned,) = call(
        row_sum_kernel,
        [((N_SP, PAD, 128), BF)],
        place,
        arrived,
        states,
        smem=(0,),
        near=(1,),
        scratch=[pltpu.VMEM((ROWS + 8, 128), F32)],
    )
    back = exchanged(returned, SP)
    (residual,) = call(residual_kernel, [((N_TP, TOK, 128), BF)], back, turned, out_grad, near=(0,))
    full_grad = exchanged(residual, "tp")
    lot_left, lot_right = call(
        relay_kernel,
        2 * [((LOT, 128), BF)],
        left_lot,
        right_lot,
        from_right,
        from_left,
        after=(residual,),
        near=(2, 3),
    )
    last_a = passed_on(lot_right, 1)
    last_b = passed_on(lot_left, -1)
    mixer_out, entering = call(
        forward_kernel,
        [((TOK, 128), BF), ((NBLK, 128, 64), F32)],
        back,
        q_t,
        k_t,
        value_rows,
        decay_t,
        near=(0,),
        near_out=(0,),
        after=(residual,),
    )
    mixer_grad, span_grad, to_other, kept = call(
        mixer_grad_kernel,
        [((TOK, 128), F32), ((32, 128), F32), ((1088, 128), BF), ((1024, 128), F32)],
        place,
        full_grad,
        w_out,
        mixer_out,
        q_t,
        decay_t,
        smem=(0,),
        near=(1, 3),
        near_out=(1, 2, 3),
    )
    from_other = lax.ppermute(to_other, "sp_1", [(0, 1), (1, 0)])
    chip_sent, other_grad = call(
        chip_kernel,
        [((16, 96, 128), BF), ((32, 128), F32)],
        place,
        from_other,
        kept,
        span_grad,
        reach,
        smem=(0,),
        near=(1, 2, 3),
    )
    later = exchanged(chip_sent, "sp_0")
    gq, *local = call(
        local_backward_kernel,
        [
            ((64, TOK), BF),
            ((TOK, 128), F32),
            ((TOK, 64), F32),
            ((TOK, 64), F32),
            ((TOK, 64), F32),
            ((TOK, 64), F32),
            ((TOK, 64), F32),
            ((NBLK, 64), F32),
        ],
        mixer_grad,
        entering,
        q_t,
        k_t,
        value_rows,
        decay_t,
        after=(chip_sent,),
    )
    grad_proj, gk, gv, gd = call(
        backward_kernel,
        [((64, 128), F32), ((64, TOK), BF), ((TOK, 128), BF), ((64, TOK), F32)],
        place,
        later,
        other_grad,
        reach,
        entering,
        value_rows,
        *local,
        smem=(0,),
        near=(1,),
    )
    gate_part, up_part, down_part = call(
        grad_sum_kernel,
        [((2048, 128), BF), ((2048, 128), BF), ((128, 2048), BF)],
        own_grad_a,
        own_grad_b,
        from_right,
        from_left,
        last_a,
        last_b,
        near=(2, 3, 4, 5),
        after=(chip_sent,),
    )
    return (gate_part[None], up_part[None], down_part[None], grad_proj, gq.T, gk.T, gv, gd.T)


def solution(mesh):
    split = Mesh(mesh.devices.reshape(16, 2, mesh.shape["tp"]), ("sp_0", "sp_1", "tp"))
    placed = (
        P(SP, "tp"),
        P(SP, "tp"),
        P(SP, None),
        P(SP, None),
        P(SP, None, "tp"),
        P(SP, None, "tp"),
        P(SP, "tp", None),
        P(None, "tp"),
        P(SP, "tp"),
        P(SP, "tp"),
        P(SP, "tp"),
        P(SP, "tp"),
    )
    return jax.shard_map(
        body,
        mesh=split,
        in_specs=placed,
        out_specs=(
            P(SP, None, "tp"),
            P(SP, None, "tp"),
            P(SP, "tp", None),
            P(SP, "tp"),
            P(SP, "tp"),
            P(SP, "tp"),
            P(SP, "tp"),
            P(SP, "tp"),
        ),
        check_vma=False,
    )
```

```python
import jax
import jax.numpy as jnp
from jax import lax
from jax.experimental import pallas as pl
from jax.experimental.pallas import tpu as pltpu
from jax.sharding import Mesh
from jax.sharding import PartitionSpec as P


KEY_CHANNELS = 32
VAL_DIM = 64
TOP = 2
BLOCK = 64
CAP = 20
PAD = 24
SP = ("sp_0", "sp_1")
N_SP = 32
N_TP = 16
TOK = 256
ROWS = N_SP * CAP
SLOTS = N_SP * PAD
PART = ROWS // 4
LOT = 3 * 1024
EARLY = LOT // 2
NBLK = TOK // BLOCK
BF = jnp.bfloat16
F32 = jnp.float32
HI = lax.Precision.HIGHEST
SCALE = KEY_CHANNELS ** (-0.5)

NN = (((1,), (0,)), ((), ()))
NT = (((1,), (1,)), ((), ()))
TN = (((0,), (0,)), ((), ()))


def mm(a, b, dims=NN):
    return lax.dot_general(a.astype(BF), b.astype(BF), dims, preferred_element_type=F32)


def mm_exact(a, b, dims=NN):
    return lax.dot_general(a, b, dims, precision=HI, preferred_element_type=F32)


def iota(shape, dim):
    return lax.broadcasted_iota(jnp.int32, shape, dim)


def call(fn, outs, *args, scratch=(), smem=(), near=(), near_out=(), after=(), raw=()):
    spaces = [pltpu.VMEM if k in near else pltpu.HBM for k in range(len(args))]
    args = [
        a if k in smem else pltpu.with_memory_space_constraint(a, spaces[k])
        for k, a in enumerate(args)
    ]
    after = [pltpu.with_memory_space_constraint(a, pltpu.HBM) for a in after]
    count = len(args)

    def run(*refs):
        fn(*refs[:count], *refs[count + len(after) :])

    return pl.pallas_call(
        run,
        out_shape=tuple(
            (pltpu.VMEM if k in near_out else pltpu.HBM)(s, d) for k, (s, d) in enumerate(outs)
        ),
        in_specs=[
            pl.BlockSpec(
                memory_space=pltpu.SMEM if k in smem else pltpu.HBM if k in raw else pltpu.VMEM
            )
            for k in range(count)
        ]
        + [pl.BlockSpec(memory_space=pltpu.HBM) for _ in after],
        out_specs=tuple(pl.BlockSpec(memory_space=pltpu.VMEM) for _ in outs),
        scratch_shapes=scratch,
        compiler_params=pltpu.CompilerParams(vmem_limit_bytes=24 * 1024 * 1024),
    )(*args, *after)


def head_masks():
    key_lane = iota((1, 64), 1) // KEY_CHANNELS
    val_lane = iota((1, 128), 1) // VAL_DIM
    keys = [(key_lane == h).astype(F32) for h in range(2)]
    vals = [(val_lane == h).astype(F32) for h in range(2)]
    own = (iota((128, 64), 0) // VAL_DIM == iota((128, 64), 1) // KEY_CHANNELS).astype(F32)
    return keys, vals, own


def packed_state(state):
    both = state[:64] + state[64:]
    return jnp.concatenate([both[:32], both[32:]], axis=1)


def opened_state(packed, own):
    both = jnp.concatenate([packed[:, :64], packed[:, 64:]], axis=0)
    return jnp.concatenate([both, both], axis=0) * own


def picked_sums(mask, values):
    high = values.astype(BF).astype(F32)
    middle = (values - high).astype(BF).astype(F32)
    sums = mm(mask, jnp.concatenate([high, middle, values - high - middle], axis=1))
    return sums[:, :64] + sums[:, 64:128] + sums[:, 128:192]


def block_sums(decay):
    row, col = iota((TOK, TOK), 0), iota((TOK, TOK), 1)
    within = ((row // BLOCK == col // BLOCK) & (col <= row)).astype(F32)
    return picked_sums(within, decay)


def whole_sums(cumulative):
    offset, parts = jnp.zeros((1, 64), F32), []
    for n in range(NBLK):
        block = cumulative[n * BLOCK : (n + 1) * BLOCK]
        parts.append(block + offset)
        offset = offset + block[BLOCK - 1 :]
    return jnp.concatenate(parts, axis=0), offset


def closings(cumulative):
    return [cumulative[(n + 1) * BLOCK - 1 : (n + 1) * BLOCK] for n in range(NBLK)]


def per_block(rows):
    return jnp.concatenate([jnp.broadcast_to(r, (BLOCK, r.shape[1])) for r in rows], axis=0)


def two_parts(values):
    high = values.astype(BF).astype(F32)
    return high, values - high


def dispatch_kernel(
    routes_ref, weight_ref, x_ref, g_ref, k_ref, v_ref, decay_ref, sent_ref, pick_ref
):
    routes = routes_ref[...]
    expert = iota((N_SP, TOK), 0)
    hot = [(expert == routes[j : j + 1, :]) for j in range(TOP)]
    both = (hot[0] | hot[1]).astype(F32)
    before = (iota((TOK, TOK), 0) < iota((TOK, TOK), 1)).astype(F32)
    place = mm(both, before)
    owner, row = iota((SLOTS, N_SP), 0) // PAD, iota((SLOTS, N_SP), 0) % PAD
    mine = owner == iota((SLOTS, N_SP), 1)
    spread = mine.astype(F32)
    slot_place = (iota((SLOTS, TOK), 0) % PAD).astype(F32)
    picks = [(mm(spread, jnp.where(h, place, -1.0)) == slot_place).astype(F32) for h in hot]
    pick = picks[0] + picks[1]
    pick_ref[...] = pick.astype(BF)

    _, _, own = head_masks()
    keys = k_ref[...].astype(F32).T * SCALE
    so_far, total = whole_sums(block_sums(decay_ref[...].T))
    state = mm(v_ref[...], keys * jnp.exp(total - so_far), TN) * own
    state_high, state_low = two_parts(packed_state(state))
    total_row = jnp.concatenate(two_parts(total), axis=1)

    first = (mine & (row == CAP)).astype(F32)
    second = (mine & (row == CAP + 1)).astype(F32)
    chosen = jnp.concatenate([pick, first, second], axis=1)
    rows = jnp.concatenate([x_ref[...].astype(F32), state_high, state_low], axis=0)
    sent_ref[:, :PAD, :] = mm(chosen, rows).astype(BF).reshape(N_SP, PAD, 128)

    grad = g_ref[...].astype(F32)
    weight = jnp.concatenate([weight_ref[...], jnp.zeros((6, TOK), F32)], axis=0).T
    rows = [(weight[:, j : j + 1] * grad).astype(BF) for j in range(TOP)]
    sent = mm(picks[0], rows[0]) + mm(picks[1], rows[1])
    sent = jnp.where(iota((SLOTS, 128), 0) % PAD == CAP, total_row, sent)
    sent_ref[:, PAD:, :] = sent.astype(BF).reshape(N_SP, PAD, 128)


def turned_kernel(pick_ref, out_ref):
    out_ref[...] = pick_ref[...].astype(F32).T.astype(BF)


def quarter_of(place_ref, k):
    return jnp.where(place_ref[1] == 0, k % 4, k // 4)


def copies_kernel(place_ref, recv_ref, out_ref, states_ref, reach_ref, packed, rounded):
    for e in range(N_SP):
        block = recv_ref[e].astype(F32)
        at = (e // 8) * 2 * PART + (e % 8) * CAP
        packed[at : at + CAP, :] = block[:CAP]
        packed[at + PART : at + PART + CAP, :] = block[PAD : PAD + CAP]
    for q in range(4):
        rounded[q] = packed[q * 2 * PART : (q + 1) * 2 * PART, :].astype(BF)
    for k in range(N_TP):
        out_ref[k] = rounded[quarter_of(place_ref, k)]
    chip = place_ref[2]
    totals = [recv_ref[s, PAD + CAP : PAD + CAP + 1, :].astype(F32) for s in range(N_SP)]
    totals = jnp.concatenate(totals, axis=0)
    totals = totals[:, :64] + totals[:, 64:]
    double = jnp.concatenate([totals, totals], axis=1)
    decays = jnp.exp(double)
    state = jnp.zeros((1, 128), F32)
    for s in range(N_SP):
        states_ref[s : s + 1, :] = state
        pair = recv_ref[s, CAP : CAP + 2, :].astype(F32)
        state = decays[s : s + 1] * state + pair[0:1] + pair[1:2]
    target, between = iota((16, N_SP), 0), iota((16, N_SP), 1)
    passed = ((between >= 2 * target + 2) & (between < 2 * chip)).astype(F32)
    reach = jnp.exp(mm_exact(passed, double))
    reach_ref[:16, :] = jnp.where(iota((16, 128), 0) < chip, reach, 0.0)
    here = iota((N_SP, 128), 0)
    even = jnp.sum(jnp.where(here == 2 * chip, decays, 0.0), axis=0, keepdims=True)
    odd = jnp.sum(jnp.where(here == 2 * chip + 1, decays, 0.0), axis=0, keepdims=True)
    reach_ref[16:, :] = jnp.concatenate([even, odd, jnp.zeros((6, 128), F32)], axis=0)


def pack_kernel(wg_ref, wu_ref, wd_ref, a_ref, b_ref):
    a_ref[:2048, :] = wg_ref[...]
    a_ref[2048:, :] = wu_ref[:1024, :]
    b_ref[:1024, :] = wu_ref[1024:, :]
    for k in range(N_TP):
        b_ref[1024 + k * 128 : 1152 + k * 128, :] = wd_ref[:, k * 128 : (k + 1) * 128]


def wide(ref, at, size):
    return jnp.concatenate([ref[k, at : at + size, :] for k in range(N_TP)], axis=1)


def partial_kernel(rows_ref, *refs):
    lots, (part_ref, grads_ref, hidden_ref, held, done) = refs[:8], refs[8:]
    copies = [pltpu.make_async_copy(lots[i], held.at[i], done.at[i]) for i in range(8)]
    for copy in copies:
        copy.start()
    x, g = wide(rows_ref, 0, PART), wide(rows_ref, PART, PART)
    for b in range(4):
        copies[2 * b].wait()
        copies[2 * b + 1].wait()
        gate_weight = held[2 * b, :2048, :]
        up_weight = jnp.concatenate([held[2 * b, 2048:, :], held[2 * b + 1, :1024, :]], axis=0)
        blocks = [held[2 * b + 1, 1024 + k * 128 : 1152 + k * 128, :] for k in range(N_TP)]
        pre = mm(x, jnp.concatenate([gate_weight, up_weight], axis=1))
        upper = mm(g, jnp.concatenate(blocks, axis=1), NT)
        gate_pre, up_pre = pre[:, :128], pre[:, 128:]
        sigmoid = jax.nn.sigmoid(gate_pre)
        activated = gate_pre * sigmoid
        hidden_ref[:, 128 * b : 128 * b + 128] = (activated * up_pre).astype(BF)
        gate = upper * up_pre * sigmoid * (1.0 + gate_pre * (1.0 - sigmoid))
        grads_ref[:, 256 * b : 256 * b + 128] = gate.astype(BF)
        grads_ref[:, 256 * b + 128 : 256 * b + 256] = (upper * activated).astype(BF)
    grads = grads_ref[...]

    def up_rows(b, at):
        if at < 1024:
            return held[2 * b, 2048 + at : 2304 + at, :]
        return held[2 * b + 1, at - 1024 : at - 768, :]

    for k in range(0, N_TP, 2):
        at = k * 128
        weight = []
        for b in range(4):
            weight += [held[2 * b, at : at + 256, :], up_rows(b, at)]
        part = mm(grads, jnp.concatenate(weight, axis=1), NT).astype(BF)
        part_ref[k] = part[:, :128]
        part_ref[k + 1] = part[:, 128:]


def weight_grads_kernel(rows_ref, grads_ref, hidden_ref, *out_refs):
    grads = grads_ref[...]
    hidden = hidden_ref[...]
    for k in range(0, N_TP, 2):
        x = jnp.concatenate([rows_ref[k, :PART, :], rows_ref[k + 1, :PART, :]], axis=1)
        g = jnp.concatenate([rows_ref[k, PART:, :], rows_ref[k + 1, PART:, :]], axis=1)
        both = mm(x, grads, TN)
        down = mm(hidden, g, TN)
        at = k * 128
        for b in range(4):

            def put(lot, row, value):
                ref, start = place_of(out_refs, b, lot, row)
                ref[start : start + len(value), :] = value.astype(ref.dtype)

            put(0, at, both[:, 256 * b : 256 * b + 128])
            up = both[:, 256 * b + 128 : 256 * b + 256]
            if k < N_TP // 2:
                put(0, 2048 + at, up)
            else:
                put(1, at - 1024, up)
            for n in range(2):
                block = down[128 * b : 128 * b + 128, n * 128 : (n + 1) * 128]
                put(1, 1024 + at + n * 128, block)


def place_of(refs, device, lot, row):
    own_a, own_b, to_left, to_right, left_b, left_late, right_a, right_late = refs
    if device == 0:
        return (own_a, own_b)[lot], row
    if device == 3:
        return ((to_right, row), (to_left, EARLY + row))[lot]
    if device == 1:
        if lot == 1:
            return left_b, row
        return (to_left, row) if row < EARLY else (left_late, row - EARLY)
    if lot == 0:
        return right_a, row
    return (to_right, LOT + row) if row < EARLY else (right_late, row - EARLY)


def relay_kernel(
    left_b_ref,
    left_late_ref,
    right_a_ref,
    right_late_ref,
    from_right_ref,
    from_left_ref,
    to_left_ref,
    to_right_ref,
):
    far_a, far_b = from_left_ref[:LOT, :].astype(F32), from_right_ref[EARLY:, :].astype(F32)
    to_right_ref[:LOT, :] = (right_a_ref[...].astype(F32) + far_a).astype(BF)
    to_right_ref[LOT:, :] = right_late_ref[...]
    to_left_ref[:EARLY, :] = left_late_ref[...]
    to_left_ref[EARLY:, :] = (left_b_ref[...].astype(F32) + far_b).astype(BF)


def grad_sum_kernel(
    own_a_ref,
    own_b_ref,
    from_right_ref,
    from_left_ref,
    last_left_ref,
    last_right_ref,
    gate_ref,
    up_ref,
    down_ref,
):
    def total(at):
        lot, row = divmod(at, LOT)
        if lot == 0:
            own, summed = (own_a_ref, row), (last_left_ref, row)
            single = (from_right_ref if row < EARLY else last_right_ref, row % EARLY)
        else:
            own, summed = (own_b_ref, row), (last_right_ref, EARLY + row)
            single = (from_left_ref if row < EARLY else last_left_ref, LOT + row % EARLY)
        rows = [r[start : start + 128, :].astype(F32) for r, start in (own, summed, single)]
        return (rows[0] + rows[1] + rows[2]).astype(BF)

    for k in range(N_TP):
        here = slice(k * 128, (k + 1) * 128)
        gate_ref[here, :] = total(k * 128)
        up_ref[here, :] = total(2048 + k * 128)
        down_ref[:, here] = total(4096 + k * 128)


def row_sum_kernel(place_ref, part_ref, states_ref, out_ref, total):
    for q in range(4):
        acc = jnp.zeros((PART, 128), F32)
        for j in range(4):
            source = jnp.where(place_ref[1] == 0, 4 * j + q, 4 * q + j)
            acc = acc + part_ref[source].astype(F32)
        total[q * PART : (q + 1) * PART, :] = acc
    total[ROWS:, :] = jnp.zeros((8, 128), F32)
    row = iota((PAD, 128), 0)
    high, low = two_parts(states_ref[...])
    for e in range(N_SP):
        rows = jnp.where(row < CAP, total[e * CAP : e * CAP + PAD, :], 0.0)
        rows = jnp.where(row == CAP, high[e : e + 1], rows)
        rows = jnp.where(row == CAP + 1, low[e : e + 1], rows)
        out_ref[e] = rows.astype(BF)


def residual_kernel(back_ref, turned_ref, g_ref, out_ref):
    routed = mm(turned_ref[...], back_ref[...].reshape(SLOTS, 128))
    residual = (g_ref[...].astype(F32) + routed).astype(BF)
    for k in range(N_TP):
        out_ref[k] = residual


def scores_of(queries, keys, mask, causal):
    return jnp.where(causal, mm(queries * mask, keys, NT), 0.0)


def causal_blocks():
    row, col = iota((TOK, TOK), 0), iota((TOK, TOK), 1)
    return (row // BLOCK == col // BLOCK) & (col <= row)


def forward_kernel(back_ref, q_ref, k_ref, v_ref, decay_ref, out_ref, entering_ref):
    key_mask, val_mask, own = head_masks()
    rows = [back_ref[s, CAP : CAP + 2, :].astype(F32) for s in range(N_SP)]
    packed = jnp.concatenate([r[0:1] + r[1:2] for r in rows], axis=0)
    state = opened_state(packed, own)
    queries = q_ref[...].astype(F32).T
    keys = k_ref[...].astype(F32).T * SCALE
    values = v_ref[...].astype(F32)
    cumulative = block_sums(decay_ref[...].T)
    closing = closings(cumulative)
    scaled_q = queries * jnp.exp(cumulative)
    scaled_k = keys * jnp.exp(-cumulative)
    tail = keys * jnp.exp(per_block(closing) - cumulative)
    causal = causal_blocks()
    within = jnp.zeros((TOK, 128), F32)
    for h in range(2):
        scores = scores_of(scaled_q, scaled_k, key_mask[h], causal)
        within = within + mm(scores, values * val_mask[h])
    for n in range(NBLK):
        here = slice(n * BLOCK, (n + 1) * BLOCK)
        entering_ref[n] = state
        out_ref[here, :] = (within[here] + mm(scaled_q[here], state, NT)).astype(BF)
        state = jnp.exp(closing[n]) * state + mm(values[here], tail[here], TN) * own


def mixer_grad_kernel(
    place_ref, full_ref, w_ref, mixed_ref, q_ref, decay_ref, grad_ref, span_ref, sent_ref, kept_ref
):
    _, _, own = head_masks()
    grad = mm(wide(full_ref, 0, TOK), w_ref[...])
    grad_ref[...] = grad
    so_far, _ = whole_sums(block_sums(decay_ref[...].T))
    scaled = q_ref[...].astype(F32).T * jnp.exp(so_far)
    packed = packed_state(mm(grad, scaled, TN) * own)
    span_ref[...] = packed
    high, low = two_parts(packed)
    sent_ref[1024:1056, :] = high.astype(BF)
    sent_ref[1056:, :] = low.astype(BF)
    mixed = mixed_ref[...]
    first = place_ref[1] == 0
    for k in range(0, N_TP, 2):
        rows = jnp.concatenate([full_ref[k], full_ref[k + 1]], axis=1)
        part = mm(rows, mixed, TN)
        for n in range(2):
            low, high = part[n * 128 : n * 128 + 64], part[n * 128 + 64 : n * 128 + 128]
            here = slice((k + n) * 64, (k + n + 1) * 64)
            kept_ref[here, :] = jnp.where(first, low, high)
            sent_ref[here, :] = jnp.where(first, high, low).astype(BF)


def chip_kernel(place_ref, recv_ref, kept_ref, span_ref, reach_ref, sent_ref, other_ref):
    other = recv_ref[1024:1056, :].astype(F32) + recv_ref[1056:, :].astype(F32)
    other_ref[...] = other
    first = place_ref[1] == 0
    mine = span_ref[...]
    both = jnp.where(first, mine, other) + reach_ref[16:17, :] * jnp.where(first, other, mine)
    for z in range(16):
        here = slice(z * 64, (z + 1) * 64)
        sent_ref[z, :32, :] = (both * reach_ref[z : z + 1, :]).astype(BF)
        sent_ref[z, 32:, :] = (kept_ref[here, :] + recv_ref[here, :].astype(F32)).astype(BF)


def local_backward_kernel(
    grad_ref,
    entering_ref,
    q_ref,
    k_ref,
    v_ref,
    decay_ref,
    gq_ref,
    value_ref,
    keys_ref,
    change_ref,
    tail_ref,
    reach_ref,
    rest_ref,
    leave_ref,
):
    key_mask, val_mask, own = head_masks()
    grad = grad_ref[...]
    queries = q_ref[...].astype(F32).T
    keys = k_ref[...].astype(F32).T * SCALE
    values = v_ref[...].astype(F32)
    cumulative = block_sums(decay_ref[...].T)
    closing = closings(cumulative)
    grow, shrink = jnp.exp(cumulative), jnp.exp(-cumulative)
    rest = jnp.exp(per_block(closing) - cumulative)
    scaled_q, scaled_k, tail = queries * grow, keys * shrink, keys * rest
    causal = causal_blocks()
    value_grad = jnp.zeros((TOK, 128), F32)
    query_grad = jnp.zeros((TOK, 64), F32)
    key_grad = jnp.zeros((TOK, 64), F32)
    for h in range(2):
        scores = scores_of(scaled_q, scaled_k, key_mask[h], causal)
        score_grad = jnp.where(causal, mm(grad * val_mask[h], values, NT), 0.0)
        value_grad = value_grad + mm(scores, grad * val_mask[h], TN)
        query_grad = query_grad + mm(score_grad, scaled_k * key_mask[h])
        key_grad = key_grad + mm(score_grad, scaled_q * key_mask[h], TN)
    carried_v, carried_q, tail_grad, close_grad, reach = ([None] * NBLK for _ in range(5))
    state_grad, later = jnp.zeros((128, 64), F32), jnp.zeros((1, 64), F32)
    for n in reversed(range(NBLK)):
        here = slice(n * BLOCK, (n + 1) * BLOCK)
        entering = entering_ref[n]
        decay_out = jnp.exp(closing[n])
        reach[n] = jnp.exp(later)
        later = later + closing[n]
        leave_ref[n : n + 1, :] = jnp.exp(later)
        carried_v[n] = mm(tail[here], state_grad, NT)
        carried_q[n] = mm(grad[here], entering)
        tail_grad[n] = mm(values[here], state_grad)
        close_grad[n] = decay_out * jnp.sum(state_grad * entering, axis=0, keepdims=True) + jnp.sum(
            tail_grad[n] * tail[here], axis=0, keepdims=True
        )
        state_grad = decay_out * state_grad + mm(grad[here], scaled_q[here], TN) * own
    value_ref[...] = value_grad + jnp.concatenate(carried_v, axis=0)
    query_grad = query_grad + jnp.concatenate(carried_q, axis=0)
    tail_grad = jnp.concatenate(tail_grad, axis=0)
    change = query_grad * scaled_q - key_grad * scaled_k - tail_grad * tail
    row, col = iota((TOK, TOK), 0), iota((TOK, TOK), 1)
    onward = ((row // BLOCK == col // BLOCK) & (col >= row)).astype(F32)
    change_ref[...] = picked_sums(onward, change) + per_block(close_grad)
    gq_ref[...] = (query_grad * grow).T.astype(BF)
    keys_ref[...] = (key_grad * shrink + tail_grad * rest) * SCALE
    tail_ref[...] = tail
    reach_ref[...] = per_block(reach)
    rest_ref[...] = rest * SCALE


def backward_kernel(
    place_ref,
    later_ref,
    other_ref,
    chips_ref,
    entering_ref,
    v_ref,
    value_ref,
    keys_ref,
    change_ref,
    tail_ref,
    reach_ref,
    rest_ref,
    leave_ref,
    gp_ref,
    gk_ref,
    gv_ref,
    gd_ref,
):
    _, _, own = head_masks()
    sums = later_ref[0].astype(F32)
    for z in range(1, 16):
        sums = sums + later_ref[z].astype(F32)
    gp_ref[...] = sums[32:]
    packed = sums[:32]
    packed = jnp.where(place_ref[1] == 0, chips_ref[17:18, :] * packed + other_ref[...], packed)
    state_grad = opened_state(packed, own)
    tail, reach = tail_ref[...], reach_ref[...]
    gv_ref[...] = (value_ref[...] + mm(tail * reach, state_grad, NT)).astype(BF)
    tail_grad = mm(v_ref[...], state_grad) * reach
    gk_ref[...] = (keys_ref[...] + tail_grad * rest_ref[...]).T.astype(BF)
    row, col = iota((TOK, TOK), 0), iota((TOK, TOK), 1)
    ahead = ((row // BLOCK == col // BLOCK) & (col < row)).astype(F32)
    passed = [
        leave_ref[n : n + 1, :] * jnp.sum(state_grad * entering_ref[n], axis=0, keepdims=True)
        for n in range(NBLK)
    ]
    change = change_ref[...] + picked_sums(ahead, tail_grad * tail) + per_block(passed)
    gd_ref[...] = change.T


def exchanged(blocks, axis):
    return lax.all_to_all(blocks, axis, split_axis=0, concat_axis=0, tiled=True)


def ring_step(step):
    pairs = []
    for t in range(N_TP):
        y, x = t // 4, t % 4
        pairs.append((t, 4 * y + (x + step) % 4))
        pairs.append((N_TP + t, N_TP + 4 * ((y + step) % 4) + x))
    return pairs


def passed_on(array, step):
    return lax.ppermute(array, ("sp_1", "tp"), ring_step(step))


def body(
    moe_input,
    out_grad,
    routes,
    route_weight,
    w_gate,
    w_up,
    w_down,
    w_out,
    queries,
    key_rows,
    value_rows,
    log_decay,
):
    q_t, k_t, decay_t = queries.T, key_rows.T, log_decay.T
    place = jnp.stack(
        [lax.axis_index(SP), lax.axis_index("sp_1"), lax.axis_index("sp_0")]
    ).astype(jnp.int32)

    sent, pick = call(
        dispatch_kernel,
        [((N_SP, 2 * PAD, 128), BF), ((SLOTS, TOK), BF)],
        routes.T,
        route_weight.T,
        moe_input,
        out_grad,
        k_t,
        value_rows,
        decay_t,
    )
    recv = exchanged(sent, SP)
    own_a, own_b = call(
        pack_kernel, [((LOT, 128), BF), ((LOT, 128), BF)], w_gate[0], w_up[0], w_down[0]
    )
    left_a = passed_on(own_a, 1)
    right_b = passed_on(own_b, -1)
    left_b = passed_on(own_b, 1)
    right_a = passed_on(own_a, -1)
    far_a = passed_on(left_a, 1)
    far_b = passed_on(right_b, -1)
    weights = (own_a, own_b, left_a, left_b, right_a, right_b, far_a, far_b)
    copies, states, reach = call(
        copies_kernel,
        [((N_TP, 2 * PART, 128), BF), ((N_SP, 128), F32), ((24, 128), F32)],
        place,
        recv,
        scratch=[pltpu.VMEM((2 * ROWS, 128), F32), pltpu.VMEM((4, 2 * PART, 128), BF)],
        smem=(0,),
        near=(1,),
        near_out=(0,),
    )
    rows = exchanged(copies, "tp")
    (turned,) = call(turned_kernel, [((TOK, SLOTS), BF)], pick, after=(copies,))
    partial_rows, grads, hidden = call(
        partial_kernel,
        [((N_TP, PART, 128), BF), ((PART, 1024), BF), ((PART, 512), BF)],
        rows,
        *weights,
        scratch=[pltpu.VMEM((8, LOT, 128), BF), pltpu.SemaphoreType.DMA((8,))],
        near=(0,),
        near_out=(1, 2),
        raw=tuple(range(1, 9)),
    )
    arrived = exchanged(partial_rows, "tp")
    own_grad_a, own_grad_b, to_left, to_right, *held_back = call(
        weight_grads_kernel,
        2 * [((LOT, 128), F32)]
        + 2 * [((LOT + EARLY, 128), BF)]
        + 2 * [((LOT, 128), BF), ((EARLY, 128), BF)],
        rows,
        grads,
        hidden,
        near=(0, 1, 2),
    )
    from_left = passed_on(to_right, 1)
    from_right = passed_on(to_left, -1)
    (returned,) = call(
        row_sum_kernel,
        [((N_SP, PAD, 128), BF)],
        place,
        arrived,
        states,
        smem=(0,),
        near=(1,),
        scratch=[pltpu.VMEM((ROWS + 8, 128), F32)],
    )
    back = exchanged(returned, SP)
    (residual,) = call(residual_kernel, [((N_TP, TOK, 128), BF)], back, turned, out_grad, near=(0,))
    full_grad = exchanged(residual, "tp")
    lot_left, lot_right = call(
        relay_kernel,
        2 * [((LOT + EARLY, 128), BF)],
        *held_back,
        from_right,
        from_left,
        after=(residual,),
        near=(4, 5),
    )
    last_a = passed_on(lot_right, 1)
    last_b = passed_on(lot_left, -1)
    mixer_out, entering = call(
        forward_kernel,
        [((TOK, 128), BF), ((NBLK, 128, 64), F32)],
        back,
        q_t,
        k_t,
        value_rows,
        decay_t,
        near=(0,),
        near_out=(0,),
        after=(residual,),
    )
    mixer_grad, span_grad, to_other, kept = call(
        mixer_grad_kernel,
        [((TOK, 128), F32), ((32, 128), F32), ((1088, 128), BF), ((1024, 128), F32)],
        place,
        full_grad,
        w_out,
        mixer_out,
        q_t,
        decay_t,
        smem=(0,),
        near=(1, 3),
        near_out=(1, 2, 3),
    )
    from_other = lax.ppermute(to_other, "sp_1", [(0, 1), (1, 0)])
    chip_sent, other_grad = call(
        chip_kernel,
        [((16, 96, 128), BF), ((32, 128), F32)],
        place,
        from_other,
        kept,
        span_grad,
        reach,
        smem=(0,),
        near=(1, 2, 3),
    )
    later = exchanged(chip_sent, "sp_0")
    gq, *local = call(
        local_backward_kernel,
        [
            ((64, TOK), BF),
            ((TOK, 128), F32),
            ((TOK, 64), F32),
            ((TOK, 64), F32),
            ((TOK, 64), F32),
            ((TOK, 64), F32),
            ((TOK, 64), F32),
            ((NBLK, 64), F32),
        ],
        mixer_grad,
        entering,
        q_t,
        k_t,
        value_rows,
        decay_t,
        after=(chip_sent,),
    )
    grad_proj, gk, gv, gd = call(
        backward_kernel,
        [((64, 128), F32), ((64, TOK), BF), ((TOK, 128), BF), ((64, TOK), F32)],
        place,
        later,
        other_grad,
        reach,
        entering,
        value_rows,
        *local,
        smem=(0,),
        near=(1,),
    )
    gate_part, up_part, down_part = call(
        grad_sum_kernel,
        [((2048, 128), BF), ((2048, 128), BF), ((128, 2048), BF)],
        own_grad_a,
        own_grad_b,
        from_right,
        from_left,
        last_a,
        last_b,
        near=(2, 3, 4, 5),
        after=(chip_sent,),
    )
    return (gate_part[None], up_part[None], down_part[None], grad_proj, gq.T, gk.T, gv, gd.T)


def solution(mesh):
    split = Mesh(mesh.devices.reshape(16, 2, mesh.shape["tp"]), ("sp_0", "sp_1", "tp"))
    placed = (
        P(SP, "tp"),
        P(SP, "tp"),
        P(SP, None),
        P(SP, None),
        P(SP, None, "tp"),
        P(SP, None, "tp"),
        P(SP, "tp", None),
        P(None, "tp"),
        P(SP, "tp"),
        P(SP, "tp"),
        P(SP, "tp"),
        P(SP, "tp"),
    )
    return jax.shard_map(
        body,
        mesh=split,
        in_specs=placed,
        out_specs=(
            P(SP, None, "tp"),
            P(SP, None, "tp"),
            P(SP, "tp", None),
            P(SP, "tp"),
            P(SP, "tp"),
            P(SP, "tp"),
            P(SP, "tp"),
            P(SP, "tp"),
        ),
        check_vma=False,
    )
```

```python
import jax
import jax.numpy as jnp
from jax import lax
from jax.experimental import pallas as pl
from jax.experimental.pallas import tpu as pltpu
from jax.sharding import Mesh
from jax.sharding import PartitionSpec as P


KEY_CHANNELS = 32
VAL_DIM = 64
TOP = 2
BLOCK = 64
CAP = 20
PAD = 24
SP = ("sp_0", "sp_1")
N_SP = 32
N_TP = 16
TOK = 256
ROWS = N_SP * CAP
SLOTS = N_SP * PAD
PART = ROWS // 4
LOT = 3 * 1024
EARLY = LOT // 2
NBLK = TOK // BLOCK
BF = jnp.bfloat16
F32 = jnp.float32
HI = lax.Precision.HIGHEST
SCALE = KEY_CHANNELS ** (-0.5)

NN = (((1,), (0,)), ((), ()))
NT = (((1,), (1,)), ((), ()))
TN = (((0,), (0,)), ((), ()))


def mm(a, b, dims=NN):
    return lax.dot_general(a.astype(BF), b.astype(BF), dims, preferred_element_type=F32)


def mm_exact(a, b, dims=NN):
    return lax.dot_general(a, b, dims, precision=HI, preferred_element_type=F32)


def iota(shape, dim):
    return lax.broadcasted_iota(jnp.int32, shape, dim)


def call(fn, outs, *args, scratch=(), smem=(), near=(), near_out=(), after=(), raw=(), near_after=False):
    spaces = [pltpu.VMEM if k in near else pltpu.HBM for k in range(len(args))]
    args = [
        a if k in smem else pltpu.with_memory_space_constraint(a, spaces[k])
        for k, a in enumerate(args)
    ]
    after_space = pltpu.VMEM if near_after else pltpu.HBM
    after = [pltpu.with_memory_space_constraint(a, after_space) for a in after]
    count = len(args)

    def run(*refs):
        fn(*refs[:count], *refs[count + len(after) :])

    return pl.pallas_call(
        run,
        out_shape=tuple(
            (pltpu.VMEM if k in near_out else pltpu.HBM)(s, d) for k, (s, d) in enumerate(outs)
        ),
        in_specs=[
            pl.BlockSpec(
                memory_space=pltpu.SMEM if k in smem else pltpu.HBM if k in raw else pltpu.VMEM
            )
            for k in range(count)
        ]
        + [pl.BlockSpec(memory_space=after_space) for _ in after],
        out_specs=tuple(pl.BlockSpec(memory_space=pltpu.VMEM) for _ in outs),
        scratch_shapes=scratch,
        compiler_params=pltpu.CompilerParams(vmem_limit_bytes=24 * 1024 * 1024),
    )(*args, *after)


def head_masks():
    key_lane = iota((1, 64), 1) // KEY_CHANNELS
    val_lane = iota((1, 128), 1) // VAL_DIM
    keys = [(key_lane == h).astype(F32) for h in range(2)]
    vals = [(val_lane == h).astype(F32) for h in range(2)]
    own = (iota((128, 64), 0) // VAL_DIM == iota((128, 64), 1) // KEY_CHANNELS).astype(F32)
    return keys, vals, own


def packed_state(state):
    both = state[:64] + state[64:]
    return jnp.concatenate([both[:32], both[32:]], axis=1)


def opened_state(packed, own):
    both = jnp.concatenate([packed[:, :64], packed[:, 64:]], axis=0)
    return jnp.concatenate([both, both], axis=0) * own


def picked_sums(mask, values):
    high = values.astype(BF).astype(F32)
    middle = (values - high).astype(BF).astype(F32)
    sums = mm(mask, jnp.concatenate([high, middle, values - high - middle], axis=1))
    return sums[:, :64] + sums[:, 64:128] + sums[:, 128:192]


def block_sums(decay):
    row, col = iota((TOK, TOK), 0), iota((TOK, TOK), 1)
    within = ((row // BLOCK == col // BLOCK) & (col <= row)).astype(F32)
    return picked_sums(within, decay)


def whole_sums(cumulative):
    offset, parts = jnp.zeros((1, 64), F32), []
    for n in range(NBLK):
        block = cumulative[n * BLOCK : (n + 1) * BLOCK]
        parts.append(block + offset)
        offset = offset + block[BLOCK - 1 :]
    return jnp.concatenate(parts, axis=0), offset


def closings(cumulative):
    return [cumulative[(n + 1) * BLOCK - 1 : (n + 1) * BLOCK] for n in range(NBLK)]


def per_block(rows):
    return jnp.concatenate([jnp.broadcast_to(r, (BLOCK, r.shape[1])) for r in rows], axis=0)


def two_parts(values):
    high = values.astype(BF).astype(F32)
    return high, values - high


def dispatch_kernel(
    routes_ref, weight_ref, x_ref, g_ref, k_ref, v_ref, decay_ref, sent_ref, pick_ref
):
    routes = routes_ref[...]
    expert = iota((N_SP, TOK), 0)
    hot = [(expert == routes[j : j + 1, :]) for j in range(TOP)]
    both = (hot[0] | hot[1]).astype(F32)
    before = (iota((TOK, TOK), 0) < iota((TOK, TOK), 1)).astype(F32)
    place = mm(both, before)
    owner, row = iota((SLOTS, N_SP), 0) // PAD, iota((SLOTS, N_SP), 0) % PAD
    mine = owner == iota((SLOTS, N_SP), 1)
    spread = mine.astype(F32)
    slot_place = (iota((SLOTS, TOK), 0) % PAD).astype(F32)
    picks = [(mm(spread, jnp.where(h, place, -1.0)) == slot_place).astype(F32) for h in hot]
    pick = picks[0] + picks[1]
    pick_ref[...] = pick.astype(BF)

    _, _, own = head_masks()
    keys = k_ref[...].astype(F32).T * SCALE
    so_far, total = whole_sums(block_sums(decay_ref[...].T))
    state = mm(v_ref[...], keys * jnp.exp(total - so_far), TN) * own
    state_high, state_low = two_parts(packed_state(state))
    total_row = jnp.concatenate(two_parts(total), axis=1)

    first = (mine & (row == CAP)).astype(F32)
    second = (mine & (row == CAP + 1)).astype(F32)
    chosen = jnp.concatenate([pick, first, second], axis=1)
    rows = jnp.concatenate([x_ref[...].astype(F32), state_high, state_low], axis=0)
    sent_ref[:, :PAD, :] = mm(chosen, rows).astype(BF).reshape(N_SP, PAD, 128)

    grad = g_ref[...].astype(F32)
    weight = jnp.concatenate([weight_ref[...], jnp.zeros((6, TOK), F32)], axis=0).T
    rows = [(weight[:, j : j + 1] * grad).astype(BF) for j in range(TOP)]
    sent = mm(picks[0], rows[0]) + mm(picks[1], rows[1])
    sent = jnp.where(iota((SLOTS, 128), 0) % PAD == CAP, total_row, sent)
    sent_ref[:, PAD:, :] = sent.astype(BF).reshape(N_SP, PAD, 128)


def turned_kernel(pick_ref, out_ref):
    out_ref[...] = pick_ref[...].astype(F32).T.astype(BF)


def quarter_of(place_ref, k):
    return jnp.where(place_ref[1] == 0, k % 4, k // 4)


def copies_kernel(place_ref, recv_ref, out_ref, packed, rounded):
    for e in range(N_SP):
        block = recv_ref[e].astype(F32)
        at = (e // 8) * 2 * PART + (e % 8) * CAP
        packed[at : at + CAP, :] = block[:CAP]
        packed[at + PART : at + PART + CAP, :] = block[PAD : PAD + CAP]
    for q in range(4):
        rounded[q] = packed[q * 2 * PART : (q + 1) * 2 * PART, :].astype(BF)
    for k in range(N_TP):
        out_ref[k] = rounded[quarter_of(place_ref, k)]


def mark_kernel(out_ref):
    out_ref[...] = jnp.zeros((8, 128), F32)


def scan_kernel(place_ref, recv_ref, states_ref, reach_ref):
    chip = place_ref[2]
    totals = [recv_ref[s, PAD + CAP : PAD + CAP + 1, :].astype(F32) for s in range(N_SP)]
    totals = jnp.concatenate(totals, axis=0)
    totals = totals[:, :64] + totals[:, 64:]
    double = jnp.concatenate([totals, totals], axis=1)
    decays = jnp.exp(double)
    state = jnp.zeros((1, 128), F32)
    for s in range(N_SP):
        states_ref[s : s + 1, :] = state
        pair = recv_ref[s, CAP : CAP + 2, :].astype(F32)
        state = decays[s : s + 1] * state + pair[0:1] + pair[1:2]
    target, between = iota((16, N_SP), 0), iota((16, N_SP), 1)
    passed = ((between >= 2 * target + 2) & (between < 2 * chip)).astype(F32)
    reach = jnp.exp(mm_exact(passed, double))
    reach_ref[:16, :] = jnp.where(iota((16, 128), 0) < chip, reach, 0.0)
    here = iota((N_SP, 128), 0)
    even = jnp.sum(jnp.where(here == 2 * chip, decays, 0.0), axis=0, keepdims=True)
    odd = jnp.sum(jnp.where(here == 2 * chip + 1, decays, 0.0), axis=0, keepdims=True)
    reach_ref[16:, :] = jnp.concatenate([even, odd, jnp.zeros((6, 128), F32)], axis=0)


def pack_kernel(wg_ref, wu_ref, wd_ref, a_ref, b_ref):
    a_ref[:2048, :] = wg_ref[...]
    a_ref[2048:, :] = wu_ref[:1024, :]
    b_ref[:1024, :] = wu_ref[1024:, :]
    for k in range(N_TP):
        b_ref[1024 + k * 128 : 1152 + k * 128, :] = wd_ref[:, k * 128 : (k + 1) * 128]


def wide(ref, at, size):
    return jnp.concatenate([ref[k, at : at + size, :] for k in range(N_TP)], axis=1)


def partial_kernel(rows_ref, *refs):
    lots, (part_ref, grads_ref, hidden_ref, held, done) = refs[:8], refs[8:]
    copies = [pltpu.make_async_copy(lots[i], held.at[i], done.at[i]) for i in range(8)]
    for copy in copies:
        copy.start()
    x, g = wide(rows_ref, 0, PART), wide(rows_ref, PART, PART)
    for b in range(4):
        copies[2 * b].wait()
        copies[2 * b + 1].wait()
        gate_weight = held[2 * b, :2048, :]
        up_weight = jnp.concatenate([held[2 * b, 2048:, :], held[2 * b + 1, :1024, :]], axis=0)
        blocks = [held[2 * b + 1, 1024 + k * 128 : 1152 + k * 128, :] for k in range(N_TP)]
        pre = mm(x, jnp.concatenate([gate_weight, up_weight], axis=1))
        upper = mm(g, jnp.concatenate(blocks, axis=1), NT)
        gate_pre, up_pre = pre[:, :128], pre[:, 128:]
        sigmoid = jax.nn.sigmoid(gate_pre)
        activated = gate_pre * sigmoid
        hidden_ref[:, 128 * b : 128 * b + 128] = (activated * up_pre).astype(BF)
        gate = upper * up_pre * sigmoid * (1.0 + gate_pre * (1.0 - sigmoid))
        grads_ref[:, 256 * b : 256 * b + 128] = gate.astype(BF)
        grads_ref[:, 256 * b + 128 : 256 * b + 256] = (upper * activated).astype(BF)
    grads = grads_ref[...]

    def up_rows(b, at):
        if at < 1024:
            return held[2 * b, 2048 + at : 2304 + at, :]
        return held[2 * b + 1, at - 1024 : at - 768, :]

    for k in range(0, N_TP, 2):
        at = k * 128
        weight = []
        for b in range(4):
            weight += [held[2 * b, at : at + 256, :], up_rows(b, at)]
        part = mm(grads, jnp.concatenate(weight, axis=1), NT).astype(BF)
        part_ref[k] = part[:, :128]
        part_ref[k + 1] = part[:, 128:]


def weight_grads_kernel(rows_ref, grads_ref, hidden_ref, *out_refs):
    grads = grads_ref[...]
    hidden = hidden_ref[...]
    for k in range(0, N_TP, 2):
        x = jnp.concatenate([rows_ref[k, :PART, :], rows_ref[k + 1, :PART, :]], axis=1)
        g = jnp.concatenate([rows_ref[k, PART:, :], rows_ref[k + 1, PART:, :]], axis=1)
        both = mm(x, grads, TN)
        down = mm(hidden, g, TN)
        at = k * 128
        for b in range(4):

            def put(lot, row, value):
                ref, start = place_of(out_refs, b, lot, row)
                ref[start : start + len(value), :] = value.astype(ref.dtype)

            put(0, at, both[:, 256 * b : 256 * b + 128])
            up = both[:, 256 * b + 128 : 256 * b + 256]
            if k < N_TP // 2:
                put(0, 2048 + at, up)
            else:
                put(1, at - 1024, up)
            for n in range(2):
                block = down[128 * b : 128 * b + 128, n * 128 : (n + 1) * 128]
                put(1, 1024 + at + n * 128, block)


def place_of(refs, device, lot, row):
    own_a, own_b, to_left, to_right, left_b, left_late, right_a, right_late = refs
    if device == 0:
        return (own_a, own_b)[lot], row
    if device == 3:
        return ((to_right, row), (to_left, EARLY + row))[lot]
    if device == 1:
        if lot == 1:
            return left_b, row
        return (to_left, row) if row < EARLY else (left_late, row - EARLY)
    if lot == 0:
        return right_a, row
    return (to_right, LOT + row) if row < EARLY else (right_late, row - EARLY)


def relay_kernel(
    left_b_ref,
    left_late_ref,
    right_a_ref,
    right_late_ref,
    from_right_ref,
    from_left_ref,
    to_left_ref,
    to_right_ref,
):
    far_a, far_b = from_left_ref[:LOT, :].astype(F32), from_right_ref[EARLY:, :].astype(F32)
    to_right_ref[:LOT, :] = (right_a_ref[...].astype(F32) + far_a).astype(BF)
    to_right_ref[LOT:, :] = right_late_ref[...]
    to_left_ref[:EARLY, :] = left_late_ref[...]
    to_left_ref[EARLY:, :] = (left_b_ref[...].astype(F32) + far_b).astype(BF)


def grad_sum_kernel(
    own_a_ref,
    own_b_ref,
    from_right_ref,
    from_left_ref,
    last_left_ref,
    last_right_ref,
    gate_ref,
    up_ref,
    down_ref,
):
    def total(at):
        lot, row = divmod(at, LOT)
        if lot == 0:
            own, summed = (own_a_ref, row), (last_left_ref, row)
            single = (from_right_ref if row < EARLY else last_right_ref, row % EARLY)
        else:
            own, summed = (own_b_ref, row), (last_right_ref, EARLY + row)
            single = (from_left_ref if row < EARLY else last_left_ref, LOT + row % EARLY)
        rows = [r[start : start + 128, :].astype(F32) for r, start in (own, summed, single)]
        return (rows[0] + rows[1] + rows[2]).astype(BF)

    for k in range(N_TP):
        here = slice(k * 128, (k + 1) * 128)
        gate_ref[here, :] = total(k * 128)
        up_ref[here, :] = total(2048 + k * 128)
        down_ref[:, here] = total(4096 + k * 128)


def row_sum_kernel(place_ref, part_ref, states_ref, out_ref, total):
    for q in range(4):
        acc = jnp.zeros((PART, 128), F32)
        for j in range(4):
            source = jnp.where(place_ref[1] == 0, 4 * j + q, 4 * q + j)
            acc = acc + part_ref[source].astype(F32)
        total[q * PART : (q + 1) * PART, :] = acc
    total[ROWS:, :] = jnp.zeros((8, 128), F32)
    row = iota((PAD, 128), 0)
    high, low = two_parts(states_ref[...])
    for e in range(N_SP):
        rows = jnp.where(row < CAP, total[e * CAP : e * CAP + PAD, :], 0.0)
        rows = jnp.where(row == CAP, high[e : e + 1], rows)
        rows = jnp.where(row == CAP + 1, low[e : e + 1], rows)
        out_ref[e] = rows.astype(BF)


def residual_kernel(back_ref, turned_ref, g_ref, out_ref):
    routed = mm(turned_ref[...], back_ref[...].reshape(SLOTS, 128))
    residual = (g_ref[...].astype(F32) + routed).astype(BF)
    for k in range(N_TP):
        out_ref[k] = residual


def scores_of(queries, keys, mask, causal):
    return jnp.where(causal, mm(queries * mask, keys, NT), 0.0)


def causal_blocks():
    row, col = iota((TOK, TOK), 0), iota((TOK, TOK), 1)
    return (row // BLOCK == col // BLOCK) & (col <= row)


def forward_kernel(back_ref, q_ref, k_ref, v_ref, decay_ref, out_ref, entering_ref):
    key_mask, val_mask, own = head_masks()
    rows = [back_ref[s, CAP : CAP + 2, :].astype(F32) for s in range(N_SP)]
    packed = jnp.concatenate([r[0:1] + r[1:2] for r in rows], axis=0)
    state = opened_state(packed, own)
    queries = q_ref[...].astype(F32).T
    keys = k_ref[...].astype(F32).T * SCALE
    values = v_ref[...].astype(F32)
    cumulative = block_sums(decay_ref[...].T)
    closing = closings(cumulative)
    scaled_q = queries * jnp.exp(cumulative)
    scaled_k = keys * jnp.exp(-cumulative)
    tail = keys * jnp.exp(per_block(closing) - cumulative)
    causal = causal_blocks()
    within = jnp.zeros((TOK, 128), F32)
    for h in range(2):
        scores = scores_of(scaled_q, scaled_k, key_mask[h], causal)
        within = within + mm(scores, values * val_mask[h])
    for n in range(NBLK):
        here = slice(n * BLOCK, (n + 1) * BLOCK)
        entering_ref[n] = state
        out_ref[here, :] = (within[here] + mm(scaled_q[here], state, NT)).astype(BF)
        state = jnp.exp(closing[n]) * state + mm(values[here], tail[here], TN) * own


def mixer_grad_kernel(
    place_ref, full_ref, w_ref, mixed_ref, q_ref, decay_ref, grad_ref, span_ref, sent_ref, kept_ref
):
    _, _, own = head_masks()
    grad = mm(wide(full_ref, 0, TOK), w_ref[...])
    grad_ref[...] = grad
    so_far, _ = whole_sums(block_sums(decay_ref[...].T))
    scaled = q_ref[...].astype(F32).T * jnp.exp(so_far)
    packed = packed_state(mm(grad, scaled, TN) * own)
    span_ref[...] = packed
    high, low = two_parts(packed)
    sent_ref[1024:1056, :] = high.astype(BF)
    sent_ref[1056:, :] = low.astype(BF)
    mixed = mixed_ref[...]
    first = place_ref[1] == 0
    for k in range(0, N_TP, 2):
        rows = jnp.concatenate([full_ref[k], full_ref[k + 1]], axis=1)
        part = mm(rows, mixed, TN)
        for n in range(2):
            low, high = part[n * 128 : n * 128 + 64], part[n * 128 + 64 : n * 128 + 128]
            here = slice((k + n) * 64, (k + n + 1) * 64)
            kept_ref[here, :] = jnp.where(first, low, high)
            sent_ref[here, :] = jnp.where(first, high, low).astype(BF)


def chip_kernel(place_ref, recv_ref, kept_ref, span_ref, reach_ref, sent_ref, other_ref):
    other = recv_ref[1024:1056, :].astype(F32) + recv_ref[1056:, :].astype(F32)
    other_ref[...] = other
    first = place_ref[1] == 0
    mine = span_ref[...]
    both = jnp.where(first, mine, other) + reach_ref[16:17, :] * jnp.where(first, other, mine)
    for z in range(16):
        here = slice(z * 64, (z + 1) * 64)
        sent_ref[z, :32, :] = (both * reach_ref[z : z + 1, :]).astype(BF)
        sent_ref[z, 32:, :] = (kept_ref[here, :] + recv_ref[here, :].astype(F32)).astype(BF)


def local_backward_kernel(
    grad_ref,
    entering_ref,
    q_ref,
    k_ref,
    v_ref,
    decay_ref,
    gq_ref,
    value_ref,
    keys_ref,
    change_ref,
    tail_ref,
    reach_ref,
    rest_ref,
    leave_ref,
):
    key_mask, val_mask, own = head_masks()
    grad = grad_ref[...]
    queries = q_ref[...].astype(F32).T
    keys = k_ref[...].astype(F32).T * SCALE
    values = v_ref[...].astype(F32)
    cumulative = block_sums(decay_ref[...].T)
    closing = closings(cumulative)
    grow, shrink = jnp.exp(cumulative), jnp.exp(-cumulative)
    rest = jnp.exp(per_block(closing) - cumulative)
    scaled_q, scaled_k, tail = queries * grow, keys * shrink, keys * rest
    causal = causal_blocks()
    value_grad = jnp.zeros((TOK, 128), F32)
    query_grad = jnp.zeros((TOK, 64), F32)
    key_grad = jnp.zeros((TOK, 64), F32)
    for h in range(2):
        scores = scores_of(scaled_q, scaled_k, key_mask[h], causal)
        score_grad = jnp.where(causal, mm(grad * val_mask[h], values, NT), 0.0)
        value_grad = value_grad + mm(scores, grad * val_mask[h], TN)
        query_grad = query_grad + mm(score_grad, scaled_k * key_mask[h])
        key_grad = key_grad + mm(score_grad, scaled_q * key_mask[h], TN)
    carried_v, carried_q, tail_grad, close_grad, reach = ([None] * NBLK for _ in range(5))
    state_grad, later = jnp.zeros((128, 64), F32), jnp.zeros((1, 64), F32)
    for n in reversed(range(NBLK)):
        here = slice(n * BLOCK, (n + 1) * BLOCK)
        entering = entering_ref[n]
        decay_out = jnp.exp(closing[n])
        reach[n] = jnp.exp(later)
        later = later + closing[n]
        leave_ref[n : n + 1, :] = jnp.exp(later)
        carried_v[n] = mm(tail[here], state_grad, NT)
        carried_q[n] = mm(grad[here], entering)
        tail_grad[n] = mm(values[here], state_grad)
        close_grad[n] = decay_out * jnp.sum(state_grad * entering, axis=0, keepdims=True) + jnp.sum(
            tail_grad[n] * tail[here], axis=0, keepdims=True
        )
        state_grad = decay_out * state_grad + mm(grad[here], scaled_q[here], TN) * own
    value_ref[...] = value_grad + jnp.concatenate(carried_v, axis=0)
    query_grad = query_grad + jnp.concatenate(carried_q, axis=0)
    tail_grad = jnp.concatenate(tail_grad, axis=0)
    change = query_grad * scaled_q - key_grad * scaled_k - tail_grad * tail
    row, col = iota((TOK, TOK), 0), iota((TOK, TOK), 1)
    onward = ((row // BLOCK == col // BLOCK) & (col >= row)).astype(F32)
    change_ref[...] = picked_sums(onward, change) + per_block(close_grad)
    gq_ref[...] = (query_grad * grow).T.astype(BF)
    keys_ref[...] = (key_grad * shrink + tail_grad * rest) * SCALE
    tail_ref[...] = tail
    reach_ref[...] = per_block(reach)
    rest_ref[...] = rest * SCALE


def backward_kernel(
    place_ref,
    later_ref,
    other_ref,
    chips_ref,
    entering_ref,
    v_ref,
    value_ref,
    keys_ref,
    change_ref,
    tail_ref,
    reach_ref,
    rest_ref,
    leave_ref,
    gp_ref,
    gk_ref,
    gv_ref,
    gd_ref,
):
    _, _, own = head_masks()
    sums = later_ref[0].astype(F32)
    for z in range(1, 16):
        sums = sums + later_ref[z].astype(F32)
    gp_ref[...] = sums[32:]
    packed = sums[:32]
    packed = jnp.where(place_ref[1] == 0, chips_ref[17:18, :] * packed + other_ref[...], packed)
    state_grad = opened_state(packed, own)
    tail, reach = tail_ref[...], reach_ref[...]
    gv_ref[...] = (value_ref[...] + mm(tail * reach, state_grad, NT)).astype(BF)
    tail_grad = mm(v_ref[...], state_grad) * reach
    gk_ref[...] = (keys_ref[...] + tail_grad * rest_ref[...]).T.astype(BF)
    row, col = iota((TOK, TOK), 0), iota((TOK, TOK), 1)
    ahead = ((row // BLOCK == col // BLOCK) & (col < row)).astype(F32)
    passed = [
        leave_ref[n : n + 1, :] * jnp.sum(state_grad * entering_ref[n], axis=0, keepdims=True)
        for n in range(NBLK)
    ]
    change = change_ref[...] + picked_sums(ahead, tail_grad * tail) + per_block(passed)
    gd_ref[...] = change.T


def exchanged(blocks, axis):
    return lax.all_to_all(blocks, axis, split_axis=0, concat_axis=0, tiled=True)


def ring_step(step):
    pairs = []
    for t in range(N_TP):
        y, x = t // 4, t % 4
        pairs.append((t, 4 * y + (x + step) % 4))
        pairs.append((N_TP + t, N_TP + 4 * ((y + step) % 4) + x))
    return pairs


def passed_on(array, step):
    return lax.ppermute(array, ("sp_1", "tp"), ring_step(step))


def body(
    moe_input,
    out_grad,
    routes,
    route_weight,
    w_gate,
    w_up,
    w_down,
    w_out,
    queries,
    key_rows,
    value_rows,
    log_decay,
):
    q_t, k_t, decay_t = queries.T, key_rows.T, log_decay.T
    place = jnp.stack(
        [lax.axis_index(SP), lax.axis_index("sp_1"), lax.axis_index("sp_0")]
    ).astype(jnp.int32)

    sent, pick = call(
        dispatch_kernel,
        [((N_SP, 2 * PAD, 128), BF), ((SLOTS, TOK), BF)],
        routes.T,
        route_weight.T,
        moe_input,
        out_grad,
        k_t,
        value_rows,
        decay_t,
    )
    recv = exchanged(sent, SP)
    own_a, own_b = call(
        pack_kernel, [((LOT, 128), BF), ((LOT, 128), BF)], w_gate[0], w_up[0], w_down[0]
    )
    left_a = passed_on(own_a, 1)
    right_b = passed_on(own_b, -1)
    left_b = passed_on(own_b, 1)
    right_a = passed_on(own_a, -1)
    far_a = passed_on(left_a, 1)
    far_b = passed_on(right_b, -1)
    weights = (own_a, own_b, left_a, left_b, right_a, right_b, far_a, far_b)
    (copies,) = call(
        copies_kernel,
        [((N_TP, 2 * PART, 128), BF)],
        place,
        recv,
        scratch=[pltpu.VMEM((2 * ROWS, 128), F32), pltpu.VMEM((4, 2 * PART, 128), BF)],
        smem=(0,),
        near=(1,),
        near_out=(0,),
    )
    rows = exchanged(copies, "tp")
    (mark,) = call(mark_kernel, [((8, 128), F32)], after=(rows,), near_after=True)
    (turned,) = call(turned_kernel, [((TOK, SLOTS), BF)], pick)
    partial_rows, grads, hidden = call(
        partial_kernel,
        [((N_TP, PART, 128), BF), ((PART, 1024), BF), ((PART, 512), BF)],
        rows,
        *weights,
        scratch=[pltpu.VMEM((8, LOT, 128), BF), pltpu.SemaphoreType.DMA((8,))],
        near=(0,),
        near_out=(1, 2),
        raw=tuple(range(1, 9)),
        after=(mark,),
    )
    states, reach = call(
        scan_kernel,
        [((N_SP, 128), F32), ((24, 128), F32)],
        place,
        recv,
        smem=(0,),
        after=(partial_rows,),
    )
    arrived = exchanged(partial_rows, "tp")
    own_grad_a, own_grad_b, to_left, to_right, *held_back = call(
        weight_grads_kernel,
        2 * [((LOT, 128), F32)]
        + 2 * [((LOT + EARLY, 128), BF)]
        + 2 * [((LOT, 128), BF), ((EARLY, 128), BF)],
        rows,
        grads,
        hidden,
        near=(0, 1, 2),
    )
    from_left = passed_on(to_right, 1)
    from_right = passed_on(to_left, -1)
    (returned,) = call(
        row_sum_kernel,
        [((N_SP, PAD, 128), BF)],
        place,
        arrived,
        states,
        smem=(0,),
        near=(1,),
        scratch=[pltpu.VMEM((ROWS + 8, 128), F32)],
    )
    back = exchanged(returned, SP)
    (residual,) = call(residual_kernel, [((N_TP, TOK, 128), BF)], back, turned, out_grad, near=(0,))
    full_grad = exchanged(residual, "tp")
    lot_left, lot_right = call(
        relay_kernel,
        2 * [((LOT + EARLY, 128), BF)],
        *held_back,
        from_right,
        from_left,
        after=(residual,),
        near=(4, 5),
    )
    last_a = passed_on(lot_right, 1)
    last_b = passed_on(lot_left, -1)
    mixer_out, entering = call(
        forward_kernel,
        [((TOK, 128), BF), ((NBLK, 128, 64), F32)],
        back,
        q_t,
        k_t,
        value_rows,
        decay_t,
        near=(0,),
        near_out=(0,),
        after=(residual,),
    )
    mixer_grad, span_grad, to_other, kept = call(
        mixer_grad_kernel,
        [((TOK, 128), F32), ((32, 128), F32), ((1088, 128), BF), ((1024, 128), F32)],
        place,
        full_grad,
        w_out,
        mixer_out,
        q_t,
        decay_t,
        smem=(0,),
        near=(1, 3),
        near_out=(1, 2, 3),
    )
    from_other = lax.ppermute(to_other, "sp_1", [(0, 1), (1, 0)])
    chip_sent, other_grad = call(
        chip_kernel,
        [((16, 96, 128), BF), ((32, 128), F32)],
        place,
        from_other,
        kept,
        span_grad,
        reach,
        smem=(0,),
        near=(1, 2, 3),
    )
    later = exchanged(chip_sent, "sp_0")
    gq, *local = call(
        local_backward_kernel,
        [
            ((64, TOK), BF),
            ((TOK, 128), F32),
            ((TOK, 64), F32),
            ((TOK, 64), F32),
            ((TOK, 64), F32),
            ((TOK, 64), F32),
            ((TOK, 64), F32),
            ((NBLK, 64), F32),
        ],
        mixer_grad,
        entering,
        q_t,
        k_t,
        value_rows,
        decay_t,
        after=(chip_sent,),
    )
    grad_proj, gk, gv, gd = call(
        backward_kernel,
        [((64, 128), F32), ((64, TOK), BF), ((TOK, 128), BF), ((64, TOK), F32)],
        place,
        later,
        other_grad,
        reach,
        entering,
        value_rows,
        *local,
        smem=(0,),
        near=(1,),
    )
    gate_part, up_part, down_part = call(
        grad_sum_kernel,
        [((2048, 128), BF), ((2048, 128), BF), ((128, 2048), BF)],
        own_grad_a,
        own_grad_b,
        from_right,
        from_left,
        last_a,
        last_b,
        near=(2, 3, 4, 5),
        after=(chip_sent,),
    )
    return (gate_part[None], up_part[None], down_part[None], grad_proj, gq.T, gk.T, gv, gd.T)


def solution(mesh):
    split = Mesh(mesh.devices.reshape(16, 2, mesh.shape["tp"]), ("sp_0", "sp_1", "tp"))
    placed = (
        P(SP, "tp"),
        P(SP, "tp"),
        P(SP, None),
        P(SP, None),
        P(SP, None, "tp"),
        P(SP, None, "tp"),
        P(SP, "tp", None),
        P(None, "tp"),
        P(SP, "tp"),
        P(SP, "tp"),
        P(SP, "tp"),
        P(SP, "tp"),
    )
    return jax.shard_map(
        body,
        mesh=split,
        in_specs=placed,
        out_specs=(
            P(SP, None, "tp"),
            P(SP, None, "tp"),
            P(SP, "tp", None),
            P(SP, "tp"),
            P(SP, "tp"),
            P(SP, "tp"),
            P(SP, "tp"),
            P(SP, "tp"),
        ),
        check_vma=False,
    )
```

```python
import jax
import jax.numpy as jnp
from jax import lax
from jax.experimental import pallas as pl
from jax.experimental.pallas import tpu as pltpu
from jax.sharding import Mesh
from jax.sharding import PartitionSpec as P


KEY_CHANNELS = 32
VAL_DIM = 64
TOP = 2
BLOCK = 64
CAP = 20
PAD = 24
SP = ("sp_0", "sp_1")
N_SP = 32
N_TP = 16
TOK = 256
ROWS = N_SP * CAP
SLOTS = N_SP * PAD
PART = ROWS // 4
LOT = 3 * 1024
EARLY = 2048
LATE = LOT - EARLY
NBLK = TOK // BLOCK
BF = jnp.bfloat16
F32 = jnp.float32
HI = lax.Precision.HIGHEST
SCALE = KEY_CHANNELS ** (-0.5)

NN = (((1,), (0,)), ((), ()))
NT = (((1,), (1,)), ((), ()))
TN = (((0,), (0,)), ((), ()))


def mm(a, b, dims=NN):
    return lax.dot_general(a.astype(BF), b.astype(BF), dims, preferred_element_type=F32)


def mm_exact(a, b, dims=NN):
    return lax.dot_general(a, b, dims, precision=HI, preferred_element_type=F32)


def iota(shape, dim):
    return lax.broadcasted_iota(jnp.int32, shape, dim)


def call(fn, outs, *args, scratch=(), smem=(), near=(), near_out=(), after=(), raw=()):
    spaces = [pltpu.VMEM if k in near else pltpu.HBM for k in range(len(args))]
    args = [
        a if k in smem else pltpu.with_memory_space_constraint(a, spaces[k])
        for k, a in enumerate(args)
    ]
    after = [pltpu.with_memory_space_constraint(a, pltpu.HBM) for a in after]
    count = len(args)

    def run(*refs):
        fn(*refs[:count], *refs[count + len(after) :])

    return pl.pallas_call(
        run,
        out_shape=tuple(
            (pltpu.VMEM if k in near_out else pltpu.HBM)(s, d) for k, (s, d) in enumerate(outs)
        ),
        in_specs=[
            pl.BlockSpec(
                memory_space=pltpu.SMEM if k in smem else pltpu.HBM if k in raw else pltpu.VMEM
            )
            for k in range(count)
        ]
        + [pl.BlockSpec(memory_space=pltpu.HBM) for _ in after],
        out_specs=tuple(pl.BlockSpec(memory_space=pltpu.VMEM) for _ in outs),
        scratch_shapes=scratch,
        compiler_params=pltpu.CompilerParams(vmem_limit_bytes=24 * 1024 * 1024),
    )(*args, *after)


def head_masks():
    key_lane = iota((1, 64), 1) // KEY_CHANNELS
    val_lane = iota((1, 128), 1) // VAL_DIM
    keys = [(key_lane == h).astype(F32) for h in range(2)]
    vals = [(val_lane == h).astype(F32) for h in range(2)]
    own = (iota((128, 64), 0) // VAL_DIM == iota((128, 64), 1) // KEY_CHANNELS).astype(F32)
    return keys, vals, own


def packed_state(state):
    both = state[:64] + state[64:]
    return jnp.concatenate([both[:32], both[32:]], axis=1)


def opened_state(packed, own):
    both = jnp.concatenate([packed[:, :64], packed[:, 64:]], axis=0)
    return jnp.concatenate([both, both], axis=0) * own


def picked_sums(mask, values):
    high = values.astype(BF).astype(F32)
    middle = (values - high).astype(BF).astype(F32)
    sums = mm(mask, jnp.concatenate([high, middle, values - high - middle], axis=1))
    return sums[:, :64] + sums[:, 64:128] + sums[:, 128:192]


def block_sums(decay):
    row, col = iota((TOK, TOK), 0), iota((TOK, TOK), 1)
    within = ((row // BLOCK == col // BLOCK) & (col <= row)).astype(F32)
    return picked_sums(within, decay)


def whole_sums(cumulative):
    offset, parts = jnp.zeros((1, 64), F32), []
    for n in range(NBLK):
        block = cumulative[n * BLOCK : (n + 1) * BLOCK]
        parts.append(block + offset)
        offset = offset + block[BLOCK - 1 :]
    return jnp.concatenate(parts, axis=0), offset


def closings(cumulative):
    return [cumulative[(n + 1) * BLOCK - 1 : (n + 1) * BLOCK] for n in range(NBLK)]


def per_block(rows):
    return jnp.concatenate([jnp.broadcast_to(r, (BLOCK, r.shape[1])) for r in rows], axis=0)


def two_parts(values):
    high = values.astype(BF).astype(F32)
    return high, values - high


def dispatch_kernel(
    routes_ref, weight_ref, x_ref, g_ref, k_ref, v_ref, decay_ref, sent_ref, pick_ref
):
    routes = routes_ref[...]
    expert = iota((N_SP, TOK), 0)
    hot = [(expert == routes[j : j + 1, :]) for j in range(TOP)]
    both = (hot[0] | hot[1]).astype(F32)
    before = (iota((TOK, TOK), 0) < iota((TOK, TOK), 1)).astype(F32)
    place = mm(both, before)
    owner, row = iota((SLOTS, N_SP), 0) // PAD, iota((SLOTS, N_SP), 0) % PAD
    mine = owner == iota((SLOTS, N_SP), 1)
    spread = mine.astype(F32)
    slot_place = (iota((SLOTS, TOK), 0) % PAD).astype(F32)
    picks = [(mm(spread, jnp.where(h, place, -1.0)) == slot_place).astype(F32) for h in hot]
    pick = picks[0] + picks[1]
    pick_ref[...] = pick.astype(BF)

    _, _, own = head_masks()
    keys = k_ref[...].astype(F32).T * SCALE
    so_far, total = whole_sums(block_sums(decay_ref[...].T))
    state = mm(v_ref[...], keys * jnp.exp(total - so_far), TN) * own
    state_high, state_low = two_parts(packed_state(state))
    total_row = jnp.concatenate(two_parts(total), axis=1)

    extra = jnp.concatenate(
        [(mine & (row == CAP)).astype(F32), (mine & (row == CAP + 1)).astype(F32)], axis=1
    )
    state_rows = mm(extra, jnp.concatenate([state_high, state_low], axis=0))

    grad = g_ref[...].astype(F32)
    weight = jnp.concatenate([weight_ref[...], jnp.zeros((6, TOK), F32)], axis=0).T
    sent = jnp.zeros((SLOTS, 256), F32)
    for j in range(TOP):
        rows = [x_ref[...], (weight[:, j : j + 1] * grad).astype(BF)]
        sent = sent + mm(picks[j], jnp.concatenate(rows, axis=1))
    sent_ref[:, :PAD, :] = (sent[:, :128] + state_rows).astype(BF).reshape(N_SP, PAD, 128)
    sent = jnp.where(iota((SLOTS, 128), 0) % PAD == CAP, total_row, sent[:, 128:])
    sent_ref[:, PAD:, :] = sent.astype(BF).reshape(N_SP, PAD, 128)


def turned_kernel(pick_ref, out_ref):
    out_ref[...] = pick_ref[...].astype(F32).T.astype(BF)


def quarter_of(place_ref, k):
    return jnp.where(place_ref[1] == 0, k % 4, k // 4)


def copies_kernel(place_ref, recv_ref, out_ref, packed, rounded):
    for e in range(N_SP):
        block = recv_ref[e].astype(F32)
        at = (e // 8) * 2 * PART + (e % 8) * CAP
        packed[at : at + CAP, :] = block[:CAP]
        packed[at + PART : at + PART + CAP, :] = block[PAD : PAD + CAP]
    for q in range(4):
        rounded[q] = packed[q * 2 * PART : (q + 1) * 2 * PART, :].astype(BF)
    for k in range(N_TP):
        out_ref[k] = rounded[quarter_of(place_ref, k)]


def scan_kernel(place_ref, recv_ref, states_ref, reach_ref):
    chip = place_ref[2]
    totals = [recv_ref[s, PAD + CAP : PAD + CAP + 1, :].astype(F32) for s in range(N_SP)]
    totals = jnp.concatenate(totals, axis=0)
    totals = totals[:, :64] + totals[:, 64:]
    double = jnp.concatenate([totals, totals], axis=1)
    decays = jnp.exp(double)
    state = jnp.zeros((1, 128), F32)
    for s in range(N_SP):
        states_ref[s : s + 1, :] = state
        pair = recv_ref[s, CAP : CAP + 2, :].astype(F32)
        state = decays[s : s + 1] * state + pair[0:1] + pair[1:2]
    target, between = iota((16, N_SP), 0), iota((16, N_SP), 1)
    passed = ((between >= 2 * target + 2) & (between < 2 * chip)).astype(F32)
    reach = jnp.exp(mm_exact(passed, double))
    reach_ref[:16, :] = jnp.where(iota((16, 128), 0) < chip, reach, 0.0)
    here = iota((N_SP, 128), 0)
    even = jnp.sum(jnp.where(here == 2 * chip, decays, 0.0), axis=0, keepdims=True)
    odd = jnp.sum(jnp.where(here == 2 * chip + 1, decays, 0.0), axis=0, keepdims=True)
    reach_ref[16:, :] = jnp.concatenate([even, odd, jnp.zeros((6, 128), F32)], axis=0)


def pack_kernel(wg_ref, wu_ref, wd_ref, a_ref, b_ref):
    a_ref[:2048, :] = wg_ref[...]
    a_ref[2048:, :] = wu_ref[:1024, :]
    b_ref[:1024, :] = wu_ref[1024:, :]
    for k in range(N_TP):
        b_ref[1024 + k * 128 : 1152 + k * 128, :] = wd_ref[:, k * 128 : (k + 1) * 128]


def wide(ref, at, size):
    return jnp.concatenate([ref[k, at : at + size, :] for k in range(N_TP)], axis=1)


def partial_kernel(rows_ref, *refs):
    lots, (part_ref, grads_ref, hidden_ref, held, done) = refs[:8], refs[8:]
    copies = [pltpu.make_async_copy(lots[i], held.at[i], done.at[i]) for i in range(8)]
    for copy in copies:
        copy.start()
    x, g = wide(rows_ref, 0, PART), wide(rows_ref, PART, PART)
    for b in range(4):
        copies[2 * b].wait()
        copies[2 * b + 1].wait()
        gate_weight = held[2 * b, :2048, :]
        up_weight = jnp.concatenate([held[2 * b, 2048:, :], held[2 * b + 1, :1024, :]], axis=0)
        blocks = [held[2 * b + 1, 1024 + k * 128 : 1152 + k * 128, :] for k in range(N_TP)]
        pre = mm(x, jnp.concatenate([gate_weight, up_weight], axis=1))
        upper = mm(g, jnp.concatenate(blocks, axis=1), NT)
        gate_pre, up_pre = pre[:, :128], pre[:, 128:]
        sigmoid = jax.nn.sigmoid(gate_pre)
        activated = gate_pre * sigmoid
        hidden_ref[:, 128 * b : 128 * b + 128] = (activated * up_pre).astype(BF)
        gate = upper * up_pre * sigmoid * (1.0 + gate_pre * (1.0 - sigmoid))
        grads_ref[:, 256 * b : 256 * b + 128] = gate.astype(BF)
        grads_ref[:, 256 * b + 128 : 256 * b + 256] = (upper * activated).astype(BF)
    grads = grads_ref[...]

    def up_rows(b, at):
        if at < 1024:
            return held[2 * b, 2048 + at : 2304 + at, :]
        return held[2 * b + 1, at - 1024 : at - 768, :]

    for k in range(0, N_TP, 2):
        at = k * 128
        weight = []
        for b in range(4):
            weight += [held[2 * b, at : at + 256, :], up_rows(b, at)]
        part = mm(grads, jnp.concatenate(weight, axis=1), NT).astype(BF)
        part_ref[k] = part[:, :128]
        part_ref[k + 1] = part[:, 128:]


def weight_grads_kernel(rows_ref, grads_ref, hidden_ref, *out_refs):
    grads = grads_ref[...]
    hidden = hidden_ref[...]
    for k in range(0, N_TP, 2):
        x = jnp.concatenate([rows_ref[k, :PART, :], rows_ref[k + 1, :PART, :]], axis=1)
        g = jnp.concatenate([rows_ref[k, PART:, :], rows_ref[k + 1, PART:, :]], axis=1)
        both = mm(x, grads, TN)
        down = mm(hidden, g, TN)
        at = k * 128
        for b in range(4):

            def put(lot, row, value):
                ref, start = place_of(out_refs, b, lot, row)
                ref[start : start + len(value), :] = value.astype(ref.dtype)

            put(0, at, both[:, 256 * b : 256 * b + 128])
            up = both[:, 256 * b + 128 : 256 * b + 256]
            if k < N_TP // 2:
                put(0, 2048 + at, up)
            else:
                put(1, at - 1024, up)
            for n in range(2):
                block = down[128 * b : 128 * b + 128, n * 128 : (n + 1) * 128]
                put(1, 1024 + at + n * 128, block)


def place_of(refs, device, lot, row):
    own_a, own_b, to_left, to_right, left_b, left_late, right_a, right_late = refs
    if device == 0:
        return (own_a, own_b)[lot], row
    if device == 3:
        return ((to_right, row), (to_left, EARLY + row))[lot]
    if device == 1:
        if lot == 1:
            return left_b, row
        return (to_left, row) if row < EARLY else (left_late, row - EARLY)
    if lot == 0:
        return right_a, row
    return (to_right, LOT + row) if row < EARLY else (right_late, row - EARLY)


def relay_kernel(
    left_b_ref,
    left_late_ref,
    right_a_ref,
    right_late_ref,
    from_right_ref,
    from_left_ref,
    to_left_ref,
    to_right_ref,
):
    far_a, far_b = from_left_ref[:LOT, :].astype(F32), from_right_ref[EARLY:, :].astype(F32)
    to_right_ref[:LOT, :] = (right_a_ref[...].astype(F32) + far_a).astype(BF)
    to_right_ref[LOT:, :] = right_late_ref[...]
    to_left_ref[:LATE, :] = left_late_ref[...]
    to_left_ref[LATE:, :] = (left_b_ref[...].astype(F32) + far_b).astype(BF)


def grad_sum_kernel(
    own_a_ref,
    own_b_ref,
    from_right_ref,
    from_left_ref,
    last_left_ref,
    last_right_ref,
    gate_ref,
    up_ref,
    down_ref,
):
    def total(at):
        lot, row = divmod(at, LOT)
        if lot == 0:
            own, summed = (own_a_ref, row), (last_left_ref, row)
            single = (from_right_ref if row < EARLY else last_right_ref, row % EARLY)
        else:
            own, summed = (own_b_ref, row), (last_right_ref, LATE + row)
            single = (from_left_ref if row < EARLY else last_left_ref, LOT + row % EARLY)
        rows = [r[start : start + 128, :].astype(F32) for r, start in (own, summed, single)]
        return (rows[0] + rows[1] + rows[2]).astype(BF)

    for k in range(N_TP):
        here = slice(k * 128, (k + 1) * 128)
        gate_ref[here, :] = total(k * 128)
        up_ref[here, :] = total(2048 + k * 128)
        down_ref[:, here] = total(4096 + k * 128)


def row_sum_kernel(place_ref, part_ref, states_ref, out_ref, total):
    for q in range(4):
        acc = jnp.zeros((PART, 128), F32)
        for j in range(4):
            source = jnp.where(place_ref[1] == 0, 4 * j + q, 4 * q + j)
            acc = acc + part_ref[source].astype(F32)
        total[q * PART : (q + 1) * PART, :] = acc
    total[ROWS:, :] = jnp.zeros((8, 128), F32)
    row = iota((PAD, 128), 0)
    high, low = two_parts(states_ref[...])
    for e in range(N_SP):
        rows = jnp.where(row < CAP, total[e * CAP : e * CAP + PAD, :], 0.0)
        rows = jnp.where(row == CAP, high[e : e + 1], rows)
        rows = jnp.where(row == CAP + 1, low[e : e + 1], rows)
        out_ref[e] = rows.astype(BF)


def residual_kernel(back_ref, turned_ref, g_ref, out_ref):
    routed = mm(turned_ref[...], back_ref[...].reshape(SLOTS, 128))
    residual = (g_ref[...].astype(F32) + routed).astype(BF)
    for k in range(N_TP):
        out_ref[k] = residual


def scores_of(queries, keys, mask, causal):
    return jnp.where(causal, mm(queries * mask, keys, NT), 0.0)


def causal_blocks():
    row, col = iota((TOK, TOK), 0), iota((TOK, TOK), 1)
    return (row // BLOCK == col // BLOCK) & (col <= row)


def forward_kernel(back_ref, q_ref, k_ref, v_ref, decay_ref, out_ref, entering_ref):
    key_mask, val_mask, own = head_masks()
    rows = [back_ref[s, CAP : CAP + 2, :].astype(F32) for s in range(N_SP)]
    packed = jnp.concatenate([r[0:1] + r[1:2] for r in rows], axis=0)
    state = opened_state(packed, own)
    queries = q_ref[...].astype(F32).T
    keys = k_ref[...].astype(F32).T * SCALE
    values = v_ref[...].astype(F32)
    cumulative = block_sums(decay_ref[...].T)
    closing = closings(cumulative)
    scaled_q = queries * jnp.exp(cumulative)
    scaled_k = keys * jnp.exp(-cumulative)
    tail = keys * jnp.exp(per_block(closing) - cumulative)
    causal = causal_blocks()
    within = jnp.zeros((TOK, 128), F32)
    for h in range(2):
        scores = scores_of(scaled_q, scaled_k, key_mask[h], causal)
        within = within + mm(scores, values * val_mask[h])
    for n in range(NBLK):
        here = slice(n * BLOCK, (n + 1) * BLOCK)
        entering_ref[n] = state
        out_ref[here, :] = (within[here] + mm(scaled_q[here], state, NT)).astype(BF)
        state = jnp.exp(closing[n]) * state + mm(values[here], tail[here], TN) * own


def mixer_grad_kernel(
    place_ref, full_ref, w_ref, mixed_ref, q_ref, decay_ref, grad_ref, span_ref, sent_ref, kept_ref
):
    _, _, own = head_masks()
    grad = mm(wide(full_ref, 0, TOK), w_ref[...])
    grad_ref[...] = grad
    so_far, _ = whole_sums(block_sums(decay_ref[...].T))
    scaled = q_ref[...].astype(F32).T * jnp.exp(so_far)
    packed = packed_state(mm(grad, scaled, TN) * own)
    span_ref[...] = packed
    high, low = two_parts(packed)
    sent_ref[1024:1056, :] = high.astype(BF)
    sent_ref[1056:, :] = low.astype(BF)
    mixed = mixed_ref[...]
    first = place_ref[1] == 0
    for k in range(0, N_TP, 2):
        rows = jnp.concatenate([full_ref[k], full_ref[k + 1]], axis=1)
        part = mm(rows, mixed, TN)
        for n in range(2):
            low, high = part[n * 128 : n * 128 + 64], part[n * 128 + 64 : n * 128 + 128]
            here = slice((k + n) * 64, (k + n + 1) * 64)
            kept_ref[here, :] = jnp.where(first, low, high)
            sent_ref[here, :] = jnp.where(first, high, low).astype(BF)


def chip_kernel(place_ref, recv_ref, kept_ref, span_ref, reach_ref, sent_ref, other_ref):
    other = recv_ref[1024:1056, :].astype(F32) + recv_ref[1056:, :].astype(F32)
    other_ref[...] = other
    first = place_ref[1] == 0
    mine = span_ref[...]
    both = jnp.where(first, mine, other) + reach_ref[16:17, :] * jnp.where(first, other, mine)
    for z in range(16):
        here = slice(z * 64, (z + 1) * 64)
        sent_ref[z, :32, :] = (both * reach_ref[z : z + 1, :]).astype(BF)
        sent_ref[z, 32:, :] = (kept_ref[here, :] + recv_ref[here, :].astype(F32)).astype(BF)


def local_backward_kernel(
    grad_ref,
    entering_ref,
    q_ref,
    k_ref,
    v_ref,
    decay_ref,
    gq_ref,
    value_ref,
    keys_ref,
    change_ref,
    tail_ref,
    reach_ref,
    rest_ref,
    leave_ref,
):
    key_mask, val_mask, own = head_masks()
    grad = grad_ref[...]
    queries = q_ref[...].astype(F32).T
    keys = k_ref[...].astype(F32).T * SCALE
    values = v_ref[...].astype(F32)
    cumulative = block_sums(decay_ref[...].T)
    closing = closings(cumulative)
    grow, shrink = jnp.exp(cumulative), jnp.exp(-cumulative)
    rest = jnp.exp(per_block(closing) - cumulative)
    scaled_q, scaled_k, tail = queries * grow, keys * shrink, keys * rest
    causal = causal_blocks()
    value_grad = jnp.zeros((TOK, 128), F32)
    query_grad = jnp.zeros((TOK, 64), F32)
    key_grad = jnp.zeros((TOK, 64), F32)
    for h in range(2):
        scores = scores_of(scaled_q, scaled_k, key_mask[h], causal)
        score_grad = jnp.where(causal, mm(grad * val_mask[h], values, NT), 0.0)
        value_grad = value_grad + mm(scores, grad * val_mask[h], TN)
        query_grad = query_grad + mm(score_grad, scaled_k * key_mask[h])
        key_grad = key_grad + mm(score_grad, scaled_q * key_mask[h], TN)
    carried_v, carried_q, tail_grad, close_grad, reach = ([None] * NBLK for _ in range(5))
    state_grad, later = jnp.zeros((128, 64), F32), jnp.zeros((1, 64), F32)
    for n in reversed(range(NBLK)):
        here = slice(n * BLOCK, (n + 1) * BLOCK)
        entering = entering_ref[n]
        decay_out = jnp.exp(closing[n])
        reach[n] = jnp.exp(later)
        later = later + closing[n]
        leave_ref[n : n + 1, :] = jnp.exp(later)
        carried_v[n] = mm(tail[here], state_grad, NT)
        carried_q[n] = mm(grad[here], entering)
        tail_grad[n] = mm(values[here], state_grad)
        close_grad[n] = decay_out * jnp.sum(state_grad * entering, axis=0, keepdims=True) + jnp.sum(
            tail_grad[n] * tail[here], axis=0, keepdims=True
        )
        state_grad = decay_out * state_grad + mm(grad[here], scaled_q[here], TN) * own
    value_ref[...] = value_grad + jnp.concatenate(carried_v, axis=0)
    query_grad = query_grad + jnp.concatenate(carried_q, axis=0)
    tail_grad = jnp.concatenate(tail_grad, axis=0)
    change = query_grad * scaled_q - key_grad * scaled_k - tail_grad * tail
    row, col = iota((TOK, TOK), 0), iota((TOK, TOK), 1)
    onward = ((row // BLOCK == col // BLOCK) & (col >= row)).astype(F32)
    change_ref[...] = picked_sums(onward, change) + per_block(close_grad)
    gq_ref[...] = (query_grad * grow).T.astype(BF)
    keys_ref[...] = (key_grad * shrink + tail_grad * rest) * SCALE
    tail_ref[...] = tail
    reach_ref[...] = per_block(reach)
    rest_ref[...] = rest * SCALE


def backward_kernel(
    place_ref,
    later_ref,
    other_ref,
    chips_ref,
    entering_ref,
    v_ref,
    value_ref,
    keys_ref,
    change_ref,
    tail_ref,
    reach_ref,
    rest_ref,
    leave_ref,
    gp_ref,
    gk_ref,
    gv_ref,
    gd_ref,
):
    _, _, own = head_masks()
    sums = later_ref[0].astype(F32)
    for z in range(1, 16):
        sums = sums + later_ref[z].astype(F32)
    gp_ref[...] = sums[32:]
    packed = sums[:32]
    packed = jnp.where(place_ref[1] == 0, chips_ref[17:18, :] * packed + other_ref[...], packed)
    state_grad = opened_state(packed, own)
    tail, reach = tail_ref[...], reach_ref[...]
    gv_ref[...] = (value_ref[...] + mm(tail * reach, state_grad, NT)).astype(BF)
    tail_grad = mm(v_ref[...], state_grad) * reach
    gk_ref[...] = (keys_ref[...] + tail_grad * rest_ref[...]).T.astype(BF)
    row, col = iota((TOK, TOK), 0), iota((TOK, TOK), 1)
    ahead = ((row // BLOCK == col // BLOCK) & (col < row)).astype(F32)
    passed = [
        leave_ref[n : n + 1, :] * jnp.sum(state_grad * entering_ref[n], axis=0, keepdims=True)
        for n in range(NBLK)
    ]
    change = change_ref[...] + picked_sums(ahead, tail_grad * tail) + per_block(passed)
    gd_ref[...] = change.T


def exchanged(blocks, axis):
    return lax.all_to_all(blocks, axis, split_axis=0, concat_axis=0, tiled=True)


def ring_step(step):
    pairs = []
    for t in range(N_TP):
        y, x = t // 4, t % 4
        pairs.append((t, 4 * y + (x + step) % 4))
        pairs.append((N_TP + t, N_TP + 4 * ((y + step) % 4) + x))
    return pairs


def passed_on(array, step):
    return lax.ppermute(array, ("sp_1", "tp"), ring_step(step))


def body(
    moe_input,
    out_grad,
    routes,
    route_weight,
    w_gate,
    w_up,
    w_down,
    w_out,
    queries,
    key_rows,
    value_rows,
    log_decay,
):
    q_t, k_t, decay_t = queries.T, key_rows.T, log_decay.T
    place = jnp.stack(
        [lax.axis_index(SP), lax.axis_index("sp_1"), lax.axis_index("sp_0")]
    ).astype(jnp.int32)

    sent, pick = call(
        dispatch_kernel,
        [((N_SP, 2 * PAD, 128), BF), ((SLOTS, TOK), BF)],
        routes.T,
        route_weight.T,
        moe_input,
        out_grad,
        k_t,
        value_rows,
        decay_t,
    )
    recv = exchanged(sent, SP)
    own_a, own_b = call(
        pack_kernel,
        [((LOT, 128), BF), ((LOT, 128), BF)],
        w_gate[0],
        w_up[0],
        w_down[0],
        near_out=(0, 1),
    )
    left_a = passed_on(own_a, 1)
    right_b = passed_on(own_b, -1)
    left_b = passed_on(own_b, 1)
    right_a = passed_on(own_a, -1)
    far_a = passed_on(left_a, 1)
    far_b = passed_on(right_b, -1)
    weights = (own_a, own_b, left_a, left_b, right_a, right_b, far_a, far_b)
    (copies,) = call(
        copies_kernel,
        [((N_TP, 2 * PART, 128), BF)],
        place,
        recv,
        scratch=[pltpu.VMEM((2 * ROWS, 128), F32), pltpu.VMEM((4, 2 * PART, 128), BF)],
        smem=(0,),
        near=(1,),
    )
    rows = exchanged(copies, "tp")
    (turned,) = call(turned_kernel, [((TOK, SLOTS), BF)], pick, after=(copies,))
    partial_rows, grads, hidden = call(
        partial_kernel,
        [((N_TP, PART, 128), BF), ((PART, 1024), BF), ((PART, 512), BF)],
        rows,
        *weights,
        scratch=[pltpu.VMEM((8, LOT, 128), BF), pltpu.SemaphoreType.DMA((8,))],
        near=(0,),
        near_out=(1, 2),
        raw=tuple(range(1, 9)),
    )
    states, reach = call(
        scan_kernel,
        [((N_SP, 128), F32), ((24, 128), F32)],
        place,
        recv,
        smem=(0,),
        after=(partial_rows,),
    )
    arrived = exchanged(partial_rows, "tp")
    own_grad_a, own_grad_b, to_left, to_right, *held_back = call(
        weight_grads_kernel,
        2 * [((LOT, 128), F32)]
        + 2 * [((LOT + EARLY, 128), BF)]
        + 2 * [((LOT, 128), BF), ((LATE, 128), BF)],
        rows,
        grads,
        hidden,
        near=(0, 1, 2),
    )
    from_left = passed_on(to_right, 1)
    from_right = passed_on(to_left, -1)
    (returned,) = call(
        row_sum_kernel,
        [((N_SP, PAD, 128), BF)],
        place,
        arrived,
        states,
        smem=(0,),
        near=(1,),
        scratch=[pltpu.VMEM((ROWS + 8, 128), F32)],
    )
    back = exchanged(returned, SP)
    (residual,) = call(residual_kernel, [((N_TP, TOK, 128), BF)], back, turned, out_grad, near=(0,))
    full_grad = exchanged(residual, "tp")
    lot_left, lot_right = call(
        relay_kernel,
        2 * [((LOT + LATE, 128), BF)],
        *held_back,
        from_right,
        from_left,
        after=(residual,),
        near=(4, 5),
    )
    last_a = passed_on(lot_right, 1)
    last_b = passed_on(lot_left, -1)
    mixer_out, entering = call(
        forward_kernel,
        [((TOK, 128), BF), ((NBLK, 128, 64), F32)],
        back,
        q_t,
        k_t,
        value_rows,
        decay_t,
        near=(0,),
        near_out=(0,),
        after=(residual,),
    )
    mixer_grad, span_grad, to_other, kept = call(
        mixer_grad_kernel,
        [((TOK, 128), F32), ((32, 128), F32), ((1088, 128), BF), ((1024, 128), F32)],
        place,
        full_grad,
        w_out,
        mixer_out,
        q_t,
        decay_t,
        smem=(0,),
        near=(1, 3),
        near_out=(1, 2, 3),
    )
    from_other = lax.ppermute(to_other, "sp_1", [(0, 1), (1, 0)])
    chip_sent, other_grad = call(
        chip_kernel,
        [((16, 96, 128), BF), ((32, 128), F32)],
        place,
        from_other,
        kept,
        span_grad,
        reach,
        smem=(0,),
        near=(1, 2, 3),
    )
    later = exchanged(chip_sent, "sp_0")
    gq, *local = call(
        local_backward_kernel,
        [
            ((64, TOK), BF),
            ((TOK, 128), F32),
            ((TOK, 64), F32),
            ((TOK, 64), F32),
            ((TOK, 64), F32),
            ((TOK, 64), F32),
            ((TOK, 64), F32),
            ((NBLK, 64), F32),
        ],
        mixer_grad,
        entering,
        q_t,
        k_t,
        value_rows,
        decay_t,
        after=(chip_sent,),
    )
    grad_proj, gk, gv, gd = call(
        backward_kernel,
        [((64, 128), F32), ((64, TOK), BF), ((TOK, 128), BF), ((64, TOK), F32)],
        place,
        later,
        other_grad,
        reach,
        entering,
        value_rows,
        *local,
        smem=(0,),
        near=(1,),
    )
    gate_part, up_part, down_part = call(
        grad_sum_kernel,
        [((2048, 128), BF), ((2048, 128), BF), ((128, 2048), BF)],
        own_grad_a,
        own_grad_b,
        from_right,
        from_left,
        last_a,
        last_b,
        near=(2, 3, 4, 5),
        after=(chip_sent,),
    )
    return (gate_part[None], up_part[None], down_part[None], grad_proj, gq.T, gk.T, gv, gd.T)


def solution(mesh):
    split = Mesh(mesh.devices.reshape(16, 2, mesh.shape["tp"]), ("sp_0", "sp_1", "tp"))
    placed = (
        P(SP, "tp"),
        P(SP, "tp"),
        P(SP, None),
        P(SP, None),
        P(SP, None, "tp"),
        P(SP, None, "tp"),
        P(SP, "tp", None),
        P(None, "tp"),
        P(SP, "tp"),
        P(SP, "tp"),
        P(SP, "tp"),
        P(SP, "tp"),
    )
    return jax.shard_map(
        body,
        mesh=split,
        in_specs=placed,
        out_specs=(
            P(SP, None, "tp"),
            P(SP, None, "tp"),
            P(SP, "tp", None),
            P(SP, "tp"),
            P(SP, "tp"),
            P(SP, "tp"),
            P(SP, "tp"),
            P(SP, "tp"),
        ),
        check_vma=False,
    )
```

```python
import jax
import jax.numpy as jnp
from jax import lax
from jax.experimental import pallas as pl
from jax.experimental.pallas import tpu as pltpu
from jax.sharding import Mesh
from jax.sharding import PartitionSpec as P


KEY_CHANNELS = 32
VAL_DIM = 64
TOP = 2
BLOCK = 64
CAP = 20
PAD = 24
SP = ("sp_0", "sp_1")
N_SP = 32
N_TP = 16
TOK = 256
ROWS = N_SP * CAP
SLOTS = N_SP * PAD
PART = ROWS // 4
LOT = 3 * 1024
EARLY = LOT // 2
NBLK = TOK // BLOCK
BF = jnp.bfloat16
F32 = jnp.float32
HI = lax.Precision.HIGHEST
SCALE = KEY_CHANNELS ** (-0.5)

NN = (((1,), (0,)), ((), ()))
NT = (((1,), (1,)), ((), ()))
TN = (((0,), (0,)), ((), ()))


def mm(a, b, dims=NN):
    return lax.dot_general(a.astype(BF), b.astype(BF), dims, preferred_element_type=F32)


def mm_exact(a, b, dims=NN):
    return lax.dot_general(a, b, dims, precision=HI, preferred_element_type=F32)


def iota(shape, dim):
    return lax.broadcasted_iota(jnp.int32, shape, dim)


def call(fn, outs, *args, scratch=(), smem=(), near=(), near_out=(), after=(), raw=()):
    spaces = [pltpu.VMEM if k in near else pltpu.HBM for k in range(len(args))]
    args = [
        a if k in smem else pltpu.with_memory_space_constraint(a, spaces[k])
        for k, a in enumerate(args)
    ]
    after = [pltpu.with_memory_space_constraint(a, pltpu.HBM) for a in after]
    count = len(args)

    def run(*refs):
        fn(*refs[:count], *refs[count + len(after) :])

    return pl.pallas_call(
        run,
        out_shape=tuple(
            (pltpu.VMEM if k in near_out else pltpu.HBM)(s, d) for k, (s, d) in enumerate(outs)
        ),
        in_specs=[
            pl.BlockSpec(
                memory_space=pltpu.SMEM if k in smem else pltpu.HBM if k in raw else pltpu.VMEM
            )
            for k in range(count)
        ]
        + [pl.BlockSpec(memory_space=pltpu.HBM) for _ in after],
        out_specs=tuple(pl.BlockSpec(memory_space=pltpu.VMEM) for _ in outs),
        scratch_shapes=scratch,
        compiler_params=pltpu.CompilerParams(vmem_limit_bytes=18 * 1024 * 1024),
    )(*args, *after)


def head_masks():
    key_lane = iota((1, 64), 1) // KEY_CHANNELS
    val_lane = iota((1, 128), 1) // VAL_DIM
    keys = [(key_lane == h).astype(F32) for h in range(2)]
    vals = [(val_lane == h).astype(F32) for h in range(2)]
    own = (iota((128, 64), 0) // VAL_DIM == iota((128, 64), 1) // KEY_CHANNELS).astype(F32)
    return keys, vals, own


def packed_state(state):
    both = state[:64] + state[64:]
    return jnp.concatenate([both[:32], both[32:]], axis=1)


def opened_state(packed, own):
    both = jnp.concatenate([packed[:, :64], packed[:, 64:]], axis=0)
    return jnp.concatenate([both, both], axis=0) * own


def picked_sums(mask, values):
    high = values.astype(BF).astype(F32)
    middle = (values - high).astype(BF).astype(F32)
    sums = mm(mask, jnp.concatenate([high, middle, values - high - middle], axis=1))
    return sums[:, :64] + sums[:, 64:128] + sums[:, 128:192]


def block_sums(decay):
    row, col = iota((TOK, TOK), 0), iota((TOK, TOK), 1)
    within = ((row // BLOCK == col // BLOCK) & (col <= row)).astype(F32)
    return picked_sums(within, decay)


def whole_sums(cumulative):
    offset, parts = jnp.zeros((1, 64), F32), []
    for n in range(NBLK):
        block = cumulative[n * BLOCK : (n + 1) * BLOCK]
        parts.append(block + offset)
        offset = offset + block[BLOCK - 1 :]
    return jnp.concatenate(parts, axis=0), offset


def closings(cumulative):
    return [cumulative[(n + 1) * BLOCK - 1 : (n + 1) * BLOCK] for n in range(NBLK)]


def per_block(rows):
    return jnp.concatenate([jnp.broadcast_to(r, (BLOCK, r.shape[1])) for r in rows], axis=0)


def two_parts(values):
    high = values.astype(BF).astype(F32)
    return high, values - high


def dispatch_kernel(
    routes_ref, weight_ref, x_ref, g_ref, k_ref, v_ref, decay_ref, sent_ref, pick_ref
):
    routes = routes_ref[...]
    expert = iota((N_SP, TOK), 0)
    hot = [(expert == routes[j : j + 1, :]) for j in range(TOP)]
    both = (hot[0] | hot[1]).astype(F32)
    before = (iota((TOK, TOK), 0) < iota((TOK, TOK), 1)).astype(F32)
    place = mm(both, before)
    owner, row = iota((SLOTS, N_SP), 0) // PAD, iota((SLOTS, N_SP), 0) % PAD
    mine = owner == iota((SLOTS, N_SP), 1)
    spread = mine.astype(F32)
    slot_place = (iota((SLOTS, TOK), 0) % PAD).astype(F32)
    picks = [(mm(spread, jnp.where(h, place, -1.0)) == slot_place).astype(F32) for h in hot]
    pick = picks[0] + picks[1]
    pick_ref[...] = pick.astype(BF)

    _, _, own = head_masks()
    keys = k_ref[...].astype(F32).T * SCALE
    so_far, total = whole_sums(block_sums(decay_ref[...].T))
    state = mm(v_ref[...], keys * jnp.exp(total - so_far), TN) * own
    state_high, state_low = two_parts(packed_state(state))
    total_row = jnp.concatenate(two_parts(total), axis=1)

    extra = jnp.concatenate(
        [(mine & (row == CAP)).astype(F32), (mine & (row == CAP + 1)).astype(F32)], axis=1
    )
    state_rows = mm(extra, jnp.concatenate([state_high, state_low], axis=0))

    grad = g_ref[...].astype(F32)
    weight = jnp.concatenate([weight_ref[...], jnp.zeros((6, TOK), F32)], axis=0).T
    sent = jnp.zeros((SLOTS, 256), F32)
    for j in range(TOP):
        rows = [x_ref[...], (weight[:, j : j + 1] * grad).astype(BF)]
        sent = sent + mm(picks[j], jnp.concatenate(rows, axis=1))
    sent_ref[:, :PAD, :] = (sent[:, :128] + state_rows).astype(BF).reshape(N_SP, PAD, 128)
    sent = jnp.where(iota((SLOTS, 128), 0) % PAD == CAP, total_row, sent[:, 128:])
    sent_ref[:, PAD:, :] = sent.astype(BF).reshape(N_SP, PAD, 128)


def turned_kernel(pick_ref, out_ref):
    out_ref[...] = pick_ref[...].astype(F32).T.astype(BF)


def quarter_of(place_ref, k):
    return jnp.where(place_ref[1] == 0, k % 4, k // 4)


def copies_kernel(place_ref, recv_ref, out_ref, packed, rounded):
    for e in range(N_SP):
        block = recv_ref[e].astype(F32)
        at = (e // 8) * 2 * PART + (e % 8) * CAP
        packed[at : at + CAP, :] = block[:CAP]
        packed[at + PART : at + PART + CAP, :] = block[PAD : PAD + CAP]
    for q in range(4):
        rounded[q] = packed[q * 2 * PART : (q + 1) * 2 * PART, :].astype(BF)
    for k in range(N_TP):
        out_ref[k] = rounded[quarter_of(place_ref, k)]


def scan_kernel(place_ref, recv_ref, states_ref, reach_ref):
    chip = place_ref[2]
    totals = [recv_ref[s, PAD + CAP : PAD + CAP + 1, :].astype(F32) for s in range(N_SP)]
    totals = jnp.concatenate(totals, axis=0)
    totals = totals[:, :64] + totals[:, 64:]
    double = jnp.concatenate([totals, totals], axis=1)
    decays = jnp.exp(double)
    state = jnp.zeros((1, 128), F32)
    for s in range(N_SP):
        states_ref[s : s + 1, :] = state
        pair = recv_ref[s, CAP : CAP + 2, :].astype(F32)
        state = decays[s : s + 1] * state + pair[0:1] + pair[1:2]
    target, between = iota((16, N_SP), 0), iota((16, N_SP), 1)
    passed = ((between >= 2 * target + 2) & (between < 2 * chip)).astype(F32)
    reach = jnp.exp(mm_exact(passed, double))
    reach_ref[:16, :] = jnp.where(iota((16, 128), 0) < chip, reach, 0.0)
    here = iota((N_SP, 128), 0)
    even = jnp.sum(jnp.where(here == 2 * chip, decays, 0.0), axis=0, keepdims=True)
    odd = jnp.sum(jnp.where(here == 2 * chip + 1, decays, 0.0), axis=0, keepdims=True)
    reach_ref[16:, :] = jnp.concatenate([even, odd, jnp.zeros((6, 128), F32)], axis=0)


def pack_kernel(wg_ref, wu_ref, wd_ref, a_ref, b_ref):
    a_ref[:2048, :] = wg_ref[...]
    a_ref[2048:, :] = wu_ref[:1024, :]
    b_ref[:1024, :] = wu_ref[1024:, :]
    for k in range(N_TP):
        b_ref[1024 + k * 128 : 1152 + k * 128, :] = wd_ref[:, k * 128 : (k + 1) * 128]


def wide(ref, at, size):
    return jnp.concatenate([ref[k, at : at + size, :] for k in range(N_TP)], axis=1)


def partial_kernel(rows_ref, *refs):
    lots, (part_ref, grads_ref, hidden_ref, held, done) = refs[:8], refs[8:]
    copies = [pltpu.make_async_copy(lots[i], held.at[i], done.at[i]) for i in range(8)]
    for copy in copies:
        copy.start()
    x, g = wide(rows_ref, 0, PART), wide(rows_ref, PART, PART)
    for b in range(4):
        copies[2 * b].wait()
        copies[2 * b + 1].wait()
        gate_weight = held[2 * b, :2048, :]
        up_weight = jnp.concatenate([held[2 * b, 2048:, :], held[2 * b + 1, :1024, :]], axis=0)
        blocks = [held[2 * b + 1, 1024 + k * 128 : 1152 + k * 128, :] for k in range(N_TP)]
        pre = mm(x, jnp.concatenate([gate_weight, up_weight], axis=1))
        upper = mm(g, jnp.concatenate(blocks, axis=1), NT)
        gate_pre, up_pre = pre[:, :128], pre[:, 128:]
        sigmoid = jax.nn.sigmoid(gate_pre)
        activated = gate_pre * sigmoid
        hidden_ref[:, 128 * b : 128 * b + 128] = (activated * up_pre).astype(BF)
        gate = upper * up_pre * sigmoid * (1.0 + gate_pre * (1.0 - sigmoid))
        grads_ref[:, 256 * b : 256 * b + 128] = gate.astype(BF)
        grads_ref[:, 256 * b + 128 : 256 * b + 256] = (upper * activated).astype(BF)
    grads = grads_ref[...]

    def up_rows(b, at):
        if at < 1024:
            return held[2 * b, 2048 + at : 2304 + at, :]
        return held[2 * b + 1, at - 1024 : at - 768, :]

    for k in range(0, N_TP, 2):
        at = k * 128
        weight = []
        for b in range(4):
            weight += [held[2 * b, at : at + 256, :], up_rows(b, at)]
        part = mm(grads, jnp.concatenate(weight, axis=1), NT).astype(BF)
        part_ref[k] = part[:, :128]
        part_ref[k + 1] = part[:, 128:]


def weight_grads_kernel(rows_ref, grads_ref, hidden_ref, *out_refs):
    grads = grads_ref[...]
    hidden = hidden_ref[...]
    for k in range(0, N_TP, 2):
        x = jnp.concatenate([rows_ref[k, :PART, :], rows_ref[k + 1, :PART, :]], axis=1)
        g = jnp.concatenate([rows_ref[k, PART:, :], rows_ref[k + 1, PART:, :]], axis=1)
        both = mm(x, grads, TN)
        down = mm(hidden, g, TN)
        at = k * 128
        for b in range(4):

            def put(lot, row, value):
                ref, start = place_of(out_refs, b, lot, row)
                ref[start : start + len(value), :] = value.astype(ref.dtype)

            put(0, at, both[:, 256 * b : 256 * b + 128])
            up = both[:, 256 * b + 128 : 256 * b + 256]
            if k < N_TP // 2:
                put(0, 2048 + at, up)
            else:
                put(1, at - 1024, up)
            for n in range(2):
                block = down[128 * b : 128 * b + 128, n * 128 : (n + 1) * 128]
                put(1, 1024 + at + n * 128, block)


def place_of(refs, device, lot, row):
    own_a, own_b, to_left, to_right, left_b, left_late, right_a, right_late = refs
    if device == 0:
        return (own_a, own_b)[lot], row
    if device == 3:
        return ((to_right, row), (to_left, EARLY + row))[lot]
    if device == 1:
        if lot == 1:
            return left_b, row
        return (to_left, row) if row < EARLY else (left_late, row - EARLY)
    if lot == 0:
        return right_a, row
    return (to_right, LOT + row) if row < EARLY else (right_late, row - EARLY)


def relay_kernel(
    left_b_ref,
    left_late_ref,
    right_a_ref,
    right_late_ref,
    from_right_ref,
    from_left_ref,
    to_left_ref,
    to_right_ref,
):
    far_a, far_b = from_left_ref[:LOT, :].astype(F32), from_right_ref[EARLY:, :].astype(F32)
    to_right_ref[:LOT, :] = (right_a_ref[...].astype(F32) + far_a).astype(BF)
    to_right_ref[LOT:, :] = right_late_ref[...]
    to_left_ref[:EARLY, :] = left_late_ref[...]
    to_left_ref[EARLY:, :] = (left_b_ref[...].astype(F32) + far_b).astype(BF)


def grad_sum_kernel(
    own_a_ref,
    own_b_ref,
    from_right_ref,
    from_left_ref,
    last_left_ref,
    last_right_ref,
    gate_ref,
    up_ref,
    down_ref,
):
    def total(at):
        lot, row = divmod(at, LOT)
        if lot == 0:
            own, summed = (own_a_ref, row), (last_left_ref, row)
            single = (from_right_ref if row < EARLY else last_right_ref, row % EARLY)
        else:
            own, summed = (own_b_ref, row), (last_right_ref, EARLY + row)
            single = (from_left_ref if row < EARLY else last_left_ref, LOT + row % EARLY)
        rows = [r[start : start + 128, :].astype(F32) for r, start in (own, summed, single)]
        return (rows[0] + rows[1] + rows[2]).astype(BF)

    for k in range(N_TP):
        here = slice(k * 128, (k + 1) * 128)
        gate_ref[here, :] = total(k * 128)
        up_ref[here, :] = total(2048 + k * 128)
        down_ref[:, here] = total(4096 + k * 128)


def row_sum_kernel(place_ref, part_ref, states_ref, out_ref, total):
    for q in range(4):
        acc = jnp.zeros((PART, 128), F32)
        for j in range(4):
            source = jnp.where(place_ref[1] == 0, 4 * j + q, 4 * q + j)
            acc = acc + part_ref[source].astype(F32)
        total[q * PART : (q + 1) * PART, :] = acc
    total[ROWS:, :] = jnp.zeros((8, 128), F32)
    row = iota((PAD, 128), 0)
    high, low = two_parts(states_ref[...])
    for e in range(N_SP):
        rows = jnp.where(row < CAP, total[e * CAP : e * CAP + PAD, :], 0.0)
        rows = jnp.where(row == CAP, high[e : e + 1], rows)
        rows = jnp.where(row == CAP + 1, low[e : e + 1], rows)
        out_ref[e] = rows.astype(BF)


def residual_kernel(back_ref, turned_ref, g_ref, out_ref):
    routed = mm(turned_ref[...], back_ref[...].reshape(SLOTS, 128))
    residual = (g_ref[...].astype(F32) + routed).astype(BF)
    for k in range(N_TP):
        out_ref[k] = residual


def scores_of(queries, keys, mask, causal):
    return jnp.where(causal, mm(queries * mask, keys, NT), 0.0)


def causal_blocks():
    row, col = iota((TOK, TOK), 0), iota((TOK, TOK), 1)
    return (row // BLOCK == col // BLOCK) & (col <= row)


def forward_kernel(back_ref, q_ref, k_ref, v_ref, decay_ref, out_ref, entering_ref):
    key_mask, val_mask, own = head_masks()
    rows = [back_ref[s, CAP : CAP + 2, :].astype(F32) for s in range(N_SP)]
    packed = jnp.concatenate([r[0:1] + r[1:2] for r in rows], axis=0)
    state = opened_state(packed, own)
    queries = q_ref[...].astype(F32).T
    keys = k_ref[...].astype(F32).T * SCALE
    values = v_ref[...].astype(F32)
    cumulative = block_sums(decay_ref[...].T)
    closing = closings(cumulative)
    scaled_q = queries * jnp.exp(cumulative)
    scaled_k = keys * jnp.exp(-cumulative)
    tail = keys * jnp.exp(per_block(closing) - cumulative)
    causal = causal_blocks()
    within = jnp.zeros((TOK, 128), F32)
    for h in range(2):
        scores = scores_of(scaled_q, scaled_k, key_mask[h], causal)
        within = within + mm(scores, values * val_mask[h])
    for n in range(NBLK):
        here = slice(n * BLOCK, (n + 1) * BLOCK)
        entering_ref[n] = state
        out_ref[here, :] = (within[here] + mm(scaled_q[here], state, NT)).astype(BF)
        state = jnp.exp(closing[n]) * state + mm(values[here], tail[here], TN) * own


def mixer_grad_kernel(
    place_ref, full_ref, w_ref, mixed_ref, q_ref, decay_ref, grad_ref, span_ref, sent_ref, kept_ref
):
    _, _, own = head_masks()
    grad = mm(wide(full_ref, 0, TOK), w_ref[...])
    grad_ref[...] = grad
    so_far, _ = whole_sums(block_sums(decay_ref[...].T))
    scaled = q_ref[...].astype(F32).T * jnp.exp(so_far)
    packed = packed_state(mm(grad, scaled, TN) * own)
    span_ref[...] = packed
    high, low = two_parts(packed)
    sent_ref[1024:1056, :] = high.astype(BF)
    sent_ref[1056:, :] = low.astype(BF)
    mixed = mixed_ref[...]
    first = place_ref[1] == 0
    for k in range(0, N_TP, 2):
        rows = jnp.concatenate([full_ref[k], full_ref[k + 1]], axis=1)
        part = mm(rows, mixed, TN)
        for n in range(2):
            low, high = part[n * 128 : n * 128 + 64], part[n * 128 + 64 : n * 128 + 128]
            here = slice((k + n) * 64, (k + n + 1) * 64)
            kept_ref[here, :] = jnp.where(first, low, high)
            sent_ref[here, :] = jnp.where(first, high, low).astype(BF)


def chip_kernel(place_ref, recv_ref, kept_ref, span_ref, reach_ref, sent_ref, other_ref):
    other = recv_ref[1024:1056, :].astype(F32) + recv_ref[1056:, :].astype(F32)
    other_ref[...] = other
    first = place_ref[1] == 0
    mine = span_ref[...]
    both = jnp.where(first, mine, other) + reach_ref[16:17, :] * jnp.where(first, other, mine)
    for z in range(16):
        here = slice(z * 64, (z + 1) * 64)
        sent_ref[z, :32, :] = (both * reach_ref[z : z + 1, :]).astype(BF)
        sent_ref[z, 32:, :] = (kept_ref[here, :] + recv_ref[here, :].astype(F32)).astype(BF)


def local_backward_kernel(
    grad_ref,
    entering_ref,
    q_ref,
    k_ref,
    v_ref,
    decay_ref,
    gq_ref,
    value_ref,
    keys_ref,
    change_ref,
    tail_ref,
    reach_ref,
    rest_ref,
    leave_ref,
):
    key_mask, val_mask, own = head_masks()
    grad = grad_ref[...]
    queries = q_ref[...].astype(F32).T
    keys = k_ref[...].astype(F32).T * SCALE
    values = v_ref[...].astype(F32)
    cumulative = block_sums(decay_ref[...].T)
    closing = closings(cumulative)
    grow, shrink = jnp.exp(cumulative), jnp.exp(-cumulative)
    rest = jnp.exp(per_block(closing) - cumulative)
    scaled_q, scaled_k, tail = queries * grow, keys * shrink, keys * rest
    causal = causal_blocks()
    value_grad = jnp.zeros((TOK, 128), F32)
    query_grad = jnp.zeros((TOK, 64), F32)
    key_grad = jnp.zeros((TOK, 64), F32)
    for h in range(2):
        scores = scores_of(scaled_q, scaled_k, key_mask[h], causal)
        score_grad = jnp.where(causal, mm(grad * val_mask[h], values, NT), 0.0)
        value_grad = value_grad + mm(scores, grad * val_mask[h], TN)
        query_grad = query_grad + mm(score_grad, scaled_k * key_mask[h])
        key_grad = key_grad + mm(score_grad, scaled_q * key_mask[h], TN)
    carried_v, carried_q, tail_grad, close_grad, reach = ([None] * NBLK for _ in range(5))
    state_grad, later = jnp.zeros((128, 64), F32), jnp.zeros((1, 64), F32)
    for n in reversed(range(NBLK)):
        here = slice(n * BLOCK, (n + 1) * BLOCK)
        entering = entering_ref[n]
        decay_out = jnp.exp(closing[n])
        reach[n] = jnp.exp(later)
        later = later + closing[n]
        leave_ref[n : n + 1, :] = jnp.exp(later)
        carried_v[n] = mm(tail[here], state_grad, NT)
        carried_q[n] = mm(grad[here], entering)
        tail_grad[n] = mm(values[here], state_grad)
        close_grad[n] = decay_out * jnp.sum(state_grad * entering, axis=0, keepdims=True) + jnp.sum(
            tail_grad[n] * tail[here], axis=0, keepdims=True
        )
        state_grad = decay_out * state_grad + mm(grad[here], scaled_q[here], TN) * own
    value_ref[...] = value_grad + jnp.concatenate(carried_v, axis=0)
    query_grad = query_grad + jnp.concatenate(carried_q, axis=0)
    tail_grad = jnp.concatenate(tail_grad, axis=0)
    change = query_grad * scaled_q - key_grad * scaled_k - tail_grad * tail
    row, col = iota((TOK, TOK), 0), iota((TOK, TOK), 1)
    onward = ((row // BLOCK == col // BLOCK) & (col >= row)).astype(F32)
    change_ref[...] = picked_sums(onward, change) + per_block(close_grad)
    gq_ref[...] = (query_grad * grow).T.astype(BF)
    keys_ref[...] = (key_grad * shrink + tail_grad * rest) * SCALE
    tail_ref[...] = tail
    reach_ref[...] = per_block(reach)
    rest_ref[...] = rest * SCALE


def backward_kernel(
    place_ref,
    later_ref,
    other_ref,
    chips_ref,
    entering_ref,
    v_ref,
    value_ref,
    keys_ref,
    change_ref,
    tail_ref,
    reach_ref,
    rest_ref,
    leave_ref,
    gp_ref,
    gk_ref,
    gv_ref,
    gd_ref,
):
    _, _, own = head_masks()
    sums = later_ref[0].astype(F32)
    for z in range(1, 16):
        sums = sums + later_ref[z].astype(F32)
    gp_ref[...] = sums[32:]
    packed = sums[:32]
    packed = jnp.where(place_ref[1] == 0, chips_ref[17:18, :] * packed + other_ref[...], packed)
    state_grad = opened_state(packed, own)
    tail, reach = tail_ref[...], reach_ref[...]
    gv_ref[...] = (value_ref[...] + mm(tail * reach, state_grad, NT)).astype(BF)
    tail_grad = mm(v_ref[...], state_grad) * reach
    gk_ref[...] = (keys_ref[...] + tail_grad * rest_ref[...]).T.astype(BF)
    row, col = iota((TOK, TOK), 0), iota((TOK, TOK), 1)
    ahead = ((row // BLOCK == col // BLOCK) & (col < row)).astype(F32)
    passed = [
        leave_ref[n : n + 1, :] * jnp.sum(state_grad * entering_ref[n], axis=0, keepdims=True)
        for n in range(NBLK)
    ]
    change = change_ref[...] + picked_sums(ahead, tail_grad * tail) + per_block(passed)
    gd_ref[...] = change.T


def exchanged(blocks, axis):
    return lax.all_to_all(blocks, axis, split_axis=0, concat_axis=0, tiled=True)


def ring_step(step):
    pairs = []
    for t in range(N_TP):
        y, x = t // 4, t % 4
        pairs.append((t, 4 * y + (x + step) % 4))
        pairs.append((N_TP + t, N_TP + 4 * ((y + step) % 4) + x))
    return pairs


def passed_on(array, step):
    return lax.ppermute(array, ("sp_1", "tp"), ring_step(step))


def body(
    moe_input,
    out_grad,
    routes,
    route_weight,
    w_gate,
    w_up,
    w_down,
    w_out,
    queries,
    key_rows,
    value_rows,
    log_decay,
):
    q_t, k_t, decay_t = queries.T, key_rows.T, log_decay.T
    place = jnp.stack(
        [lax.axis_index(SP), lax.axis_index("sp_1"), lax.axis_index("sp_0")]
    ).astype(jnp.int32)

    sent, pick = call(
        dispatch_kernel,
        [((N_SP, 2 * PAD, 128), BF), ((SLOTS, TOK), BF)],
        routes.T,
        route_weight.T,
        moe_input,
        out_grad,
        k_t,
        value_rows,
        decay_t,
    )
    recv = exchanged(sent, SP)
    own_a, own_b = call(
        pack_kernel,
        [((LOT, 128), BF), ((LOT, 128), BF)],
        w_gate[0],
        w_up[0],
        w_down[0],
        near_out=(0, 1),
    )
    left_a = passed_on(own_a, 1)
    right_b = passed_on(own_b, -1)
    left_b = passed_on(own_b, 1)
    right_a = passed_on(own_a, -1)
    far_a = passed_on(left_a, 1)
    far_b = passed_on(right_b, -1)
    weights = (own_a, own_b, left_a, left_b, right_a, right_b, far_a, far_b)
    (copies,) = call(
        copies_kernel,
        [((N_TP, 2 * PART, 128), BF)],
        place,
        recv,
        scratch=[pltpu.VMEM((2 * ROWS, 128), F32), pltpu.VMEM((4, 2 * PART, 128), BF)],
        smem=(0,),
        near=(1,),
    )
    rows = exchanged(copies, "tp")
    (turned,) = call(turned_kernel, [((TOK, SLOTS), BF)], pick, after=(copies,))
    partial_rows, grads, hidden = call(
        partial_kernel,
        [((N_TP, PART, 128), BF), ((PART, 1024), BF), ((PART, 512), BF)],
        rows,
        *weights,
        scratch=[pltpu.VMEM((8, LOT, 128), BF), pltpu.SemaphoreType.DMA((8,))],
        near=(0,),
        near_out=(1, 2),
        raw=tuple(range(1, 9)),
    )
    states, reach = call(
        scan_kernel,
        [((N_SP, 128), F32), ((24, 128), F32)],
        place,
        recv,
        smem=(0,),
        after=(partial_rows,),
    )
    arrived = exchanged(partial_rows, "tp")
    own_grad_a, own_grad_b, to_left, to_right, *held_back = call(
        weight_grads_kernel,
        2 * [((LOT, 128), F32)]
        + 2 * [((LOT + EARLY, 128), BF)]
        + 2 * [((LOT, 128), BF), ((EARLY, 128), BF)],
        rows,
        grads,
        hidden,
        near=(0, 1, 2),
    )
    from_left = passed_on(to_right, 1)
    from_right = passed_on(to_left, -1)
    (returned,) = call(
        row_sum_kernel,
        [((N_SP, PAD, 128), BF)],
        place,
        arrived,
        states,
        smem=(0,),
        near=(1,),
        scratch=[pltpu.VMEM((ROWS + 8, 128), F32)],
    )
    back = exchanged(returned, SP)
    (residual,) = call(residual_kernel, [((N_TP, TOK, 128), BF)], back, turned, out_grad, near=(0,))
    full_grad = exchanged(residual, "tp")
    lot_left, lot_right = call(
        relay_kernel,
        2 * [((LOT + EARLY, 128), BF)],
        *held_back,
        from_right,
        from_left,
        after=(residual,),
        near=(4, 5),
    )
    last_a = passed_on(lot_right, 1)
    last_b = passed_on(lot_left, -1)
    mixer_out, entering = call(
        forward_kernel,
        [((TOK, 128), BF), ((NBLK, 128, 64), F32)],
        back,
        q_t,
        k_t,
        value_rows,
        decay_t,
        near=(0,),
        near_out=(0,),
        after=(residual,),
    )
    mixer_grad, span_grad, to_other, kept = call(
        mixer_grad_kernel,
        [((TOK, 128), F32), ((32, 128), F32), ((1088, 128), BF), ((1024, 128), F32)],
        place,
        full_grad,
        w_out,
        mixer_out,
        q_t,
        decay_t,
        smem=(0,),
        near=(1, 3),
        near_out=(1, 2, 3),
    )
    from_other = lax.ppermute(to_other, "sp_1", [(0, 1), (1, 0)])
    chip_sent, other_grad = call(
        chip_kernel,
        [((16, 96, 128), BF), ((32, 128), F32)],
        place,
        from_other,
        kept,
        span_grad,
        reach,
        smem=(0,),
        near=(1, 2, 3),
    )
    later = exchanged(chip_sent, "sp_0")
    gq, *local = call(
        local_backward_kernel,
        [
            ((64, TOK), BF),
            ((TOK, 128), F32),
            ((TOK, 64), F32),
            ((TOK, 64), F32),
            ((TOK, 64), F32),
            ((TOK, 64), F32),
            ((TOK, 64), F32),
            ((NBLK, 64), F32),
        ],
        mixer_grad,
        entering,
        q_t,
        k_t,
        value_rows,
        decay_t,
        after=(chip_sent,),
    )
    grad_proj, gk, gv, gd = call(
        backward_kernel,
        [((64, 128), F32), ((64, TOK), BF), ((TOK, 128), BF), ((64, TOK), F32)],
        place,
        later,
        other_grad,
        reach,
        entering,
        value_rows,
        *local,
        smem=(0,),
        near=(1,),
    )
    gate_part, up_part, down_part = call(
        grad_sum_kernel,
        [((2048, 128), BF), ((2048, 128), BF), ((128, 2048), BF)],
        own_grad_a,
        own_grad_b,
        from_right,
        from_left,
        last_a,
        last_b,
        near=(2, 3, 4, 5),
        after=(chip_sent,),
    )
    return (gate_part[None], up_part[None], down_part[None], grad_proj, gq.T, gk.T, gv, gd.T)


def solution(mesh):
    split = Mesh(mesh.devices.reshape(16, 2, mesh.shape["tp"]), ("sp_0", "sp_1", "tp"))
    placed = (
        P(SP, "tp"),
        P(SP, "tp"),
        P(SP, None),
        P(SP, None),
        P(SP, None, "tp"),
        P(SP, None, "tp"),
        P(SP, "tp", None),
        P(None, "tp"),
        P(SP, "tp"),
        P(SP, "tp"),
        P(SP, "tp"),
        P(SP, "tp"),
    )
    return jax.shard_map(
        body,
        mesh=split,
        in_specs=placed,
        out_specs=(
            P(SP, None, "tp"),
            P(SP, None, "tp"),
            P(SP, "tp", None),
            P(SP, "tp"),
            P(SP, "tp"),
            P(SP, "tp"),
            P(SP, "tp"),
            P(SP, "tp"),
        ),
        check_vma=False,
    )
```
